512 devices in a mesh: fs: 32 (over z, core), tp: 16 (over y, x).
Axes of the slice: x: 4, y: 4, z: 16, core: 2. Of those that a mesh axis runs over, the one named last changes fastest.
Arguments:
- attn_out: bfloat16 [49152, 2048], P('fs', 'tp'), may hold values from -6 to 6
- out_cot: bfloat16 [49152, 4096], P('fs', 'tp'), may hold values from -6 to 6
- latent: bfloat16 [49152, 1024], P('fs', 'tp'), may hold values from -6 to 6
- value_cot: bfloat16 [49152, 2048], P('fs', 'tp'), may hold values from -6 to 6
- out_weight: float32 [2048, 4096], P('fs', 'tp'), may hold values from -0.125 to 0.125
- value_up_matrix: float32 [1024, 2048], P('fs', 'tp'), may hold values from -0.1875 to 0.1875
- out_basis: bfloat16 [2048, 256], P('fs'), as said below
- value_basis: bfloat16 [1024, 256], P('fs'), as said below
- out_mean: float32 [256, 4096], P(None, 'tp'), may hold values from -5320.86 to 5320.86
- out_square: float32 [256, 4096], P(None, 'tp'), may hold values from 49152 to 9830400, as said below
- value_mean: float32 [256, 2048], P(None, 'tp'), may hold values from -5320.86 to 5320.86
- value_square: float32 [256, 2048], P(None, 'tp'), may hold values from 49152 to 9830400, as said below
Outputs:
- out_step: float32 [2048, 4096], P('fs', 'tp')
- out_new: float32 [2048, 4096], P('fs', 'tp')
- out_copy: bfloat16 [2048, 4096], P(None, 'tp')
- out_mean_new: float32 [256, 4096], P(None, 'tp')
- out_square_new: float32 [256, 4096], P(None, 'tp')
- value_step: float32 [1024, 2048], P('fs', 'tp')
- value_new: float32 [1024, 2048], P('fs', 'tp')
- value_copy: bfloat16 [1024, 2048], P(None, 'tp')
- value_mean_new: float32 [256, 2048], P(None, 'tp')
- value_square_new: float32 [256, 2048], P(None, 'tp')
The draws below stay inside these ranges and needn't reach their ends.
Inputs may be any that keep to these rules, and one draw needn't show every extreme that they name: `out_basis`: factors of full rank, rows of differing scales. `value_basis`: factors of full rank, rows of differing scales. `out_square`: Positive. `value_square`: Positive.
All inputs are finite; a program needn't handle non-finite values.
Results may differ from the reference program's by a relative error of at most 0.012.
Values may be sent and summed in bfloat16 or wider, within the bound.
No kernel may reach another device: no remote copies, remote signals or barrier semaphores. Data moves between devices by JAX's collectives and lax.ppermute only.
A program may use at most 64 MiB of HBM per device.

```python
import jax
import jax.numpy as jnp
from jax import lax

D = 4096
LATENT_WIDTH = 1024
RANK = 256
VALUE_FEATURES = 2048
TOKEN_TOTAL = 49152


def draw_out_basis(key, part):
    row_slices = VALUE_FEATURES
    index = jnp.arange(row_slices, dtype=jnp.float32) / (row_slices - 1)
    base = jnp.clip(jax.random.normal(jax.random.fold_in(key, 22), (row_slices, RANK), jnp.float32), -4.0, 4.0)
    ramp = 10.0 ** index
    return (base * ramp[:, None] * row_slices ** (-0.5)).astype(jnp.bfloat16)


def draw_value_basis(key, part):
    row_slices = LATENT_WIDTH
    index = jnp.arange(row_slices, dtype=jnp.float32) / (row_slices - 1)
    base = jnp.clip(jax.random.normal(jax.random.fold_in(key, 32), (row_slices, RANK), jnp.float32), -4.0, 4.0)
    ramp = 10.0 ** index
    return (base * ramp[:, None] * row_slices ** (-0.5)).astype(jnp.bfloat16)


def draw_out_square(key, part):
    cols = D
    index = jnp.arange(cols, dtype=jnp.float32) / (cols - 1)
    base = jnp.exp(jax.random.uniform(jax.random.fold_in(key, 42), (RANK, cols), jnp.float32, -1.2, 1.09))
    ramp = 10.0 ** (index - 0.5)
    return 20.0 * TOKEN_TOTAL * base * ramp[None, :]


def draw_value_square(key, part):
    cols = VALUE_FEATURES
    index = jnp.arange(cols, dtype=jnp.float32) / (cols - 1)
    base = jnp.exp(jax.random.uniform(jax.random.fold_in(key, 52), (RANK, cols), jnp.float32, -1.2, 1.09))
    ramp = 10.0 ** (index - 0.5)
    return 20.0 * TOKEN_TOTAL * base * ramp[None, :]


def strengthened(array, own_key, source, target, parts, factor):
    def block_of(axis_at):
        return (jnp.arange(array.shape[axis_at]) // (array.shape[axis_at] // parts)).reshape((-1,) + (1,) * (array.ndim - 1 - axis_at))

    first = jax.random.permutation(own_key, parts)[block_of(target)]
    other_side = (block_of(target) + parts // 2) % parts
    return jnp.where((block_of(source) == first) | (block_of(source) == other_side), factor * array, array)


def steps_of(key, dims, shards, smallest, largest):
    loudness = 1.0
    for position, shards_of in shards:
        draws = jax.random.uniform(jax.random.fold_in(jax.random.fold_in(key, 6), position), (shards_of,), jnp.float32, smallest / len(shards), largest / len(shards))
        loudness = loudness * jnp.repeat(jnp.exp(draws), dims[position] // shards_of).reshape((-1,) + (1,) * (len(dims) - 1 - position))
    return loudness


def noise(own_key, shape, scale, most, shards=(), kind=jnp.bfloat16):
    array = scale * jax.random.normal(own_key, shape, jnp.float32)
    if shards:
        array = array * steps_of(own_key, shape, shards, -0.22, 0.18)
    return jnp.clip(array, -most, most).astype(kind)


def noise_with(rng, extent, scale, bound, split, heavy, kind=jnp.bfloat16):
    values = scale * jax.random.normal(rng, extent, jnp.float32)
    if split:
        values = values * steps_of(rng, extent, split, -0.22, 0.18)
    return jnp.clip(strengthened(values, jax.random.fold_in(rng, 3), *heavy), -bound, bound).astype(kind)


def setup_inputs(seed: int = 0) -> dict:
    seeds = jax.random.split(jax.random.key(seed), 13)
    attn_out = noise_with(seeds[0], (TOKEN_TOTAL, VALUE_FEATURES), 1.0, 6.0, ((0, 32), (1, 16)), (0, 1, 32, 2.75))
    out_cot = noise(seeds[1], (TOKEN_TOTAL, D), 1.0, 6.0, ((0, 32), (1, 16)))
    latent = noise_with(seeds[2], (TOKEN_TOTAL, LATENT_WIDTH), 1.0, 6.0, ((0, 32), (1, 16)), (0, 1, 32, 2.75))
    value_cot = noise(seeds[3], (TOKEN_TOTAL, VALUE_FEATURES), 1.0, 6.0, ((0, 32), (1, 16)))
    out_weight = noise(seeds[4], (VALUE_FEATURES, D), VALUE_FEATURES ** -0.5, 0.125, ((0, 32), (1, 16)), jnp.float32)
    value_up_matrix = noise(seeds[5], (LATENT_WIDTH, VALUE_FEATURES), LATENT_WIDTH ** -0.5, 0.1875, ((0, 32), (1, 16)), jnp.float32)
    out_basis = draw_out_basis(jax.random.fold_in(seeds[12], 71), 0)
    value_basis = draw_value_basis(jax.random.fold_in(seeds[12], 71), 0)
    out_mean = noise(seeds[8], (RANK, D), (4 * TOKEN_TOTAL ** 0.5), 5320.86, ((1, 16),), jnp.float32)
    out_square = draw_out_square(jax.random.fold_in(seeds[12], 71), 0)
    value_mean = noise(seeds[10], (RANK, VALUE_FEATURES), (4 * TOKEN_TOTAL ** 0.5), 5320.86, ((1, 16),), jnp.float32)
    value_square = draw_value_square(jax.random.fold_in(seeds[12], 71), 0)
    return {"attn_out": attn_out, "out_cot": out_cot, "latent": latent, "value_cot": value_cot, "out_weight": out_weight, "value_up_matrix": value_up_matrix, "out_basis": out_basis, "value_basis": value_basis, "out_mean": out_mean, "out_square": out_square, "value_mean": value_mean, "value_square": value_square}


LEARN_RATE = 0.01
MEAN_DECAY = 0.8
BETA_SQUARE = 0.9
EPS_RMS = 1e-06

def adapt(grad, basis, mean_in, square_in, weight_in):
    basis_f = basis.astype(jnp.float32)
    proj = jnp.dot(basis_f.T, grad, precision=lax.Precision.HIGHEST)
    mean_new = MEAN_DECAY * mean_in + (1.0 - MEAN_DECAY) * proj
    square_new = BETA_SQUARE * square_in + (1.0 - BETA_SQUARE) * proj * proj
    direction = mean_new / jnp.sqrt(square_new)
    update_delta = jnp.dot(basis_f, direction, precision=lax.Precision.HIGHEST)
    total = jnp.sum(update_delta * update_delta)
    count = update_delta.shape[0] * update_delta.shape[1]
    step = LEARN_RATE * update_delta * lax.rsqrt(total / count + EPS_RMS)
    weight_new = weight_in - step
    return (step, weight_new, weight_new.astype(jnp.bfloat16), mean_new, square_new)

def reference(attn_out, out_cot, latent, value_cot, out_weight, value_up_matrix, out_basis, value_basis, out_mean, out_square, value_mean, value_square):
    grad_out = jnp.dot(attn_out.T, out_cot, preferred_element_type=jnp.float32)
    grad_value = jnp.dot(latent.T, value_cot, preferred_element_type=jnp.float32)
    first = adapt(grad_out, out_basis, out_mean, out_square, out_weight)
    second = adapt(grad_value, value_basis, value_mean, value_square, value_up_matrix)
    return (first[0], first[1], first[2], first[3], first[4], second[0], second[1], second[2], second[3], second[4])
```

```python
import jax
import jax.numpy as jnp
from jax import lax
from jax.sharding import Mesh
from jax.sharding import PartitionSpec as P


TP = ("y", "x")
FS = ("zh", "zl", "c")
PLANE = ("c", "y", "x")
ALL = ("zh", "zl", "c", "y", "x")

LEARN_RATE = 0.01
MEAN_DECAY = 0.8
BETA_SQUARE = 0.9
EPS_RMS = 1e-06

BF = jnp.bfloat16
F32 = jnp.float32


def exchange(value, axes):
    return lax.all_to_all(value, axes, 0, 0, tiled=True)


def from_everyone(value, axes):
    devices = lax.axis_size(axes)
    return exchange(jnp.broadcast_to(value[None], (devices, *value.shape)), axes)


def swapped_blocks(value):
    pairs = []
    for j in range(16):
        for b in range(2):
            for t in range(16):
                pairs.append(((2 * j + b) * 16 + t, (2 * t + b) * 16 + j))
    return lax.ppermute(value, ALL, pairs)


def moments(proj, mean_in, square_in):
    mean_new = MEAN_DECAY * mean_in + (1.0 - MEAN_DECAY) * proj
    square_new = BETA_SQUARE * square_in + (1.0 - BETA_SQUARE) * proj * proj
    return (mean_new, square_new, mean_new / jnp.sqrt(square_new))


def split_dot(basis, direction):
    upper = direction.astype(BF)
    lower = (direction - upper.astype(F32)).astype(BF)
    return jnp.dot(basis, upper, preferred_element_type=F32) + jnp.dot(
        basis, lower, preferred_element_type=F32
    )


def per_device(
    attn_out,
    out_cot,
    latent,
    value_cot,
    out_weight,
    value_up_matrix,
    out_basis,
    value_basis,
    out_mean,
    out_square,
    value_mean,
    value_square,
):
    tokens, heads = attn_out.shape
    lat = latent.shape[1]
    cols_o = out_cot.shape[1]
    cols_v = value_cot.shape[1]
    rows_o, rank = out_basis.shape
    rows_v = value_basis.shape[0]
    tp = lax.axis_size(TP)
    fs = lax.axis_size(FS)
    mine = tokens // tp

    early_o, early_v = lax.optimization_barrier((out_weight, value_up_matrix))
    w_o = early_o.astype(BF).reshape(-1, 128)
    w_v = early_v.astype(BF)
    packed = lax.optimization_barrier(jnp.concatenate([w_o, w_v], 0))
    held = lax.all_gather(packed, FS)

    block = jnp.concatenate([out_basis, value_basis], 0)
    block = swapped_blocks(block)

    lat3 = latent.reshape(tp, 2, mine // 2, lat)
    lat_packed = jnp.concatenate([lat3[:, 0], lat3[:, 1]], -1)
    sent = jnp.concatenate([attn_out.reshape(tp, mine, heads), lat_packed], 1)
    got = exchange(sent, TP)

    blocks = from_everyone(block, PLANE).reshape(2, tp, rows_o + rows_v, rank)
    whole_o = blocks[:, :, :rows_o].swapaxes(0, 1).reshape(-1, rank)
    whole_v = blocks[:, :, rows_o:].swapaxes(0, 1).reshape(-1, rank)

    heads_all = got[:, :mine].swapaxes(0, 1).reshape(mine, -1)
    lat_got = got[:, mine:]
    lat_all = jnp.concatenate(
        [
            lat_got[:, :, :lat].swapaxes(0, 1).reshape(mine // 2, -1),
            lat_got[:, :, lat:].swapaxes(0, 1).reshape(mine // 2, -1),
        ],
        0,
    )
    lifted_o = jnp.dot(heads_all, whole_o, preferred_element_type=F32)
    lifted_v = jnp.dot(lat_all, whole_v, preferred_element_type=F32)
    lifted = jnp.concatenate([lifted_o.astype(BF), lifted_v.astype(BF)], 1)
    lifted = from_everyone(lifted, TP).reshape(tokens, 2 * rank)

    part_o = jnp.dot(lifted[:, :rank].T, out_cot, preferred_element_type=F32)
    part_v = jnp.dot(lifted[:, rank:].T, value_cot, preferred_element_type=F32)
    part = jnp.concatenate([part_o.astype(BF), part_v.astype(BF)], 1)
    near = lax.axis_size(("zl", "c"))
    part = exchange(part.reshape(near, rank // near, -1), ("zl", "c"))
    part = part.astype(F32).sum(0)
    part = from_everyone(part, "zh").sum(0)
    proj = from_everyone(part.astype(BF), ("zl", "c")).reshape(rank, -1).astype(F32)

    mean_o, square_o, direction_o = moments(proj[:, :cols_o], out_mean, out_square)
    mean_v, square_v, direction_v = moments(proj[:, cols_o:], value_mean, value_square)
    update_o = jnp.dot(whole_o, direction_o.astype(BF), preferred_element_type=F32)
    update_v = jnp.dot(whole_v, direction_v.astype(BF), preferred_element_type=F32)
    totals = jnp.stack([jnp.sum(update_o * update_o), jnp.sum(update_v * update_v)])
    totals = jnp.broadcast_to(totals[:, None], (2, 128))
    totals = from_everyone(totals, TP).sum(0)
    count_o = rows_o * fs * cols_o * tp
    count_v = rows_v * fs * cols_v * tp
    scale_o = LEARN_RATE * lax.rsqrt(totals[0, 0] / count_o + EPS_RMS)
    scale_v = LEARN_RATE * lax.rsqrt(totals[1, 0] / count_v + EPS_RMS)
    step_o = split_dot(out_basis, direction_o) * scale_o
    step_v = split_dot(value_basis, direction_v) * scale_v
    new_o = out_weight - step_o
    new_v = value_up_matrix - step_v

    split = w_o.shape[0]
    held_o = held[:, :split].reshape(rows_o * fs, cols_o)
    held_v = held[:, split:].reshape(rows_v * fs, cols_v)
    copy_o = (held_o.astype(F32) - scale_o * update_o).astype(BF)
    copy_v = (held_v.astype(F32) - scale_v * update_v).astype(BF)
    return (step_o, new_o, copy_o, mean_o, square_o, step_v, new_v, copy_v, mean_v, square_v)


def solution(mesh):
    torus = Mesh(mesh.devices.reshape(4, 4, 2, 4, 4), ALL)
    both = P(FS, TP)
    cols = P(None, TP)
    rows = P(FS, None)

    return jax.shard_map(
        per_device,
        mesh=torus,
        in_specs=(both, both, both, both, both, both, rows, rows, cols, cols, cols, cols),
        out_specs=(both, both, cols, cols, cols, both, both, cols, cols, cols),
        check_vma=False,
    )
```

```python
import functools

import jax
import jax.numpy as jnp
from jax import lax
from jax.experimental import pallas as pl
from jax.experimental.pallas import tpu as pltpu
from jax.sharding import Mesh
from jax.sharding import PartitionSpec as P


TP = ("y", "x")
FS = ("zh", "zl", "c")
NEAR = ("zl", "c")
ALL = ("zh", "zl", "c", "y", "x")

LEARN_RATE = 0.01
MEAN_DECAY = 0.8
BETA_SQUARE = 0.9
EPS_RMS = 1e-06

BF = jnp.bfloat16
ROOM = 20 * 2**20
F32 = jnp.float32


def exchange(value, axes):
    return lax.all_to_all(value, axes, 0, 0, tiled=True)


def from_everyone(value, axes):
    devices = lax.axis_size(axes)
    return exchange(jnp.broadcast_to(value[None], (devices, *value.shape)), axes)


def swapped_blocks(value):
    pairs = []
    for j in range(16):
        for b in range(2):
            for t in range(16):
                pairs.append(((2 * j + b) * 16 + t, (2 * t + b) * 16 + j))
    return lax.ppermute(value, ALL, pairs)


def shifted(value, axis, by):
    devices = lax.axis_size(axis)
    return lax.ppermute(value, axis, [(i, (i + by) % devices) for i in range(devices)])


def dot(a, b):
    return jnp.dot(a, b, preferred_element_type=F32)


def pack_kernel(attn_ref, lat_ref, out_ref):
    groups = out_ref.shape[0]
    tokens = attn_ref.shape[0] // groups
    each = tokens // groups
    turned = lat_ref[...].T
    for g in range(groups):
        pieces = []
        for p in range(groups):
            at = (p * groups + g) * each
            out_ref[g, p * each : (p + 1) * each, :] = attn_ref[at : at + each, :]
            pieces.append(turned[at : at + each])
        half = groups // 2
        for p in range(half):
            at = tokens + p * each
            out_ref[g, at : at + each, :] = jnp.concatenate([pieces[p], pieces[half + p]], axis=1)


def pack(attn_out, lat_turned, groups):
    tokens, heads = attn_out.shape
    rows = tokens // groups
    return pl.pallas_call(
        pack_kernel,
        out_shape=jax.ShapeDtypeStruct((groups, rows + rows // 2, heads), BF),
        cost_estimate=pl.CostEstimate(flops=10**7, bytes_accessed=10**6, transcendentals=0),
        compiler_params=pltpu.CompilerParams(vmem_limit_bytes=ROOM),
        name="pack",
    )(attn_out, lat_turned)


def lift_kernel(rows_o, tokens, got_ref, blocks_ref, out_ref):
    groups = got_ref.shape[0]
    rank = blocks_ref.shape[2]
    half = tokens // 2
    first = jnp.zeros((tokens, rank), F32)
    second = jnp.zeros((half, 2 * rank), F32)
    for g in range(groups):
        low, high = blocks_ref[g], blocks_ref[groups + g]
        basis_o = jnp.concatenate([low[:rows_o], high[:rows_o]], 0)
        basis_v = jnp.concatenate([low[rows_o:], high[rows_o:]], 0)
        none = jnp.zeros_like(basis_v)
        pair = jnp.concatenate(
            [jnp.concatenate([basis_v, none], 0), jnp.concatenate([none, basis_v], 0)], 1
        )
        first = first + dot(got_ref[g, :tokens, :], basis_o)
        second = second + dot(got_ref[g, tokens:, :], pair)
    parts, each = out_ref.shape[:2]
    for p in range(parts):
        at = p * each
        out_ref[p, :, :rank] = first[at : at + each].astype(BF)
        row, side = at % half, at // half
        out_ref[p, :, rank:] = second[row : row + each, side * rank : (side + 1) * rank].astype(BF)


def lift(got, blocks, rows_o, tokens, parts):
    rank = blocks.shape[2]
    return pl.pallas_call(
        functools.partial(lift_kernel, rows_o, tokens),
        out_shape=jax.ShapeDtypeStruct((parts, tokens // parts, 2 * rank), BF),
        cost_estimate=pl.CostEstimate(flops=2 * 10**8, bytes_accessed=10**6, transcendentals=0),
        compiler_params=pltpu.CompilerParams(vmem_limit_bytes=ROOM),
        name="lift",
    )(got, blocks)


def spread_kernel(got_ref, out_ref):
    total = got_ref[0].astype(F32)
    for i in range(1, got_ref.shape[0]):
        total = total + got_ref[i].astype(F32)
    total = total.astype(out_ref.dtype)
    for i in range(out_ref.shape[0]):
        out_ref[i] = total


def summed_for(got, copies, kind):
    return pl.pallas_call(
        spread_kernel,
        out_shape=jax.ShapeDtypeStruct((copies, *got.shape[1:]), kind),
        cost_estimate=pl.CostEstimate(flops=10**7, bytes_accessed=10**6, transcendentals=0),
        compiler_params=pltpu.CompilerParams(vmem_limit_bytes=ROOM),
    )(got)


def direction_kernel(
    rows_o, got_ref, mean_o, square_o, mean_v, square_v, b0, b1, b2, b3,
    mean_o_out, square_o_out, mean_v_out, square_v_out, way_out, total_out,
):
    cols_o = mean_o.shape[1]
    near, _, _ = got_ref.shape
    proj = jnp.concatenate([got_ref[i] for i in range(near)], 0).astype(F32)
    ways = []
    for p, mean, square, mean_out, square_out in (
        (proj[:, :cols_o], mean_o, square_o, mean_o_out, square_o_out),
        (proj[:, cols_o:], mean_v, square_v, mean_v_out, square_v_out),
    ):
        mean_new = MEAN_DECAY * mean[...] + (1.0 - MEAN_DECAY) * p
        square_new = BETA_SQUARE * square[...] + (1.0 - BETA_SQUARE) * p * p
        mean_out[...] = mean_new
        square_out[...] = square_new
        ways.append(mean_new / jnp.sqrt(square_new))
    way_out[:, :cols_o] = ways[0]
    way_out[:, cols_o:] = ways[1]
    upper_o, upper_v = ways[0].astype(BF), ways[1].astype(BF)
    total_o = jnp.zeros((8, cols_o), F32)
    total_v = jnp.zeros((8, ways[1].shape[1]), F32)
    for ref in (b0, b1, b2, b3):
        count, _, _ = ref.shape
        basis_o = jnp.concatenate([ref[i, :rows_o, :] for i in range(count)], 0)
        basis_v = jnp.concatenate([ref[i, rows_o:, :] for i in range(count)], 0)
        update = dot(basis_o, upper_o)
        total_o = total_o + jnp.sum((update * update).reshape(-1, 8, cols_o), 0)
        update = dot(basis_v, upper_v)
        total_v = total_v + jnp.sum((update * update).reshape(-1, 8, update.shape[1]), 0)
    sums = [
        jnp.broadcast_to(jnp.sum(t, keepdims=True), (4, 128)) for t in (total_o, total_v)
    ]
    tile = jnp.concatenate(sums, 0)
    for i in range(total_out.shape[0]):
        total_out[i] = tile


def directions(rows_o, copies, got, mean_o, square_o, mean_v, square_v, segments):
    rank = mean_o.shape[0]
    shape = jax.ShapeDtypeStruct
    return pl.pallas_call(
        functools.partial(direction_kernel, rows_o),
        out_shape=(
            shape(mean_o.shape, F32),
            shape(mean_o.shape, F32),
            shape(mean_v.shape, F32),
            shape(mean_v.shape, F32),
            shape((rank, mean_o.shape[1] + mean_v.shape[1]), F32),
            shape((copies, 8, 128), F32),
        ),
        cost_estimate=pl.CostEstimate(flops=4 * 10**8, bytes_accessed=4 * 10**6, transcendentals=10**5),
        compiler_params=pltpu.CompilerParams(vmem_limit_bytes=ROOM),
        name="directions",
    )(got, mean_o, square_o, mean_v, square_v, *segments)


def output_kernel(
    rows_o, rows_v, counts, y_ref, total_ref, way_ref, weight_o, weight_v, local_o, local_v, held_ref,
    b0, b1, b2, b3,
    step_o_out, new_o_out, copy_o_out, step_v_out, new_v_out, copy_v_out,
):
    cols_o = weight_o.shape[1]
    total = total_ref[0]
    for i in range(1, total_ref.shape[0]):
        total = total + total_ref[i]
    scale = LEARN_RATE * lax.rsqrt(total[0:1, 0:1] / counts[0] + EPS_RMS)
    scale_o = scale
    scale_v = LEARN_RATE * lax.rsqrt(total[4:5, 0:1] / counts[1] + EPS_RMS)
    way_o, way_v = way_ref[:, :cols_o], way_ref[:, cols_o:]
    for way, local, scale, weight, step_out, new_out in (
        (way_o, local_o, scale_o, weight_o, step_o_out, new_o_out),
        (way_v, local_v, scale_v, weight_v, step_v_out, new_v_out),
    ):
        upper = way.astype(BF)
        lower = (way - upper.astype(F32)).astype(BF)
        step = (dot(local[...], upper) + dot(local[...], lower)) * scale
        step_out[...] = step
        new_out[...] = weight[...] - step
    scaled_o = (way_o * scale_o).astype(BF)
    scaled_v = (way_v * scale_v).astype(BF)
    y = y_ref[0]
    for k, ref in enumerate((b0, b1, b2, b3)):
        origin = lax.rem(y + 4 - k, 4)
        count = ref.shape[0]
        basis_o = jnp.concatenate([ref[i, :rows_o, :] for i in range(count)], 0)
        basis_v = jnp.concatenate([ref[i, rows_o:, :] for i in range(count)], 0)
        update_o = dot(basis_o, scaled_o)
        update_v = dot(basis_v, scaled_v)
        for i in range(count):
            c, x = divmod(i, count // 2)
            index = 8 * origin + 2 * x + c
            held = held_ref[index].astype(F32)
            old_o = jnp.concatenate([held[:rows_o], held[rows_o : 2 * rows_o]], 1)
            at = pl.multiple_of(index * rows_o, rows_o)
            copy_o_out[pl.ds(at, rows_o), :] = (old_o - update_o[i * rows_o : (i + 1) * rows_o]).astype(BF)
            at = pl.multiple_of(index * rows_v, rows_v)
            copy_v_out[pl.ds(at, rows_v), :] = (
                held[2 * rows_o :] - update_v[i * rows_v : (i + 1) * rows_v]
            ).astype(BF)


def outputs(counts, y, total, way, weight_o, weight_v, local_o, local_v, held, segments):
    rows_o, rows_v = local_o.shape[0], local_v.shape[0]
    fs = held.shape[0]
    shape = jax.ShapeDtypeStruct
    vmem = pl.BlockSpec(memory_space=pltpu.VMEM)
    return pl.pallas_call(
        functools.partial(output_kernel, rows_o, rows_v, counts),
        in_specs=[pl.BlockSpec(memory_space=pltpu.SMEM)] + [vmem] * 11,
        out_shape=(
            shape(weight_o.shape, F32),
            shape(weight_o.shape, F32),
            shape((rows_o * fs, weight_o.shape[1]), BF),
            shape(weight_v.shape, F32),
            shape(weight_v.shape, F32),
            shape((rows_v * fs, weight_v.shape[1]), BF),
        ),
        cost_estimate=pl.CostEstimate(flops=4 * 10**8, bytes_accessed=4 * 10**6, transcendentals=10),
        compiler_params=pltpu.CompilerParams(vmem_limit_bytes=ROOM),
        name="outputs",
    )(y, total, way, weight_o, weight_v, local_o, local_v, held, *segments)


def per_device(
    attn_out,
    out_cot,
    latent,
    value_cot,
    out_weight,
    value_up_matrix,
    out_basis,
    value_basis,
    out_mean,
    out_square,
    value_mean,
    value_square,
):
    tokens = attn_out.shape[0]
    cols_o = out_cot.shape[1]
    cols_v = value_cot.shape[1]
    rows_o, rank = out_basis.shape
    rows_v = value_basis.shape[0]
    tp = lax.axis_size(TP)
    fs = lax.axis_size(FS)
    xs, ys = lax.axis_size("x"), lax.axis_size("y")

    early_o, early_v = lax.optimization_barrier((out_weight, value_up_matrix))
    early_o, early_v = early_o.astype(BF), early_v.astype(BF)
    packed = jnp.concatenate([early_o[:, :128], early_o[:, 128:], early_v], 0)
    packed = lax.optimization_barrier(packed)
    held = lax.all_gather(packed, FS)

    block = swapped_blocks(jnp.concatenate([out_basis, value_basis], 0))

    sent = pack(attn_out, latent.T, xs)
    got = exchange(sent, "x")
    blocks = from_everyone(block, ("c", "x"))
    partial = lift(got, blocks, rows_o, tokens // xs, ys)
    partial = exchange(partial, "y")
    lifted = summed_for(partial, tp, BF)
    lifted = exchange(lifted, TP).reshape(tokens, 2 * rank)

    part_o = dot(lifted[:, :rank].T, out_cot)
    part_v = dot(lifted[:, rank:].T, value_cot)
    part = jnp.concatenate([part_o.astype(BF), part_v.astype(BF)], 1)
    near = lax.axis_size(NEAR)
    part = exchange(part.reshape(near, rank // near, -1), NEAR)
    part = exchange(summed_for(part, lax.axis_size("zh"), F32), "zh")
    proj = exchange(summed_for(part, near, BF), NEAR)

    segments = [blocks]
    for k in range(1, ys):
        segments.append(shifted(blocks, "y", k))

    mean_o, square_o, mean_v, square_v, way, total = directions(
        rows_o, tp, proj, out_mean, out_square, value_mean, value_square, segments
    )
    total = exchange(total, TP)
    counts = (rows_o * fs * cols_o * tp, rows_v * fs * cols_v * tp)
    y = lax.axis_index("y").astype(jnp.int32).reshape(1)
    step_o, new_o, copy_o, step_v, new_v, copy_v = outputs(
        counts, y, total, way, out_weight, value_up_matrix, out_basis, value_basis, held, segments
    )
    return (step_o, new_o, copy_o, mean_o, square_o, step_v, new_v, copy_v, mean_v, square_v)


def solution(mesh):
    torus = Mesh(mesh.devices.reshape(4, 4, 2, 4, 4), ALL)
    both = P(FS, TP)
    cols = P(None, TP)
    rows = P(FS, None)

    return jax.shard_map(
        per_device,
        mesh=torus,
        in_specs=(both, both, both, both, both, both, rows, rows, cols, cols, cols, cols),
        out_specs=(both, both, cols, cols, cols, both, both, cols, cols, cols),
        check_vma=False,
    )
```

```python
import functools

import jax
import jax.numpy as jnp
from jax import lax
from jax.experimental import pallas as pl
from jax.experimental.pallas import tpu as pltpu
from jax.sharding import Mesh
from jax.sharding import PartitionSpec as P


TP = ("y", "x")
FS = ("zh", "zl", "c")
NEAR = ("zl", "c")
Z = ("zh", "zl")
ALL = ("zh", "zl", "c", "y", "x")

LEARN_RATE = 0.01
MEAN_DECAY = 0.8
BETA_SQUARE = 0.9
EPS_RMS = 1e-06

BF = jnp.bfloat16
ROOM = 12 * 2**20
F32 = jnp.float32


def exchange(value, axes):
    return lax.all_to_all(value, axes, 0, 0, tiled=True)


def from_everyone(value, axes):
    devices = lax.axis_size(axes)
    return exchange(jnp.broadcast_to(value[None], (devices, *value.shape)), axes)


def swapped_blocks(value):
    pairs = []
    for j in range(16):
        for b in range(2):
            for t in range(16):
                pairs.append(((2 * j + b) * 16 + t, (2 * t + b) * 16 + j))
    return lax.ppermute(value, ALL, pairs)


def shifted(value, axis, by):
    devices = lax.axis_size(axis)
    return lax.ppermute(value, axis, [(i, (i + by) % devices) for i in range(devices)])


def dot(a, b):
    return jnp.dot(a, b, preferred_element_type=F32)


def pack_kernel(at_ref, attn_ref, lat_ref, *refs):
    outs, turned = refs[:-1], refs[-1]
    groups = len(outs)
    each = attn_ref.shape[0] // groups**2
    turned[...] = lat_ref[...].T
    for k in range(groups):
        g = lax.rem(at_ref[0] + k, groups)
        pieces = []
        for p in range(groups):
            at = pl.multiple_of((p * groups + g) * each, each)
            outs[k][p * each : (p + 1) * each, :] = attn_ref[pl.ds(at, each), :]
            pieces.append(turned[pl.ds(at, each), :])
        half = groups // 2
        for p in range(half):
            at = (groups + p) * each
            outs[k][at : at + each, :] = jnp.concatenate([pieces[p], pieces[half + p]], axis=1)


def pack(at, attn_out, lat_turned, groups):
    tokens, heads = attn_out.shape
    rows = tokens // groups
    vmem = pl.BlockSpec(memory_space=pltpu.VMEM)
    return pl.pallas_call(
        pack_kernel,
        in_specs=[pl.BlockSpec(memory_space=pltpu.SMEM), vmem, vmem],
        out_shape=tuple(jax.ShapeDtypeStruct((rows + rows // 2, heads), BF) for _ in range(groups)),
        scratch_shapes=[pltpu.VMEM(lat_turned.shape[::-1], BF)],
        cost_estimate=pl.CostEstimate(flops=10**7, bytes_accessed=10**6, transcendentals=0),
        compiler_params=pltpu.CompilerParams(vmem_limit_bytes=ROOM),
        name="pack",
    )(at, attn_out, lat_turned)


def old_kernel(weight_o, weight_v, out_ref):
    rows_o = weight_o.shape[0]
    out_ref[:rows_o] = weight_o[:, :128].astype(BF)
    out_ref[rows_o : 2 * rows_o] = weight_o[:, 128:].astype(BF)
    out_ref[2 * rows_o :] = weight_v[...].astype(BF)


def old_rows(weight_o, weight_v):
    rows = 2 * weight_o.shape[0] + weight_v.shape[0]
    return pl.pallas_call(
        old_kernel,
        out_shape=jax.ShapeDtypeStruct((rows, 128), BF),
        cost_estimate=pl.CostEstimate(flops=10**6, bytes_accessed=10**5, transcendentals=0),
        compiler_params=pltpu.CompilerParams(vmem_limit_bytes=ROOM),
        name="old",
    )(weight_o, weight_v)


def lift_kernel(rows_o, tokens, at_ref, blocks_ref, *refs):
    gots, out_ref = refs[:-1], refs[-1]
    groups = len(gots)
    rank = blocks_ref.shape[2]
    half = tokens // 2
    first = jnp.zeros((tokens, rank), F32)
    second = jnp.zeros((half, 2 * rank), F32)
    for k, got_ref in enumerate(gots):
        g = lax.rem(at_ref[0] + groups - k, groups)
        low, high = blocks_ref[g], blocks_ref[groups + g]
        basis_o = jnp.concatenate([low[:rows_o], high[:rows_o]], 0)
        basis_v = jnp.concatenate([low[rows_o:], high[rows_o:]], 0)
        none = jnp.zeros_like(basis_v)
        pair = jnp.concatenate(
            [jnp.concatenate([basis_v, none], 0), jnp.concatenate([none, basis_v], 0)], 1
        )
        first = first + dot(got_ref[:tokens, :], basis_o)
        second = second + dot(got_ref[tokens:, :], pair)
    parts, each = out_ref.shape[:2]
    for p in range(parts):
        at = p * each
        out_ref[p, :, :rank] = first[at : at + each].astype(BF)
        row, side = at % half, at // half
        out_ref[p, :, rank:] = second[row : row + each, side * rank : (side + 1) * rank].astype(BF)


def lift(at, blocks, gots, rows_o, tokens, parts):
    rank = blocks.shape[2]
    vmem = pl.BlockSpec(memory_space=pltpu.VMEM)
    return pl.pallas_call(
        functools.partial(lift_kernel, rows_o, tokens),
        in_specs=[pl.BlockSpec(memory_space=pltpu.SMEM)] + [vmem] * (1 + len(gots)),
        out_shape=jax.ShapeDtypeStruct((parts, tokens // parts, 2 * rank), BF),
        cost_estimate=pl.CostEstimate(flops=2 * 10**8, bytes_accessed=10**6, transcendentals=0),
        compiler_params=pltpu.CompilerParams(vmem_limit_bytes=ROOM),
        name="lift",
    )(at, blocks, *gots)


def spread_kernel(got_ref, out_ref):
    total = got_ref[0].astype(F32)
    for i in range(1, got_ref.shape[0]):
        total = total + got_ref[i].astype(F32)
    total = total.astype(out_ref.dtype)
    for i in range(out_ref.shape[0]):
        out_ref[i] = total


def summed_for(got, copies, kind):
    return pl.pallas_call(
        spread_kernel,
        out_shape=jax.ShapeDtypeStruct((copies, *got.shape[1:]), kind),
        cost_estimate=pl.CostEstimate(flops=10**7, bytes_accessed=10**6, transcendentals=0),
        compiler_params=pltpu.CompilerParams(vmem_limit_bytes=ROOM),
    )(got)


def decay_kernel(mean_o, square_o, mean_v, square_v, mean_out, square_out):
    cols_o = mean_o.shape[1]
    mean_out[:, :cols_o] = MEAN_DECAY * mean_o[...]
    mean_out[:, cols_o:] = MEAN_DECAY * mean_v[...]
    square_out[:, :cols_o] = BETA_SQUARE * square_o[...]
    square_out[:, cols_o:] = BETA_SQUARE * square_v[...]


def decayed(mean_o, square_o, mean_v, square_v):
    shape = jax.ShapeDtypeStruct((mean_o.shape[0], mean_o.shape[1] + mean_v.shape[1]), F32)
    return pl.pallas_call(
        decay_kernel,
        out_shape=(shape, shape),
        cost_estimate=pl.CostEstimate(flops=10**6, bytes_accessed=10**6, transcendentals=0),
        compiler_params=pltpu.CompilerParams(vmem_limit_bytes=ROOM),
        name="decay",
    )(mean_o, square_o, mean_v, square_v)


def direction_kernel(
    rows_o, cols_o, got_ref, mean_ref, square_ref, b0, b1, b2, b3,
    mean_o_out, square_o_out, mean_v_out, square_v_out, way_out, total_out,
):
    near = got_ref.shape[0]
    proj = jnp.concatenate([got_ref[i] for i in range(near)], 0).astype(F32)
    mean = mean_ref[...] + (1.0 - MEAN_DECAY) * proj
    square = square_ref[...] + (1.0 - BETA_SQUARE) * proj * proj
    mean_o_out[...] = mean[:, :cols_o]
    mean_v_out[...] = mean[:, cols_o:]
    square_o_out[...] = square[:, :cols_o]
    square_v_out[...] = square[:, cols_o:]
    way = mean / jnp.sqrt(square)
    way_out[...] = way
    upper = way.astype(BF)
    upper_o, upper_v = upper[:, :cols_o], upper[:, cols_o:]
    total_o = jnp.zeros((8, cols_o), F32)
    total_v = jnp.zeros((8, upper_v.shape[1]), F32)
    for ref in (b0, b1, b2, b3):
        count = ref.shape[0]
        basis_o = jnp.concatenate([ref[i, :rows_o, :] for i in range(count)], 0)
        basis_v = jnp.concatenate([ref[i, rows_o:, :] for i in range(count)], 0)
        update = dot(basis_o, upper_o)
        total_o = total_o + jnp.sum((update * update).reshape(-1, 8, cols_o), 0)
        update = dot(basis_v, upper_v)
        total_v = total_v + jnp.sum((update * update).reshape(-1, 8, update.shape[1]), 0)
    sums = [
        jnp.broadcast_to(jnp.sum(t, keepdims=True), (4, 128)) for t in (total_o, total_v)
    ]
    tile = jnp.concatenate(sums, 0)
    for i in range(total_out.shape[0]):
        total_out[i] = tile


def directions(rows_o, cols_o, copies, got, mean, square, segments):
    rank, cols = mean.shape
    shape = jax.ShapeDtypeStruct
    return pl.pallas_call(
        functools.partial(direction_kernel, rows_o, cols_o),
        out_shape=(
            shape((rank, cols_o), F32),
            shape((rank, cols_o), F32),
            shape((rank, cols - cols_o), F32),
            shape((rank, cols - cols_o), F32),
            shape((rank, cols), F32),
            shape((copies, 8, 128), F32),
        ),
        cost_estimate=pl.CostEstimate(flops=4 * 10**8, bytes_accessed=4 * 10**6, transcendentals=10**5),
        compiler_params=pltpu.CompilerParams(vmem_limit_bytes=ROOM),
        name="directions",
    )(got, mean, square, *segments)


def ready_kernel(
    rows_o, rows_v, cols_o, at_ref, way_ref, local_o, local_v, h0, h1, h2, h3, b0, b1, b2, b3,
    step_o_out, step_v_out, update_o_out, update_v_out, old_o_out, old_v_out,
):
    way = way_ref[...]
    upper = way.astype(BF)
    lower = (way - upper.astype(F32)).astype(BF)
    upper_o, upper_v = upper[:, :cols_o], upper[:, cols_o:]
    step_o_out[...] = dot(local_o[...], upper_o) + dot(local_o[...], lower[:, :cols_o])
    step_v_out[...] = dot(local_v[...], upper_v) + dot(local_v[...], lower[:, cols_o:])
    y, z, c = at_ref[1], at_ref[2], at_ref[3]
    for k, ref in enumerate((b0, b1, b2, b3)):
        origin = lax.rem(y + 4 - k, 4)
        count = ref.shape[0]
        basis_o = jnp.concatenate([ref[i, :rows_o, :] for i in range(count)], 0)
        basis_v = jnp.concatenate([ref[i, rows_o:, :] for i in range(count)], 0)
        update_o = dot(basis_o, upper_o).astype(BF)
        update_v = dot(basis_v, upper_v).astype(BF)
        for i in range(count):
            core, x = divmod(i, count // 2)
            index = 8 * origin + 2 * x + core
            at = pl.multiple_of(index * rows_o, rows_o)
            update_o_out[pl.ds(at, rows_o), :] = update_o[i * rows_o : (i + 1) * rows_o]
            at = pl.multiple_of(index * rows_v, rows_v)
            update_v_out[pl.ds(at, rows_v), :] = update_v[i * rows_v : (i + 1) * rows_v]
    for ref, core, last in ((h0, c, 0), (h1, c, 1), (h2, 1 - c, 0), (h3, 1 - c, 1)):
        for p in range(ref.shape[0]):
            behind = (p & 1) * 8 + (p >> 1 & 1) * 4 + (p >> 2) * 2 + last
            index = 2 * lax.rem(z + 16 - behind, 16) + core
            at = pl.multiple_of(index * rows_o, rows_o)
            old_o_out[pl.ds(at, rows_o), :128] = ref[p, :rows_o]
            old_o_out[pl.ds(at, rows_o), 128:] = ref[p, rows_o : 2 * rows_o]
            at = pl.multiple_of(index * rows_v, rows_v)
            old_v_out[pl.ds(at, rows_v), :] = ref[p, 2 * rows_o :]


def ready(cols_o, at, way, local_o, local_v, held, segments):
    rows_o, rows_v = local_o.shape[0], local_v.shape[0]
    cols_v = way.shape[1] - cols_o
    fs = 4 * held[0].shape[0]
    shape = jax.ShapeDtypeStruct
    vmem = pl.BlockSpec(memory_space=pltpu.VMEM)
    return pl.pallas_call(
        functools.partial(ready_kernel, rows_o, rows_v, cols_o),
        in_specs=[pl.BlockSpec(memory_space=pltpu.SMEM)] + [vmem] * 11,
        out_shape=(
            shape((rows_o, cols_o), F32),
            shape((rows_v, cols_v), F32),
            shape((rows_o * fs, cols_o), BF),
            shape((rows_v * fs, cols_v), BF),
            shape((rows_o * fs, cols_o), BF),
            shape((rows_v * fs, cols_v), BF),
        ),
        cost_estimate=pl.CostEstimate(flops=4 * 10**8, bytes_accessed=4 * 10**6, transcendentals=0),
        compiler_params=pltpu.CompilerParams(vmem_limit_bytes=ROOM),
        name="ready",
    )(at, way, local_o, local_v, *held, *segments)


def output_kernel(
    counts, total_ref, weight_o, weight_v, step_o, step_v, update_o, update_v, old_o, old_v,
    step_o_out, new_o_out, copy_o_out, step_v_out, new_v_out, copy_v_out,
):
    total = total_ref[0]
    for i in range(1, total_ref.shape[0]):
        total = total + total_ref[i]
    for row, count, weight, step, update, old, step_out, new_out, copy_out in (
        (0, counts[0], weight_o, step_o, update_o, old_o, step_o_out, new_o_out, copy_o_out),
        (4, counts[1], weight_v, step_v, update_v, old_v, step_v_out, new_v_out, copy_v_out),
    ):
        scale = LEARN_RATE * lax.rsqrt(total[row : row + 1, 0:1] / count + EPS_RMS)
        mine = step[...] * scale
        step_out[...] = mine
        new_out[...] = weight[...] - mine
        copy_out[...] = (old[...].astype(F32) - update[...].astype(F32) * scale).astype(BF)


def outputs(counts, total, weight_o, weight_v, step_o, step_v, update_o, update_v, old_o, old_v):
    shape = jax.ShapeDtypeStruct
    return pl.pallas_call(
        functools.partial(output_kernel, counts),
        out_shape=(
            shape(weight_o.shape, F32),
            shape(weight_o.shape, F32),
            shape(old_o.shape, BF),
            shape(weight_v.shape, F32),
            shape(weight_v.shape, F32),
            shape(old_v.shape, BF),
        ),
        cost_estimate=pl.CostEstimate(flops=10**7, bytes_accessed=4 * 10**6, transcendentals=10),
        compiler_params=pltpu.CompilerParams(vmem_limit_bytes=ROOM),
        name="outputs",
    )(total, weight_o, weight_v, step_o, step_v, update_o, update_v, old_o, old_v)


def per_device(
    attn_out,
    out_cot,
    latent,
    value_cot,
    out_weight,
    value_up_matrix,
    out_basis,
    value_basis,
    out_mean,
    out_square,
    value_mean,
    value_square,
):
    tokens = attn_out.shape[0]
    cols_o = out_cot.shape[1]
    cols_v = value_cot.shape[1]
    rows_o, rank = out_basis.shape
    rows_v = value_basis.shape[0]
    tp = lax.axis_size(TP)
    fs = lax.axis_size(FS)
    xs, ys = lax.axis_size("x"), lax.axis_size("y")

    x = lax.axis_index("x").astype(jnp.int32)
    y = lax.axis_index("y").astype(jnp.int32)
    z = lax.axis_index(Z).astype(jnp.int32)
    c = lax.axis_index("c").astype(jnp.int32)
    at = jnp.stack([x, y, z, c])

    block = swapped_blocks(jnp.concatenate([out_basis, value_basis], 0))

    gots = list(pack(at, attn_out, latent.T, xs))
    for k in range(1, xs):
        gots[k] = shifted(gots[k], "x", k)

    own = old_rows(out_weight, value_up_matrix)[None]
    for k in (8, 4, 2):
        more = shifted(own, Z, k)
        own = lax.optimization_barrier(jnp.concatenate([own, more], 0))
    more = shifted(own, Z, 1)
    held = [own, more, shifted(own, "c", 1)]
    held.append(shifted(more, "c", 1))

    blocks = from_everyone(block, ("c", "x"))
    partial = lift(at, blocks, gots, rows_o, tokens // xs, ys)
    partial = exchange(partial, "y")
    lifted = summed_for(partial, tp, BF)
    lifted = exchange(lifted, TP).reshape(tokens, 2 * rank)

    part_o = dot(lifted[:, :rank].T, out_cot)
    part_v = dot(lifted[:, rank:].T, value_cot)
    part = jnp.concatenate([part_o.astype(BF), part_v.astype(BF)], 1)
    near = lax.axis_size(NEAR)
    part = exchange(part.reshape(near, rank // near, -1), NEAR)
    part = exchange(summed_for(part, lax.axis_size("zh"), F32), "zh")
    proj = exchange(summed_for(part, near, BF), NEAR)

    segments = [blocks]
    for k in range(1, ys):
        segments.append(shifted(blocks, "y", k))

    mean, square = decayed(out_mean, out_square, value_mean, value_square)
    mean_o, square_o, mean_v, square_v, way, total = directions(
        rows_o, cols_o, tp, proj, mean, square, segments
    )
    total = exchange(total, TP)
    prepared = ready(cols_o, at, way, out_basis, value_basis, held, segments)
    counts = (rows_o * fs * cols_o * tp, rows_v * fs * cols_v * tp)
    step_o, new_o, copy_o, step_v, new_v, copy_v = outputs(
        counts, total, out_weight, value_up_matrix, *prepared
    )
    return (step_o, new_o, copy_o, mean_o, square_o, step_v, new_v, copy_v, mean_v, square_v)


def solution(mesh):
    torus = Mesh(mesh.devices.reshape(4, 4, 2, 4, 4), ALL)
    both = P(FS, TP)
    cols = P(None, TP)
    rows = P(FS, None)

    return jax.shard_map(
        per_device,
        mesh=torus,
        in_specs=(both, both, both, both, both, both, rows, rows, cols, cols, cols, cols),
        out_specs=(both, both, cols, cols, cols, both, both, cols, cols, cols),
        check_vma=False,
    )
```

```python
import functools

import jax
import jax.numpy as jnp
from jax import lax
from jax.experimental import pallas as pl
from jax.experimental.pallas import tpu as pltpu
from jax.sharding import Mesh
from jax.sharding import PartitionSpec as P


TP = ("y", "x")
FS = ("zh", "zl", "c")
NEAR = ("zl", "c")
Z = ("zh", "zl")
ALL = ("zh", "zl", "c", "y", "x")

LEARN_RATE = 0.01
MEAN_DECAY = 0.8
BETA_SQUARE = 0.9
EPS_RMS = 1e-06

BF = jnp.bfloat16
ROOM = 12 * 2**20
WHOLE = 67043328
F32 = jnp.float32


def exchange(value, axes):
    return lax.all_to_all(value, axes, 0, 0, tiled=True)


def from_everyone(value, axes):
    devices = lax.axis_size(axes)
    return exchange(jnp.broadcast_to(value[None], (devices, *value.shape)), axes)


def swapped_blocks(value):
    pairs = []
    for j in range(16):
        for b in range(2):
            for t in range(16):
                pairs.append(((2 * j + b) * 16 + t, (2 * t + b) * 16 + j))
    return lax.ppermute(value, ALL, pairs)


def shifted(value, axis, by):
    devices = lax.axis_size(axis)
    return lax.ppermute(value, axis, [(i, (i + by) % devices) for i in range(devices)])


def dot(a, b):
    return jnp.dot(a, b, preferred_element_type=F32)


def pack_kernel(at_ref, attn_ref, lat_ref, *refs):
    outs, (attn_here, lat_here, turned, sems) = refs[:-4], refs[-4:]
    groups = len(outs)
    each = attn_ref.shape[0] // groups**2
    copies = [
        pltpu.make_async_copy(lat_ref, lat_here, sems.at[0]),
        pltpu.make_async_copy(attn_ref, attn_here, sems.at[1]),
    ]
    for copy in copies:
        copy.start()
    copies[0].wait()
    turned[...] = lat_here[...].T
    copies[1].wait()
    for k in range(groups):
        g = lax.rem(at_ref[0] + k, groups)
        pieces = []
        for p in range(groups):
            at = pl.multiple_of((p * groups + g) * each, each)
            outs[k][p * each : (p + 1) * each, :] = attn_here[pl.ds(at, each), :]
            pieces.append(turned[pl.ds(at, each), :])
        half = groups // 2
        for p in range(half):
            at = (groups + p) * each
            outs[k][at : at + each, :] = jnp.concatenate([pieces[p], pieces[half + p]], axis=1)


def pack(at, attn_out, lat_turned, groups):
    tokens, heads = attn_out.shape
    rows = tokens // groups
    hbm = pl.BlockSpec(memory_space=pltpu.HBM)
    return pl.pallas_call(
        pack_kernel,
        in_specs=[pl.BlockSpec(memory_space=pltpu.SMEM), hbm, hbm],
        out_shape=tuple(jax.ShapeDtypeStruct((rows + rows // 2, heads), BF) for _ in range(groups)),
        scratch_shapes=[
            pltpu.VMEM(attn_out.shape, BF),
            pltpu.VMEM(lat_turned.shape, BF),
            pltpu.VMEM(lat_turned.shape[::-1], BF),
            pltpu.SemaphoreType.DMA((2,)),
        ],
        cost_estimate=pl.CostEstimate(flops=10**7, bytes_accessed=10**6, transcendentals=0),
        compiler_params=pltpu.CompilerParams(vmem_limit_bytes=WHOLE),
        name="pack",
    )(at, attn_out, lat_turned)


def old_kernel(weight_o, weight_v, out_ref):
    rows_o = weight_o.shape[0]
    out_ref[:rows_o] = weight_o[:, :128].astype(BF)
    out_ref[rows_o : 2 * rows_o] = weight_o[:, 128:].astype(BF)
    out_ref[2 * rows_o :] = weight_v[...].astype(BF)


def old_rows(weight_o, weight_v):
    rows = 2 * weight_o.shape[0] + weight_v.shape[0]
    return pl.pallas_call(
        old_kernel,
        out_shape=jax.ShapeDtypeStruct((rows, 128), BF),
        cost_estimate=pl.CostEstimate(flops=10**6, bytes_accessed=10**5, transcendentals=0),
        compiler_params=pltpu.CompilerParams(vmem_limit_bytes=ROOM),
        name="old",
    )(weight_o, weight_v)


def lift_kernel(rows_o, tokens, at_ref, blocks_ref, *refs):
    gots, out_ref = refs[:-1], refs[-1]
    groups = len(gots)
    rank = blocks_ref.shape[2]
    half = tokens // 2
    first = jnp.zeros((tokens, rank), F32)
    second = jnp.zeros((half, 2 * rank), F32)
    for k, got_ref in enumerate(gots):
        g = lax.rem(at_ref[0] + groups - k, groups)
        low, high = blocks_ref[g], blocks_ref[groups + g]
        basis_o = jnp.concatenate([low[:rows_o], high[:rows_o]], 0)
        basis_v = jnp.concatenate([low[rows_o:], high[rows_o:]], 0)
        none = jnp.zeros_like(basis_v)
        pair = jnp.concatenate(
            [jnp.concatenate([basis_v, none], 0), jnp.concatenate([none, basis_v], 0)], 1
        )
        first = first + dot(got_ref[:tokens, :], basis_o)
        second = second + dot(got_ref[tokens:, :], pair)
    parts, each = out_ref.shape[:2]
    for p in range(parts):
        at = p * each
        out_ref[p, :, :rank] = first[at : at + each].astype(BF)
        row, side = at % half, at // half
        out_ref[p, :, rank:] = second[row : row + each, side * rank : (side + 1) * rank].astype(BF)


def lift(at, blocks, gots, rows_o, tokens, parts):
    rank = blocks.shape[2]
    vmem = pl.BlockSpec(memory_space=pltpu.VMEM)
    return pl.pallas_call(
        functools.partial(lift_kernel, rows_o, tokens),
        in_specs=[pl.BlockSpec(memory_space=pltpu.SMEM)] + [vmem] * (1 + len(gots)),
        out_shape=jax.ShapeDtypeStruct((parts, tokens // parts, 2 * rank), BF),
        cost_estimate=pl.CostEstimate(flops=2 * 10**8, bytes_accessed=10**6, transcendentals=0),
        compiler_params=pltpu.CompilerParams(vmem_limit_bytes=ROOM),
        name="lift",
    )(at, blocks, *gots)


def spread_kernel(got_ref, out_ref):
    total = got_ref[0].astype(F32)
    for i in range(1, got_ref.shape[0]):
        total = total + got_ref[i].astype(F32)
    total = total.astype(out_ref.dtype)
    for i in range(out_ref.shape[0]):
        out_ref[i] = total


def summed_for(got, copies, kind):
    return pl.pallas_call(
        spread_kernel,
        out_shape=jax.ShapeDtypeStruct((copies, *got.shape[1:]), kind),
        cost_estimate=pl.CostEstimate(flops=10**7, bytes_accessed=10**6, transcendentals=0),
        compiler_params=pltpu.CompilerParams(vmem_limit_bytes=ROOM),
    )(got)


def contract_kernel(lifted_ref, cot_o, cot_v, out_ref, total_o, total_v):
    step = pl.program_id(0)
    rank = total_o.shape[0]
    dims = (((0,), (0,)), ((), ()))

    def term(side, cot):
        rows = lifted_ref[:, side * rank : (side + 1) * rank]
        return lax.dot_general(rows, cot[...], dims, preferred_element_type=F32)

    @pl.when(step == 0)
    def _():
        total_o[...] = term(0, cot_o)
        total_v[...] = term(1, cot_v)

    @pl.when(step > 0)
    def _():
        total_o[...] += term(0, cot_o)
        total_v[...] += term(1, cot_v)

    @pl.when(step == pl.num_programs(0) - 1)
    def _():
        cols_o = total_o.shape[1]
        parts, each, _ = out_ref.shape
        for p in range(parts):
            out_ref[p, :, :cols_o] = total_o[p * each : (p + 1) * each].astype(BF)
            out_ref[p, :, cols_o:] = total_v[p * each : (p + 1) * each].astype(BF)


def contract(lifted, cot_o, cot_v, parts, steps):
    tokens, both = lifted.shape
    rank, cols_o, cols_v = both // 2, cot_o.shape[1], cot_v.shape[1]
    rows = tokens // steps
    shape = (parts, rank // parts, cols_o + cols_v)
    return pl.pallas_call(
        contract_kernel,
        grid=(steps,),
        in_specs=[
            pl.BlockSpec((rows, both), lambda i: (i, 0)),
            pl.BlockSpec((rows, cols_o), lambda i: (i, 0)),
            pl.BlockSpec((rows, cols_v), lambda i: (i, 0)),
        ],
        out_specs=pl.BlockSpec(shape, lambda i: (0, 0, 0)),
        out_shape=jax.ShapeDtypeStruct(shape, BF),
        scratch_shapes=[pltpu.VMEM((rank, cols_o), F32), pltpu.VMEM((rank, cols_v), F32)],
        cost_estimate=pl.CostEstimate(flops=3 * 10**8, bytes_accessed=3 * 10**6, transcendentals=0),
        compiler_params=pltpu.CompilerParams(vmem_limit_bytes=ROOM),
        name="contract",
    )(lifted, cot_o, cot_v)


def direction_kernel(
    rows_o, cols_o, got_ref, mean_o, square_o, mean_v, square_v, b0, b1, b2, b3,
    mean_o_out, square_o_out, mean_v_out, square_v_out, way_out, total_out,
):
    near = got_ref.shape[0]
    proj = jnp.concatenate([got_ref[i] for i in range(near)], 0).astype(F32)
    mean = jnp.concatenate([mean_o[...], mean_v[...]], 1)
    square = jnp.concatenate([square_o[...], square_v[...]], 1)
    mean = MEAN_DECAY * mean + (1.0 - MEAN_DECAY) * proj
    square = BETA_SQUARE * square + (1.0 - BETA_SQUARE) * proj * proj
    mean_o_out[...] = mean[:, :cols_o]
    mean_v_out[...] = mean[:, cols_o:]
    square_o_out[...] = square[:, :cols_o]
    square_v_out[...] = square[:, cols_o:]
    way = mean / jnp.sqrt(square)
    way_out[...] = way
    upper = way.astype(BF)
    upper_o, upper_v = upper[:, :cols_o], upper[:, cols_o:]
    total_o = jnp.zeros((8, cols_o), F32)
    total_v = jnp.zeros((8, upper_v.shape[1]), F32)
    for ref in (b0, b1, b2, b3):
        count = ref.shape[0]
        basis_o = jnp.concatenate([ref[i, :rows_o, :] for i in range(count)], 0)
        basis_v = jnp.concatenate([ref[i, rows_o:, :] for i in range(count)], 0)
        update = dot(basis_o, upper_o)
        total_o = total_o + jnp.sum((update * update).reshape(-1, 8, cols_o), 0)
        update = dot(basis_v, upper_v)
        total_v = total_v + jnp.sum((update * update).reshape(-1, 8, update.shape[1]), 0)
    sums = [
        jnp.broadcast_to(jnp.sum(t, keepdims=True), (4, 128)) for t in (total_o, total_v)
    ]
    tile = jnp.concatenate(sums, 0)
    for i in range(total_out.shape[0]):
        total_out[i] = tile


def directions(rows_o, copies, got, mean_o, square_o, mean_v, square_v, segments):
    rank, cols_o = mean_o.shape
    cols = cols_o + mean_v.shape[1]
    shape = jax.ShapeDtypeStruct
    return pl.pallas_call(
        functools.partial(direction_kernel, rows_o, cols_o),
        out_shape=(
            shape(mean_o.shape, F32),
            shape(mean_o.shape, F32),
            shape(mean_v.shape, F32),
            shape(mean_v.shape, F32),
            shape((rank, cols), F32),
            shape((copies, 8, 128), F32),
        ),
        cost_estimate=pl.CostEstimate(flops=4 * 10**8, bytes_accessed=4 * 10**6, transcendentals=10**5),
        compiler_params=pltpu.CompilerParams(vmem_limit_bytes=ROOM),
        name="directions",
    )(got, mean_o, square_o, mean_v, square_v, *segments)


def ready_kernel(
    rows_o, rows_v, cols_o, at_ref, way_ref, local_o, local_v, h0, h1, h2, h3, b0, b1, b2, b3,
    step_o_out, step_v_out, update_o_out, update_v_out, old_o_out, old_v_out,
):
    way = way_ref[...]
    upper = way.astype(BF)
    lower = (way - upper.astype(F32)).astype(BF)
    upper_o, upper_v = upper[:, :cols_o], upper[:, cols_o:]
    step_o_out[...] = dot(local_o[...], upper_o) + dot(local_o[...], lower[:, :cols_o])
    step_v_out[...] = dot(local_v[...], upper_v) + dot(local_v[...], lower[:, cols_o:])
    y, z, c = at_ref[1], at_ref[2], at_ref[3]
    for k, ref in enumerate((b0, b1, b2, b3)):
        origin = lax.rem(y + 4 - k, 4)
        count = ref.shape[0]
        basis_o = jnp.concatenate([ref[i, :rows_o, :] for i in range(count)], 0)
        basis_v = jnp.concatenate([ref[i, rows_o:, :] for i in range(count)], 0)
        update_o = dot(basis_o, upper_o).astype(BF)
        update_v = dot(basis_v, upper_v).astype(BF)
        for i in range(count):
            core, x = divmod(i, count // 2)
            index = 8 * origin + 2 * x + core
            at = pl.multiple_of(index * rows_o, rows_o)
            update_o_out[pl.ds(at, rows_o), :] = update_o[i * rows_o : (i + 1) * rows_o]
            at = pl.multiple_of(index * rows_v, rows_v)
            update_v_out[pl.ds(at, rows_v), :] = update_v[i * rows_v : (i + 1) * rows_v]
    for ref, core, last in ((h0, c, 0), (h1, c, 1), (h2, 1 - c, 0), (h3, 1 - c, 1)):
        for p in range(ref.shape[0]):
            behind = (p & 1) * 8 + (p >> 1 & 1) * 4 + (p >> 2) * 2 + last
            index = 2 * lax.rem(z + 16 - behind, 16) + core
            at = pl.multiple_of(index * rows_o, rows_o)
            old_o_out[pl.ds(at, rows_o), :128] = ref[p, :rows_o]
            old_o_out[pl.ds(at, rows_o), 128:] = ref[p, rows_o : 2 * rows_o]
            at = pl.multiple_of(index * rows_v, rows_v)
            old_v_out[pl.ds(at, rows_v), :] = ref[p, 2 * rows_o :]


def ready(cols_o, at, way, local_o, local_v, held, segments):
    rows_o, rows_v = local_o.shape[0], local_v.shape[0]
    cols_v = way.shape[1] - cols_o
    fs = 4 * held[0].shape[0]
    shape = jax.ShapeDtypeStruct
    vmem = pl.BlockSpec(memory_space=pltpu.VMEM)
    return pl.pallas_call(
        functools.partial(ready_kernel, rows_o, rows_v, cols_o),
        in_specs=[pl.BlockSpec(memory_space=pltpu.SMEM)] + [vmem] * 11,
        out_shape=(
            shape((rows_o, cols_o), F32),
            shape((rows_v, cols_v), F32),
            shape((rows_o * fs, cols_o), BF),
            shape((rows_v * fs, cols_v), BF),
            shape((rows_o * fs, cols_o), BF),
            shape((rows_v * fs, cols_v), BF),
        ),
        cost_estimate=pl.CostEstimate(flops=4 * 10**8, bytes_accessed=4 * 10**6, transcendentals=0),
        compiler_params=pltpu.CompilerParams(vmem_limit_bytes=WHOLE),
        name="ready",
    )(at, way, local_o, local_v, *held, *segments)


def output_kernel(
    counts, pieces, total_ref, weight_o, weight_v, step_o, step_v, update_o, update_v, old_o, old_v,
    step_o_out, new_o_out, copy_o_out, step_v_out, new_v_out, copy_v_out,
    update_o_here, update_v_here, old_o_here, old_v_here, sems,
):
    copies = []
    for n, (source, here) in enumerate(
        ((update_o, update_o_here), (old_o, old_o_here), (update_v, update_v_here), (old_v, old_v_here))
    ):
        rows = source.shape[0] // pieces
        for p in range(pieces):
            part = pl.ds(p * rows, rows)
            copies.append(pltpu.make_async_copy(source.at[part], here.at[part], sems.at[n, p]))
    for copy in copies:
        copy.start()
    total = total_ref[0]
    for i in range(1, total_ref.shape[0]):
        total = total + total_ref[i]
    scales = []
    for row, count, weight, step, step_out, new_out in (
        (0, counts[0], weight_o, step_o, step_o_out, new_o_out),
        (4, counts[1], weight_v, step_v, step_v_out, new_v_out),
    ):
        scale = LEARN_RATE * lax.rsqrt(total[row : row + 1, 0:1] / count + EPS_RMS)
        mine = step[...] * scale
        step_out[...] = mine
        new_out[...] = weight[...] - mine
        scales.append(scale)
    for n, (scale, update, old, copy_out) in enumerate(
        (
            (scales[0], update_o_here, old_o_here, copy_o_out),
            (scales[1], update_v_here, old_v_here, copy_v_out),
        )
    ):
        rows = old.shape[0] // pieces
        for p in range(pieces):
            copies[2 * n * pieces + p].wait()
            copies[(2 * n + 1) * pieces + p].wait()
            part = pl.ds(p * rows, rows)
            copy_out[part, :] = (old[part, :].astype(F32) - update[part, :].astype(F32) * scale).astype(BF)


def outputs(counts, total, weight_o, weight_v, step_o, step_v, update_o, update_v, old_o, old_v):
    shape = jax.ShapeDtypeStruct
    vmem = pl.BlockSpec(memory_space=pltpu.VMEM)
    hbm = pl.BlockSpec(memory_space=pltpu.HBM)
    pieces = 4
    return pl.pallas_call(
        functools.partial(output_kernel, counts, pieces),
        in_specs=[vmem] * 5 + [hbm] * 4,
        out_shape=(
            shape(weight_o.shape, F32),
            shape(weight_o.shape, F32),
            shape(old_o.shape, BF),
            shape(weight_v.shape, F32),
            shape(weight_v.shape, F32),
            shape(old_v.shape, BF),
        ),
        scratch_shapes=[pltpu.VMEM(a.shape, BF) for a in (update_o, update_v, old_o, old_v)]
        + [pltpu.SemaphoreType.DMA((4, pieces))],
        cost_estimate=pl.CostEstimate(flops=10**7, bytes_accessed=4 * 10**6, transcendentals=10),
        compiler_params=pltpu.CompilerParams(vmem_limit_bytes=WHOLE),
        name="outputs",
    )(total, weight_o, weight_v, step_o, step_v, update_o, update_v, old_o, old_v)


def per_device(
    attn_out,
    out_cot,
    latent,
    value_cot,
    out_weight,
    value_up_matrix,
    out_basis,
    value_basis,
    out_mean,
    out_square,
    value_mean,
    value_square,
):
    tokens = attn_out.shape[0]
    cols_o = out_cot.shape[1]
    cols_v = value_cot.shape[1]
    rows_o, rank = out_basis.shape
    rows_v = value_basis.shape[0]
    tp = lax.axis_size(TP)
    fs = lax.axis_size(FS)
    xs, ys = lax.axis_size("x"), lax.axis_size("y")

    x = lax.axis_index("x").astype(jnp.int32)
    y = lax.axis_index("y").astype(jnp.int32)
    z = lax.axis_index(Z).astype(jnp.int32)
    c = lax.axis_index("c").astype(jnp.int32)
    at = jnp.stack([x, y, z, c])

    block = swapped_blocks(jnp.concatenate([out_basis, value_basis], 0))

    gots = list(pack(at, attn_out, latent.T, xs))
    for k in range(1, xs):
        gots[k] = shifted(gots[k], "x", k)

    own = old_rows(out_weight, value_up_matrix)[None]
    for k in (8, 4, 2):
        more = shifted(own, Z, k)
        own = lax.optimization_barrier(jnp.concatenate([own, more], 0))
    more = shifted(own, Z, 1)
    held = [own, more, shifted(own, "c", 1)]
    held.append(shifted(more, "c", 1))

    blocks = from_everyone(block, ("c", "x"))
    partial = lift(at, blocks, gots, rows_o, tokens // xs, ys)
    partial = exchange(partial, "y")
    lifted = summed_for(partial, tp, BF)
    lifted = exchange(lifted, TP).reshape(tokens, 2 * rank)

    near = lax.axis_size(NEAR)
    part = contract(lifted, out_cot, value_cot, near, 4)
    part = exchange(part, NEAR)
    part = exchange(summed_for(part, lax.axis_size("zh"), F32), "zh")
    proj = exchange(summed_for(part, near, BF), NEAR)

    segments = [blocks]
    for k in range(1, ys):
        segments.append(shifted(blocks, "y", k))

    mean_o, square_o, mean_v, square_v, way, total = directions(
        rows_o, tp, proj, out_mean, out_square, value_mean, value_square, segments
    )
    total = exchange(total, TP)
    prepared = ready(cols_o, at, way, out_basis, value_basis, held, segments)
    counts = (rows_o * fs * cols_o * tp, rows_v * fs * cols_v * tp)
    step_o, new_o, copy_o, step_v, new_v, copy_v = outputs(
        counts, total, out_weight, value_up_matrix, *prepared
    )
    return (step_o, new_o, copy_o, mean_o, square_o, step_v, new_v, copy_v, mean_v, square_v)


def solution(mesh):
    torus = Mesh(mesh.devices.reshape(4, 4, 2, 4, 4), ALL)
    both = P(FS, TP)
    cols = P(None, TP)
    rows = P(FS, None)

    return jax.shard_map(
        per_device,
        mesh=torus,
        in_specs=(both, both, both, both, both, both, rows, rows, cols, cols, cols, cols),
        out_specs=(both, both, cols, cols, cols, both, both, cols, cols, cols),
        check_vma=False,
    )
```

```python
import functools

import jax
import jax.numpy as jnp
from jax import lax
from jax.experimental import pallas as pl
from jax.experimental.pallas import tpu as pltpu
from jax.sharding import Mesh
from jax.sharding import PartitionSpec as P


TP = ("y", "x")
FS = ("zh", "zl", "c")
NEAR = ("zl", "c")
Z = ("zh", "zl")
ALL = ("zh", "zl", "c", "y", "x")

LEARN_RATE = 0.01
MEAN_DECAY = 0.8
BETA_SQUARE = 0.9
EPS_RMS = 1e-06

BF = jnp.bfloat16
ROOM = 12 * 2**20
WHOLE = 67043328
STEPS = (0, 1, 2, -1)
F32 = jnp.float32


def exchange(value, axes):
    return lax.all_to_all(value, axes, 0, 0, tiled=True)


def from_everyone(value, axes):
    devices = lax.axis_size(axes)
    return exchange(jnp.broadcast_to(value[None], (devices, *value.shape)), axes)


def swapped_blocks(value):
    pairs = []
    for j in range(16):
        for b in range(2):
            for t in range(16):
                pairs.append(((2 * j + b) * 16 + t, (2 * t + b) * 16 + j))
    return lax.ppermute(value, ALL, pairs)


def shifted(value, axis, by):
    devices = lax.axis_size(axis)
    return lax.ppermute(value, axis, [(i, (i + by) % devices) for i in range(devices)])


def dot(a, b):
    return jnp.dot(a, b, preferred_element_type=F32)


def pack_kernel( attn_ref, lat_ref, *refs):
    outs, (attn_here, lat_here, turned, sems) = refs[:-4], refs[-4:]
    groups = len(outs)
    each = attn_ref.shape[0] // groups**2
    copies = [
        pltpu.make_async_copy(lat_ref, lat_here, sems.at[0]),
        pltpu.make_async_copy(attn_ref, attn_here, sems.at[1]),
    ]
    for copy in copies:
        copy.start()
    copies[0].wait()
    turned[...] = lat_here[...].T
    copies[1].wait()
    for k in range(groups):
        g = lax.rem(lax.axis_index("x") + k, groups)
        pieces = []
        for p in range(groups):
            at = pl.multiple_of((p * groups + g) * each, each)
            outs[k][p * each : (p + 1) * each, :] = attn_here[pl.ds(at, each), :]
            pieces.append(turned[pl.ds(at, each), :])
        half = groups // 2
        for p in range(half):
            at = (groups + p) * each
            outs[k][at : at + each, :] = jnp.concatenate([pieces[p], pieces[half + p]], axis=1)


def pack(attn_out, lat_turned, groups):
    tokens, heads = attn_out.shape
    rows = tokens // groups
    hbm = pl.BlockSpec(memory_space=pltpu.HBM)
    return pl.pallas_call(
        pack_kernel,
        in_specs=[hbm, hbm],
        out_shape=tuple(jax.ShapeDtypeStruct((rows + rows // 2, heads), BF) for _ in range(groups)),
        scratch_shapes=[
            pltpu.VMEM(attn_out.shape, BF),
            pltpu.VMEM(lat_turned.shape, BF),
            pltpu.VMEM(lat_turned.shape[::-1], BF),
            pltpu.SemaphoreType.DMA((2,)),
        ],
        cost_estimate=pl.CostEstimate(flops=10**7, bytes_accessed=10**6, transcendentals=0),
        compiler_params=pltpu.CompilerParams(vmem_limit_bytes=WHOLE),
        name="pack",
    )(attn_out, lat_turned)


def old_kernel(weight_o, weight_v, out_ref):
    rows_o = weight_o.shape[0]
    out_ref[:rows_o] = weight_o[:, :128].astype(BF)
    out_ref[rows_o : 2 * rows_o] = weight_o[:, 128:].astype(BF)
    out_ref[2 * rows_o :] = weight_v[...].astype(BF)


def old_rows(weight_o, weight_v):
    rows = 2 * weight_o.shape[0] + weight_v.shape[0]
    return pl.pallas_call(
        old_kernel,
        out_shape=jax.ShapeDtypeStruct((rows, 128), BF),
        cost_estimate=pl.CostEstimate(flops=10**6, bytes_accessed=10**5, transcendentals=0),
        compiler_params=pltpu.CompilerParams(vmem_limit_bytes=ROOM),
        name="old",
    )(weight_o, weight_v)


def lift_kernel(rows_o, tokens, blocks_ref, *refs):
    gots, out_ref = refs[:-1], refs[-1]
    groups = len(gots)
    rank = blocks_ref.shape[2]
    half = tokens // 2
    first = jnp.zeros((tokens, rank), F32)
    second = jnp.zeros((half, 2 * rank), F32)
    for k, got_ref in enumerate(gots):
        g = lax.rem(lax.axis_index("x") + groups - k, groups)
        low, high = blocks_ref[g], blocks_ref[groups + g]
        basis_o = jnp.concatenate([low[:rows_o], high[:rows_o]], 0)
        basis_v = jnp.concatenate([low[rows_o:], high[rows_o:]], 0)
        none = jnp.zeros_like(basis_v)
        pair = jnp.concatenate(
            [jnp.concatenate([basis_v, none], 0), jnp.concatenate([none, basis_v], 0)], 1
        )
        first = first + dot(got_ref[:tokens, :], basis_o)
        second = second + dot(got_ref[tokens:, :], pair)
    parts, each = out_ref.shape[:2]
    for p in range(parts):
        at = p * each
        out_ref[p, :, :rank] = first[at : at + each].astype(BF)
        row, side = at % half, at // half
        out_ref[p, :, rank:] = second[row : row + each, side * rank : (side + 1) * rank].astype(BF)


def lift(blocks, gots, rows_o, tokens, parts):
    rank = blocks.shape[2]
    return pl.pallas_call(
        functools.partial(lift_kernel, rows_o, tokens),
        out_shape=jax.ShapeDtypeStruct((parts, tokens // parts, 2 * rank), BF),
        cost_estimate=pl.CostEstimate(flops=2 * 10**8, bytes_accessed=10**6, transcendentals=0),
        compiler_params=pltpu.CompilerParams(vmem_limit_bytes=ROOM),
        name="lift",
    )(blocks, *gots)


def spread_kernel(got_ref, out_ref):
    total = got_ref[0].astype(F32)
    for i in range(1, got_ref.shape[0]):
        total = total + got_ref[i].astype(F32)
    total = total.astype(out_ref.dtype)
    for i in range(out_ref.shape[0]):
        out_ref[i] = total


def summed_for(got, copies, kind):
    return pl.pallas_call(
        spread_kernel,
        out_shape=jax.ShapeDtypeStruct((copies, *got.shape[1:]), kind),
        cost_estimate=pl.CostEstimate(flops=10**7, bytes_accessed=10**6, transcendentals=0),
        compiler_params=pltpu.CompilerParams(vmem_limit_bytes=ROOM),
    )(got)


def contract_kernel(lifted_ref, cot_o, cot_v, out_ref, total_o, total_v):
    step = pl.program_id(0)
    rank = total_o.shape[0]
    dims = (((0,), (0,)), ((), ()))

    def term(side, cot):
        rows = lifted_ref[:, side * rank : (side + 1) * rank]
        return lax.dot_general(rows, cot[...], dims, preferred_element_type=F32)

    @pl.when(step == 0)
    def _():
        total_o[...] = term(0, cot_o)
        total_v[...] = term(1, cot_v)

    @pl.when(step > 0)
    def _():
        total_o[...] += term(0, cot_o)
        total_v[...] += term(1, cot_v)

    @pl.when(step == pl.num_programs(0) - 1)
    def _():
        cols_o = total_o.shape[1]
        parts, each, _ = out_ref.shape
        for p in range(parts):
            out_ref[p, :, :cols_o] = total_o[p * each : (p + 1) * each].astype(BF)
            out_ref[p, :, cols_o:] = total_v[p * each : (p + 1) * each].astype(BF)


def contract(lifted, cot_o, cot_v, parts, steps):
    tokens, both = lifted.shape
    rank, cols_o, cols_v = both // 2, cot_o.shape[1], cot_v.shape[1]
    rows = tokens // steps
    shape = (parts, rank // parts, cols_o + cols_v)
    return pl.pallas_call(
        contract_kernel,
        grid=(steps,),
        in_specs=[
            pl.BlockSpec((rows, both), lambda i: (i, 0)),
            pl.BlockSpec((rows, cols_o), lambda i: (i, 0)),
            pl.BlockSpec((rows, cols_v), lambda i: (i, 0)),
        ],
        out_specs=pl.BlockSpec(shape, lambda i: (0, 0, 0)),
        out_shape=jax.ShapeDtypeStruct(shape, BF),
        scratch_shapes=[pltpu.VMEM((rank, cols_o), F32), pltpu.VMEM((rank, cols_v), F32)],
        cost_estimate=pl.CostEstimate(flops=3 * 10**8, bytes_accessed=3 * 10**6, transcendentals=0),
        compiler_params=pltpu.CompilerParams(vmem_limit_bytes=ROOM),
        name="contract",
    )(lifted, cot_o, cot_v)


def direction_kernel(
    rows_o, cols_o, got_ref, mean_o, square_o, mean_v, square_v, b0, b1, b2, b3,
    mean_o_out, square_o_out, mean_v_out, square_v_out, way_out, total_out,
):
    near = got_ref.shape[0]
    proj = jnp.concatenate([got_ref[i] for i in range(near)], 0).astype(F32)
    mean = jnp.concatenate([mean_o[...], mean_v[...]], 1)
    square = jnp.concatenate([square_o[...], square_v[...]], 1)
    mean = MEAN_DECAY * mean + (1.0 - MEAN_DECAY) * proj
    square = BETA_SQUARE * square + (1.0 - BETA_SQUARE) * proj * proj
    mean_o_out[...] = mean[:, :cols_o]
    mean_v_out[...] = mean[:, cols_o:]
    square_o_out[...] = square[:, :cols_o]
    square_v_out[...] = square[:, cols_o:]
    way = mean / jnp.sqrt(square)
    way_out[...] = way
    upper = way.astype(BF)
    upper_o, upper_v = upper[:, :cols_o], upper[:, cols_o:]
    total_o = jnp.zeros((8, cols_o), F32)
    total_v = jnp.zeros((8, upper_v.shape[1]), F32)
    for ref in (b0, b1, b2, b3):
        count = ref.shape[0]
        basis_o = jnp.concatenate([ref[i, :rows_o, :] for i in range(count)], 0)
        basis_v = jnp.concatenate([ref[i, rows_o:, :] for i in range(count)], 0)
        update = dot(basis_o, upper_o)
        total_o = total_o + jnp.sum((update * update).reshape(-1, 8, cols_o), 0)
        update = dot(basis_v, upper_v)
        total_v = total_v + jnp.sum((update * update).reshape(-1, 8, update.shape[1]), 0)
    sums = [
        jnp.broadcast_to(jnp.sum(t, keepdims=True), (4, 128)) for t in (total_o, total_v)
    ]
    tile = jnp.concatenate(sums, 0)
    for i in range(total_out.shape[0]):
        total_out[i] = tile


def directions(rows_o, copies, got, mean_o, square_o, mean_v, square_v, segments):
    rank, cols_o = mean_o.shape
    cols = cols_o + mean_v.shape[1]
    shape = jax.ShapeDtypeStruct
    return pl.pallas_call(
        functools.partial(direction_kernel, rows_o, cols_o),
        out_shape=(
            shape(mean_o.shape, F32),
            shape(mean_o.shape, F32),
            shape(mean_v.shape, F32),
            shape(mean_v.shape, F32),
            shape((rank, cols), F32),
            shape((copies, 8, 128), F32),
        ),
        cost_estimate=pl.CostEstimate(flops=4 * 10**8, bytes_accessed=4 * 10**6, transcendentals=10**5),
        compiler_params=pltpu.CompilerParams(vmem_limit_bytes=ROOM),
        name="directions",
    )(got, mean_o, square_o, mean_v, square_v, *segments)


def ready_kernel(
    rows_o, rows_v, cols_o, way_ref, local_o, local_v, own_ref, other_ref, b0, b1, b2, b3,
    step_o_out, step_v_out, update_o_out, update_v_out, old_o_out, old_v_out,
):
    way = way_ref[...]
    upper = way.astype(BF)
    lower = (way - upper.astype(F32)).astype(BF)
    upper_o, upper_v = upper[:, :cols_o], upper[:, cols_o:]
    step_o_out[...] = dot(local_o[...], upper_o) + dot(local_o[...], lower[:, :cols_o])
    step_v_out[...] = dot(local_v[...], upper_v) + dot(local_v[...], lower[:, cols_o:])
    y, c = lax.axis_index("y"), lax.axis_index("c")
    z = 4 * lax.axis_index("zh") + lax.axis_index("zl")
    for k, ref in enumerate((b0, b1, b2, b3)):
        origin = lax.rem(y + 4 - k, 4)
        count = ref.shape[0]
        basis_o = jnp.concatenate([ref[i, :rows_o, :] for i in range(count)], 0)
        basis_v = jnp.concatenate([ref[i, rows_o:, :] for i in range(count)], 0)
        update_o = dot(basis_o, upper_o).astype(BF)
        update_v = dot(basis_v, upper_v).astype(BF)
        for i in range(count):
            core, x = divmod(i, count // 2)
            index = 8 * origin + 2 * x + core
            at = pl.multiple_of(index * rows_o, rows_o)
            update_o_out[pl.ds(at, rows_o), :] = update_o[i * rows_o : (i + 1) * rows_o]
            at = pl.multiple_of(index * rows_v, rows_v)
            update_v_out[pl.ds(at, rows_v), :] = update_v[i * rows_v : (i + 1) * rows_v]
    for ref, core in ((own_ref, c), (other_ref, 1 - c)):
        for p in range(ref.shape[0]):
            behind = (p & 1) * 8 + (p >> 1 & 1) * 4 + STEPS[p >> 2]
            index = 2 * lax.rem(z + 16 - behind, 16) + core
            at = pl.multiple_of(index * rows_o, rows_o)
            old_o_out[pl.ds(at, rows_o), :128] = ref[p, :rows_o]
            old_o_out[pl.ds(at, rows_o), 128:] = ref[p, rows_o : 2 * rows_o]
            at = pl.multiple_of(index * rows_v, rows_v)
            old_v_out[pl.ds(at, rows_v), :] = ref[p, 2 * rows_o :]


def ready(cols_o, way, local_o, local_v, own, other, segments):
    rows_o, rows_v = local_o.shape[0], local_v.shape[0]
    cols_v = way.shape[1] - cols_o
    fs = 2 * own.shape[0]
    shape = jax.ShapeDtypeStruct
    return pl.pallas_call(
        functools.partial(ready_kernel, rows_o, rows_v, cols_o),
        out_shape=(
            shape((rows_o, cols_o), F32),
            shape((rows_v, cols_v), F32),
            shape((rows_o * fs, cols_o), BF),
            shape((rows_v * fs, cols_v), BF),
            shape((rows_o * fs, cols_o), BF),
            shape((rows_v * fs, cols_v), BF),
        ),
        cost_estimate=pl.CostEstimate(flops=4 * 10**8, bytes_accessed=4 * 10**6, transcendentals=0),
        compiler_params=pltpu.CompilerParams(vmem_limit_bytes=WHOLE),
        name="ready",
    )(way, local_o, local_v, own, other, *segments)


def output_kernel(
    counts, pieces, total_ref, weight_o, weight_v, step_o, step_v, update_o, update_v, old_o, old_v,
    step_o_out, new_o_out, copy_o_out, step_v_out, new_v_out, copy_v_out,
    update_o_here, update_v_here, old_o_here, old_v_here, sems,
):
    copies = []
    for n, (source, here) in enumerate(
        ((update_o, update_o_here), (old_o, old_o_here), (update_v, update_v_here), (old_v, old_v_here))
    ):
        rows = source.shape[0] // pieces
        for p in range(pieces):
            part = pl.ds(p * rows, rows)
            copies.append(pltpu.make_async_copy(source.at[part], here.at[part], sems.at[n, p]))
    for copy in copies:
        copy.start()
    total = total_ref[0]
    for i in range(1, total_ref.shape[0]):
        total = total + total_ref[i]
    scales = []
    for row, count, weight, step, step_out, new_out in (
        (0, counts[0], weight_o, step_o, step_o_out, new_o_out),
        (4, counts[1], weight_v, step_v, step_v_out, new_v_out),
    ):
        scale = LEARN_RATE * lax.rsqrt(total[row : row + 1, 0:1] / count + EPS_RMS)
        mine = step[...] * scale
        step_out[...] = mine
        new_out[...] = weight[...] - mine
        scales.append(scale)
    for n, (scale, update, old, copy_out) in enumerate(
        (
            (scales[0], update_o_here, old_o_here, copy_o_out),
            (scales[1], update_v_here, old_v_here, copy_v_out),
        )
    ):
        rows = old.shape[0] // pieces
        for p in range(pieces):
            copies[2 * n * pieces + p].wait()
            copies[(2 * n + 1) * pieces + p].wait()
            part = pl.ds(p * rows, rows)
            copy_out[part, :] = (old[part, :].astype(F32) - update[part, :].astype(F32) * scale).astype(BF)


def outputs(counts, total, weight_o, weight_v, step_o, step_v, update_o, update_v, old_o, old_v):
    shape = jax.ShapeDtypeStruct
    vmem = pl.BlockSpec(memory_space=pltpu.VMEM)
    hbm = pl.BlockSpec(memory_space=pltpu.HBM)
    pieces = 4
    return pl.pallas_call(
        functools.partial(output_kernel, counts, pieces),
        in_specs=[vmem] * 5 + [hbm] * 4,
        out_shape=(
            shape(weight_o.shape, F32),
            shape(weight_o.shape, F32),
            shape(old_o.shape, BF),
            shape(weight_v.shape, F32),
            shape(weight_v.shape, F32),
            shape(old_v.shape, BF),
        ),
        scratch_shapes=[pltpu.VMEM(a.shape, BF) for a in (update_o, update_v, old_o, old_v)]
        + [pltpu.SemaphoreType.DMA((4, pieces))],
        cost_estimate=pl.CostEstimate(flops=10**7, bytes_accessed=4 * 10**6, transcendentals=10),
        compiler_params=pltpu.CompilerParams(vmem_limit_bytes=WHOLE),
        name="outputs",
    )(total, weight_o, weight_v, step_o, step_v, update_o, update_v, old_o, old_v)


def per_device(
    attn_out,
    out_cot,
    latent,
    value_cot,
    out_weight,
    value_up_matrix,
    out_basis,
    value_basis,
    out_mean,
    out_square,
    value_mean,
    value_square,
):
    tokens = attn_out.shape[0]
    cols_o = out_cot.shape[1]
    cols_v = value_cot.shape[1]
    rows_o, rank = out_basis.shape
    rows_v = value_basis.shape[0]
    tp = lax.axis_size(TP)
    fs = lax.axis_size(FS)
    xs, ys = lax.axis_size("x"), lax.axis_size("y")


    block = swapped_blocks(jnp.concatenate([out_basis, value_basis], 0))

    gots = list(pack(attn_out, latent.T, xs))
    for k in range(1, xs):
        gots[k] = shifted(gots[k], "x", k)

    own = old_rows(out_weight, value_up_matrix)[None]
    for k in (8, 4):
        more = shifted(own, Z, k)
        own = lax.optimization_barrier(jnp.concatenate([own, more], 0))
    rows = [own]
    for k in STEPS[1:]:
        rows.append(shifted(own, Z, k))
    own = lax.optimization_barrier(jnp.concatenate(rows, 0))
    other = shifted(own, "c", 1)

    blocks = from_everyone(block, ("c", "x"))
    partial = lift(blocks, gots, rows_o, tokens // xs, ys)
    partial = exchange(partial, "y")
    lifted = summed_for(partial, tp, BF)
    lifted = exchange(lifted, TP).reshape(tokens, 2 * rank)

    near = lax.axis_size(NEAR)
    part = contract(lifted, out_cot, value_cot, near, 4)
    part = exchange(part, NEAR)
    part = exchange(summed_for(part, lax.axis_size("zh"), BF), "zh")
    proj = exchange(summed_for(part, near, BF), NEAR)

    segments = [blocks]
    for k in range(1, ys):
        segments.append(shifted(blocks, "y", k))

    mean_o, square_o, mean_v, square_v, way, total = directions(
        rows_o, tp, proj, out_mean, out_square, value_mean, value_square, segments
    )
    total = exchange(total, TP)
    prepared = ready(cols_o, way, out_basis, value_basis, own, other, segments)
    counts = (rows_o * fs * cols_o * tp, rows_v * fs * cols_v * tp)
    step_o, new_o, copy_o, step_v, new_v, copy_v = outputs(
        counts, total, out_weight, value_up_matrix, *prepared
    )
    return (step_o, new_o, copy_o, mean_o, square_o, step_v, new_v, copy_v, mean_v, square_v)


def solution(mesh):
    torus = Mesh(mesh.devices.reshape(4, 4, 2, 4, 4), ALL)
    both = P(FS, TP)
    cols = P(None, TP)
    rows = P(FS, None)

    return jax.shard_map(
        per_device,
        mesh=torus,
        in_specs=(both, both, both, both, both, both, rows, rows, cols, cols, cols, cols),
        out_specs=(both, both, cols, cols, cols, both, both, cols, cols, cols),
        check_vma=False,
    )
```

```python
import functools

import jax
import jax.numpy as jnp
from jax import lax
from jax.experimental import pallas as pl
from jax.experimental.pallas import tpu as pltpu
from jax.sharding import Mesh
from jax.sharding import PartitionSpec as P


TP = ("y", "x")
FS = ("zh", "zl", "c")
NEAR = ("zl", "c")
Z = ("zh", "zl")
ALL = ("zh", "zl", "c", "y", "x")

LEARN_RATE = 0.01
MEAN_DECAY = 0.8
BETA_SQUARE = 0.9
EPS_RMS = 1e-06

BF = jnp.bfloat16
ROOM = 12 * 2**20
WHOLE = 67043328
STEPS = (0, 1, 2, -1)
F32 = jnp.float32


def exchange(value, axes):
    return lax.all_to_all(value, axes, 0, 0, tiled=True)


def from_everyone(value, axes):
    devices = lax.axis_size(axes)
    return exchange(jnp.broadcast_to(value[None], (devices, *value.shape)), axes)


def swapped_blocks(value):
    pairs = []
    for j in range(16):
        for b in range(2):
            for t in range(16):
                pairs.append(((2 * j + b) * 16 + t, (2 * t + b) * 16 + j))
    return lax.ppermute(value, ALL, pairs)


def shifted(value, axis, by):
    devices = lax.axis_size(axis)
    return lax.ppermute(value, axis, [(i, (i + by) % devices) for i in range(devices)])


def dot(a, b):
    return jnp.dot(a, b, preferred_element_type=F32)


def pack_kernel( attn_ref, lat_ref, *refs):
    outs, (attn_here, lat_here, turned, sems) = refs[:-4], refs[-4:]
    groups = len(outs)
    each = attn_ref.shape[0] // groups**2
    copies = [
        pltpu.make_async_copy(lat_ref, lat_here, sems.at[0]),
        pltpu.make_async_copy(attn_ref, attn_here, sems.at[1]),
    ]
    for copy in copies:
        copy.start()
    copies[0].wait()
    turned[...] = lat_here[...].T
    copies[1].wait()
    for k in range(groups):
        g = lax.rem(lax.axis_index("x") + k, groups)
        pieces = []
        for p in range(groups):
            at = pl.multiple_of((p * groups + g) * each, each)
            outs[k][p * each : (p + 1) * each, :] = attn_here[pl.ds(at, each), :]
            pieces.append(turned[pl.ds(at, each), :])
        half = groups // 2
        for p in range(half):
            at = (groups + p) * each
            outs[k][at : at + each, :] = jnp.concatenate([pieces[p], pieces[half + p]], axis=1)


def pack(attn_out, lat_turned, groups):
    tokens, heads = attn_out.shape
    rows = tokens // groups
    hbm = pl.BlockSpec(memory_space=pltpu.HBM)
    return pl.pallas_call(
        pack_kernel,
        in_specs=[hbm, hbm],
        out_shape=tuple(jax.ShapeDtypeStruct((rows + rows // 2, heads), BF) for _ in range(groups)),
        scratch_shapes=[
            pltpu.VMEM(attn_out.shape, BF),
            pltpu.VMEM(lat_turned.shape, BF),
            pltpu.VMEM(lat_turned.shape[::-1], BF),
            pltpu.SemaphoreType.DMA((2,)),
        ],
        cost_estimate=pl.CostEstimate(flops=10**7, bytes_accessed=10**6, transcendentals=0),
        compiler_params=pltpu.CompilerParams(vmem_limit_bytes=WHOLE),
        name="pack",
    )(attn_out, lat_turned)


def old_kernel(weight_o, weight_v, out_ref):
    rows_o = weight_o.shape[0]
    out_ref[:rows_o] = weight_o[:, :128].astype(BF)
    out_ref[rows_o : 2 * rows_o] = weight_o[:, 128:].astype(BF)
    out_ref[2 * rows_o :] = weight_v[...].astype(BF)


def old_rows(weight_o, weight_v):
    rows = 2 * weight_o.shape[0] + weight_v.shape[0]
    return pl.pallas_call(
        old_kernel,
        out_shape=jax.ShapeDtypeStruct((rows, 128), BF),
        cost_estimate=pl.CostEstimate(flops=10**6, bytes_accessed=10**5, transcendentals=0),
        compiler_params=pltpu.CompilerParams(vmem_limit_bytes=ROOM),
        name="old",
    )(weight_o, weight_v)


def lift_kernel(rows_o, tokens, blocks_ref, *refs):
    gots, out_ref = refs[:-1], refs[-1]
    groups = len(gots)
    rank = blocks_ref.shape[2]
    half = tokens // 2
    first = jnp.zeros((tokens, rank), F32)
    second = jnp.zeros((half, 2 * rank), F32)
    for k, got_ref in enumerate(gots):
        g = lax.rem(lax.axis_index("x") + groups - k, groups)
        low, high = blocks_ref[g], blocks_ref[groups + g]
        basis_o = jnp.concatenate([low[:rows_o], high[:rows_o]], 0)
        basis_v = jnp.concatenate([low[rows_o:], high[rows_o:]], 0)
        none = jnp.zeros_like(basis_v)
        pair = jnp.concatenate(
            [jnp.concatenate([basis_v, none], 0), jnp.concatenate([none, basis_v], 0)], 1
        )
        first = first + dot(got_ref[:tokens, :], basis_o)
        second = second + dot(got_ref[tokens:, :], pair)
    parts, each = out_ref.shape[:2]
    for p in range(parts):
        at = p * each
        out_ref[p, :, :rank] = first[at : at + each].astype(BF)
        row, side = at % half, at // half
        out_ref[p, :, rank:] = second[row : row + each, side * rank : (side + 1) * rank].astype(BF)


def lift(blocks, gots, rows_o, tokens, parts):
    rank = blocks.shape[2]
    return pl.pallas_call(
        functools.partial(lift_kernel, rows_o, tokens),
        out_shape=jax.ShapeDtypeStruct((parts, tokens // parts, 2 * rank), BF),
        cost_estimate=pl.CostEstimate(flops=2 * 10**8, bytes_accessed=10**6, transcendentals=0),
        compiler_params=pltpu.CompilerParams(vmem_limit_bytes=ROOM),
        name="lift",
    )(blocks, *gots)


def spread_kernel(got_ref, out_ref):
    total = got_ref[0].astype(F32)
    for i in range(1, got_ref.shape[0]):
        total = total + got_ref[i].astype(F32)
    total = total.astype(out_ref.dtype)
    for i in range(out_ref.shape[0]):
        out_ref[i] = total


def summed_for(got, copies, kind):
    return pl.pallas_call(
        spread_kernel,
        out_shape=jax.ShapeDtypeStruct((copies, *got.shape[1:]), kind),
        cost_estimate=pl.CostEstimate(flops=10**7, bytes_accessed=10**6, transcendentals=0),
        compiler_params=pltpu.CompilerParams(vmem_limit_bytes=ROOM),
    )(got)


def contract_kernel(lifted_ref, cot_o, cot_v, out_ref, total_o, total_v):
    step = pl.program_id(0)
    rank = total_o.shape[0]
    dims = (((0,), (0,)), ((), ()))

    def term(side, cot):
        rows = lifted_ref[:, side * rank : (side + 1) * rank]
        return lax.dot_general(rows, cot[...], dims, preferred_element_type=F32)

    @pl.when(step == 0)
    def _():
        total_o[...] = term(0, cot_o)
        total_v[...] = term(1, cot_v)

    @pl.when(step > 0)
    def _():
        total_o[...] += term(0, cot_o)
        total_v[...] += term(1, cot_v)

    @pl.when(step == pl.num_programs(0) - 1)
    def _():
        cols_o = total_o.shape[1]
        parts, each, _ = out_ref.shape
        for p in range(parts):
            out_ref[p, :, :cols_o] = total_o[p * each : (p + 1) * each].astype(BF)
            out_ref[p, :, cols_o:] = total_v[p * each : (p + 1) * each].astype(BF)


def contract(lifted, cot_o, cot_v, parts, steps):
    tokens, both = lifted.shape
    rank, cols_o, cols_v = both // 2, cot_o.shape[1], cot_v.shape[1]
    rows = tokens // steps
    shape = (parts, rank // parts, cols_o + cols_v)
    return pl.pallas_call(
        contract_kernel,
        grid=(steps,),
        in_specs=[
            pl.BlockSpec((rows, both), lambda i: (i, 0)),
            pl.BlockSpec((rows, cols_o), lambda i: (i, 0)),
            pl.BlockSpec((rows, cols_v), lambda i: (i, 0)),
        ],
        out_specs=pl.BlockSpec(shape, lambda i: (0, 0, 0)),
        out_shape=jax.ShapeDtypeStruct(shape, BF),
        scratch_shapes=[pltpu.VMEM((rank, cols_o), F32), pltpu.VMEM((rank, cols_v), F32)],
        cost_estimate=pl.CostEstimate(flops=3 * 10**8, bytes_accessed=3 * 10**6, transcendentals=0),
        compiler_params=pltpu.CompilerParams(vmem_limit_bytes=ROOM),
        name="contract",
    )(lifted, cot_o, cot_v)


def direction_kernel(
    rows_o, cols_o, got_ref, mean_o, square_o, mean_v, square_v, b0, b1, b2, b3,
    mean_o_out, square_o_out, mean_v_out, square_v_out, total_out,
):
    near = got_ref.shape[0]
    proj = jnp.concatenate([got_ref[i] for i in range(near)], 0).astype(F32)
    mean = jnp.concatenate([mean_o[...], mean_v[...]], 1)
    square = jnp.concatenate([square_o[...], square_v[...]], 1)
    mean = MEAN_DECAY * mean + (1.0 - MEAN_DECAY) * proj
    square = BETA_SQUARE * square + (1.0 - BETA_SQUARE) * proj * proj
    mean_o_out[...] = mean[:, :cols_o]
    mean_v_out[...] = mean[:, cols_o:]
    square_o_out[...] = square[:, :cols_o]
    square_v_out[...] = square[:, cols_o:]
    upper = (mean / jnp.sqrt(square)).astype(BF)
    upper_o, upper_v = upper[:, :cols_o], upper[:, cols_o:]
    total_o = jnp.zeros((8, cols_o), F32)
    total_v = jnp.zeros((8, upper_v.shape[1]), F32)
    for ref in (b0, b1, b2, b3):
        count = ref.shape[0]
        basis_o = jnp.concatenate([ref[i, :rows_o, :] for i in range(count)], 0)
        basis_v = jnp.concatenate([ref[i, rows_o:, :] for i in range(count)], 0)
        update = dot(basis_o, upper_o)
        total_o = total_o + jnp.sum((update * update).reshape(-1, 8, cols_o), 0)
        update = dot(basis_v, upper_v)
        total_v = total_v + jnp.sum((update * update).reshape(-1, 8, update.shape[1]), 0)
    sums = [
        jnp.broadcast_to(jnp.sum(t, keepdims=True), (4, 128)) for t in (total_o, total_v)
    ]
    tile = jnp.concatenate(sums, 0)
    for i in range(total_out.shape[0]):
        total_out[i] = tile


def directions(rows_o, copies, got, mean_o, square_o, mean_v, square_v, segments):
    cols_o = mean_o.shape[1]
    shape = jax.ShapeDtypeStruct
    return pl.pallas_call(
        functools.partial(direction_kernel, rows_o, cols_o),
        out_shape=(
            shape(mean_o.shape, F32),
            shape(mean_o.shape, F32),
            shape(mean_v.shape, F32),
            shape(mean_v.shape, F32),
            shape((copies, 8, 128), F32),
        ),
        cost_estimate=pl.CostEstimate(flops=4 * 10**8, bytes_accessed=4 * 10**6, transcendentals=10**5),
        compiler_params=pltpu.CompilerParams(vmem_limit_bytes=ROOM),
        name="directions",
    )(got, mean_o, square_o, mean_v, square_v, *segments)


def ready_kernel(
    rows_o, rows_v, mean_o, square_o, mean_v, square_v, local_o, local_v, own_ref, other_ref, b0, b1, b2, b3,
    step_o_out, step_v_out, update_o_out, update_v_out, old_o_out, old_v_out,
):
    uppers = []
    for mean, square, local, step_out in (
        (mean_o, square_o, local_o, step_o_out),
        (mean_v, square_v, local_v, step_v_out),
    ):
        way = mean[...] / jnp.sqrt(square[...])
        upper = way.astype(BF)
        lower = (way - upper.astype(F32)).astype(BF)
        step_out[...] = dot(local[...], upper) + dot(local[...], lower)
        uppers.append(upper)
    upper_o, upper_v = uppers
    y, c = lax.axis_index("y"), lax.axis_index("c")
    z = 4 * lax.axis_index("zh") + lax.axis_index("zl")
    for k, ref in enumerate((b0, b1, b2, b3)):
        origin = lax.rem(y + 4 - k, 4)
        count = ref.shape[0]
        basis_o = jnp.concatenate([ref[i, :rows_o, :] for i in range(count)], 0)
        basis_v = jnp.concatenate([ref[i, rows_o:, :] for i in range(count)], 0)
        update_o = dot(basis_o, upper_o).astype(BF)
        update_v = dot(basis_v, upper_v).astype(BF)
        for i in range(count):
            core, x = divmod(i, count // 2)
            index = 8 * origin + 2 * x + core
            at = pl.multiple_of(index * rows_o, rows_o)
            update_o_out[pl.ds(at, rows_o), :] = update_o[i * rows_o : (i + 1) * rows_o]
            at = pl.multiple_of(index * rows_v, rows_v)
            update_v_out[pl.ds(at, rows_v), :] = update_v[i * rows_v : (i + 1) * rows_v]
    for ref, core in ((own_ref, c), (other_ref, 1 - c)):
        for p in range(ref.shape[0]):
            behind = (p & 1) * 8 + (p >> 1 & 1) * 4 + STEPS[p >> 2]
            index = 2 * lax.rem(z + 16 - behind, 16) + core
            at = pl.multiple_of(index * rows_o, rows_o)
            old_o_out[pl.ds(at, rows_o), :128] = ref[p, :rows_o]
            old_o_out[pl.ds(at, rows_o), 128:] = ref[p, rows_o : 2 * rows_o]
            at = pl.multiple_of(index * rows_v, rows_v)
            old_v_out[pl.ds(at, rows_v), :] = ref[p, 2 * rows_o :]


def ready(moments, local_o, local_v, own, other, segments):
    rows_o, rows_v = local_o.shape[0], local_v.shape[0]
    cols_o, cols_v = moments[0].shape[1], moments[2].shape[1]
    fs = 2 * own.shape[0]
    shape = jax.ShapeDtypeStruct
    return pl.pallas_call(
        functools.partial(ready_kernel, rows_o, rows_v),
        out_shape=(
            shape((rows_o, cols_o), F32),
            shape((rows_v, cols_v), F32),
            shape((rows_o * fs, cols_o), BF),
            shape((rows_v * fs, cols_v), BF),
            shape((rows_o * fs, cols_o), BF),
            shape((rows_v * fs, cols_v), BF),
        ),
        cost_estimate=pl.CostEstimate(flops=4 * 10**8, bytes_accessed=4 * 10**6, transcendentals=0),
        compiler_params=pltpu.CompilerParams(vmem_limit_bytes=WHOLE),
        name="ready",
    )(*moments, local_o, local_v, own, other, *segments)


def output_kernel(
    counts, pieces, total_ref, weight_o, weight_v, step_o, step_v, update_o, update_v, old_o, old_v,
    step_o_out, new_o_out, copy_o_out, step_v_out, new_v_out, copy_v_out,
    update_o_here, update_v_here, old_o_here, old_v_here, sems,
):
    copies = []
    for n, (source, here) in enumerate(
        ((update_o, update_o_here), (old_o, old_o_here), (update_v, update_v_here), (old_v, old_v_here))
    ):
        rows = source.shape[0] // pieces
        for p in range(pieces):
            part = pl.ds(p * rows, rows)
            copies.append(pltpu.make_async_copy(source.at[part], here.at[part], sems.at[n, p]))
    for copy in copies:
        copy.start()
    total = total_ref[0]
    for i in range(1, total_ref.shape[0]):
        total = total + total_ref[i]
    scales = []
    for row, count, weight, step, step_out, new_out in (
        (0, counts[0], weight_o, step_o, step_o_out, new_o_out),
        (4, counts[1], weight_v, step_v, step_v_out, new_v_out),
    ):
        scale = LEARN_RATE * lax.rsqrt(total[row : row + 1, 0:1] / count + EPS_RMS)
        mine = step[...] * scale
        step_out[...] = mine
        new_out[...] = weight[...] - mine
        scales.append(scale)
    for n, (scale, update, old, copy_out) in enumerate(
        (
            (scales[0], update_o_here, old_o_here, copy_o_out),
            (scales[1], update_v_here, old_v_here, copy_v_out),
        )
    ):
        rows = old.shape[0] // pieces
        for p in range(pieces):
            copies[2 * n * pieces + p].wait()
            copies[(2 * n + 1) * pieces + p].wait()
            part = pl.ds(p * rows, rows)
            copy_out[part, :] = (old[part, :].astype(F32) - update[part, :].astype(F32) * scale).astype(BF)


def outputs(counts, total, weight_o, weight_v, step_o, step_v, update_o, update_v, old_o, old_v):
    shape = jax.ShapeDtypeStruct
    vmem = pl.BlockSpec(memory_space=pltpu.VMEM)
    hbm = pl.BlockSpec(memory_space=pltpu.HBM)
    pieces = 4
    return pl.pallas_call(
        functools.partial(output_kernel, counts, pieces),
        in_specs=[vmem] * 5 + [hbm] * 4,
        out_shape=(
            shape(weight_o.shape, F32),
            shape(weight_o.shape, F32),
            shape(old_o.shape, BF),
            shape(weight_v.shape, F32),
            shape(weight_v.shape, F32),
            shape(old_v.shape, BF),
        ),
        scratch_shapes=[pltpu.VMEM(a.shape, BF) for a in (update_o, update_v, old_o, old_v)]
        + [pltpu.SemaphoreType.DMA((4, pieces))],
        cost_estimate=pl.CostEstimate(flops=10**7, bytes_accessed=4 * 10**6, transcendentals=10),
        compiler_params=pltpu.CompilerParams(vmem_limit_bytes=WHOLE),
        name="outputs",
    )(total, weight_o, weight_v, step_o, step_v, update_o, update_v, old_o, old_v)


def per_device(
    attn_out,
    out_cot,
    latent,
    value_cot,
    out_weight,
    value_up_matrix,
    out_basis,
    value_basis,
    out_mean,
    out_square,
    value_mean,
    value_square,
):
    tokens = attn_out.shape[0]
    cols_o = out_cot.shape[1]
    cols_v = value_cot.shape[1]
    rows_o, rank = out_basis.shape
    rows_v = value_basis.shape[0]
    tp = lax.axis_size(TP)
    fs = lax.axis_size(FS)
    xs, ys = lax.axis_size("x"), lax.axis_size("y")


    block = swapped_blocks(jnp.concatenate([out_basis, value_basis], 0))

    gots = list(pack(attn_out, latent.T, xs))
    for k in range(1, xs):
        gots[k] = shifted(gots[k], "x", k)

    own = old_rows(out_weight, value_up_matrix)[None]
    for k in (8, 4):
        more = shifted(own, Z, k)
        own = lax.optimization_barrier(jnp.concatenate([own, more], 0))
    rows = [own]
    for k in STEPS[1:]:
        rows.append(shifted(own, Z, k))
    own = lax.optimization_barrier(jnp.concatenate(rows, 0))
    other = shifted(own, "c", 1)

    blocks = from_everyone(block, ("c", "x"))
    partial = lift(blocks, gots, rows_o, tokens // xs, ys)
    partial = exchange(partial, "y")
    lifted = summed_for(partial, tp, BF)
    lifted = exchange(lifted, TP).reshape(tokens, 2 * rank)

    near = lax.axis_size(NEAR)
    part = contract(lifted, out_cot, value_cot, near, 4)
    part = exchange(part, NEAR)
    part = exchange(summed_for(part, lax.axis_size("zh"), BF), "zh")
    proj = exchange(summed_for(part, near, BF), NEAR)

    segments = [blocks]
    for k in range(1, ys):
        segments.append(shifted(blocks, "y", k))

    mean_o, square_o, mean_v, square_v, total = directions(
        rows_o, tp, proj, out_mean, out_square, value_mean, value_square, segments
    )
    total = exchange(total, TP)
    moments = (mean_o, square_o, mean_v, square_v)
    prepared = ready(moments, out_basis, value_basis, own, other, segments)
    counts = (rows_o * fs * cols_o * tp, rows_v * fs * cols_v * tp)
    step_o, new_o, copy_o, step_v, new_v, copy_v = outputs(
        counts, total, out_weight, value_up_matrix, *prepared
    )
    return (step_o, new_o, copy_o, mean_o, square_o, step_v, new_v, copy_v, mean_v, square_v)


def solution(mesh):
    torus = Mesh(mesh.devices.reshape(4, 4, 2, 4, 4), ALL)
    both = P(FS, TP)
    cols = P(None, TP)
    rows = P(FS, None)

    return jax.shard_map(
        per_device,
        mesh=torus,
        in_specs=(both, both, both, both, both, both, rows, rows, cols, cols, cols, cols),
        out_specs=(both, both, cols, cols, cols, both, both, cols, cols, cols),
        check_vma=False,
    )
```

```python
import functools

import jax
import jax.numpy as jnp
from jax import lax
from jax.experimental import pallas as pl
from jax.experimental.pallas import tpu as pltpu
from jax.sharding import Mesh
from jax.sharding import PartitionSpec as P


TP = ("y", "x")
FS = ("zh", "zl", "c")
NEAR = ("zl", "c")
Z = ("zh", "zl")
ALL = ("zh", "zl", "c", "y", "x")

LEARN_RATE = 0.01
MEAN_DECAY = 0.8
BETA_SQUARE = 0.9
EPS_RMS = 1e-06

BF = jnp.bfloat16
ROOM = 12 * 2**20
WHOLE = 67043328
STEPS = (0, 1, 2, -1)
F32 = jnp.float32


def exchange(value, axes):
    return lax.all_to_all(value, axes, 0, 0, tiled=True)


def from_everyone(value, axes):
    devices = lax.axis_size(axes)
    return exchange(jnp.broadcast_to(value[None], (devices, *value.shape)), axes)


def swapped_blocks(value):
    pairs = []
    for j in range(16):
        for b in range(2):
            for t in range(16):
                pairs.append(((2 * j + b) * 16 + t, (2 * t + b) * 16 + j))
    return lax.ppermute(value, ALL, pairs)


def shifted(value, axis, by):
    devices = lax.axis_size(axis)
    return lax.ppermute(value, axis, [(i, (i + by) % devices) for i in range(devices)])


def dot(a, b):
    return jnp.dot(a, b, preferred_element_type=F32)


def pack_kernel( attn_ref, lat_ref, *refs):
    outs, (attn_here, lat_here, turned, sems) = refs[:-4], refs[-4:]
    groups = len(outs)
    each = attn_ref.shape[0] // groups**2
    copies = [
        pltpu.make_async_copy(lat_ref, lat_here, sems.at[0]),
        pltpu.make_async_copy(attn_ref, attn_here, sems.at[1]),
    ]
    for copy in copies:
        copy.start()
    copies[0].wait()
    turned[...] = lat_here[...].T
    copies[1].wait()
    for k in range(groups):
        g = lax.rem(lax.axis_index("x") + k, groups)
        pieces = []
        for p in range(groups):
            at = pl.multiple_of((g * groups + p) * each, each)
            outs[k][p * each : (p + 1) * each, :] = attn_here[pl.ds(at, each), :]
            pieces.append(turned[pl.ds(at, each), :])
        half = groups // 2
        for p in range(half):
            at = (groups + p) * each
            outs[k][at : at + each, :] = jnp.concatenate([pieces[p], pieces[half + p]], axis=1)


def pack(attn_out, lat_turned, groups):
    tokens, heads = attn_out.shape
    rows = tokens // groups
    hbm = pl.BlockSpec(memory_space=pltpu.HBM)
    return pl.pallas_call(
        pack_kernel,
        in_specs=[hbm, hbm],
        out_shape=tuple(jax.ShapeDtypeStruct((rows + rows // 2, heads), BF) for _ in range(groups)),
        scratch_shapes=[
            pltpu.VMEM(attn_out.shape, BF),
            pltpu.VMEM(lat_turned.shape, BF),
            pltpu.VMEM(lat_turned.shape[::-1], BF),
            pltpu.SemaphoreType.DMA((2,)),
        ],
        cost_estimate=pl.CostEstimate(flops=10**7, bytes_accessed=10**6, transcendentals=0),
        compiler_params=pltpu.CompilerParams(vmem_limit_bytes=WHOLE - 2**18),
        name="pack",
    )(attn_out, lat_turned)


def old_kernel(weight_o, weight_v, out_ref):
    rows_o = weight_o.shape[0]
    out_ref[:rows_o] = weight_o[:, :128].astype(BF)
    out_ref[rows_o : 2 * rows_o] = weight_o[:, 128:].astype(BF)
    out_ref[2 * rows_o :] = weight_v[...].astype(BF)


def old_rows(weight_o, weight_v):
    rows = 2 * weight_o.shape[0] + weight_v.shape[0]
    return pl.pallas_call(
        old_kernel,
        out_shape=jax.ShapeDtypeStruct((rows, 128), BF),
        cost_estimate=pl.CostEstimate(flops=10**6, bytes_accessed=10**5, transcendentals=0),
        compiler_params=pltpu.CompilerParams(vmem_limit_bytes=ROOM),
        name="old",
    )(weight_o, weight_v)


def lift_kernel(rows_o, tokens, blocks_ref, *refs):
    gots, out_ref = refs[:-1], refs[-1]
    groups = len(gots)
    rank = blocks_ref.shape[2]
    half = tokens // 2
    first = jnp.zeros((tokens, rank), F32)
    second = jnp.zeros((half, 2 * rank), F32)
    for k, got_ref in enumerate(gots):
        g = lax.rem(lax.axis_index("x") + groups - k, groups)
        low, high = blocks_ref[g], blocks_ref[groups + g]
        basis_o = jnp.concatenate([low[:rows_o], high[:rows_o]], 0)
        basis_v = jnp.concatenate([low[rows_o:], high[rows_o:]], 0)
        none = jnp.zeros_like(basis_v)
        pair = jnp.concatenate(
            [jnp.concatenate([basis_v, none], 0), jnp.concatenate([none, basis_v], 0)], 1
        )
        first = first + dot(got_ref[:tokens, :], basis_o)
        second = second + dot(got_ref[tokens:, :], pair)
    parts, each = out_ref.shape[:2]
    for p in range(parts):
        at = p * each
        out_ref[p, :, :rank] = first[at : at + each].astype(BF)
        row, side = at % half, at // half
        out_ref[p, :, rank:] = second[row : row + each, side * rank : (side + 1) * rank].astype(BF)


def lift(blocks, gots, rows_o, tokens, parts):
    rank = blocks.shape[2]
    return pl.pallas_call(
        functools.partial(lift_kernel, rows_o, tokens),
        out_shape=jax.ShapeDtypeStruct((parts, tokens // parts, 2 * rank), BF),
        cost_estimate=pl.CostEstimate(flops=2 * 10**8, bytes_accessed=10**6, transcendentals=0),
        compiler_params=pltpu.CompilerParams(vmem_limit_bytes=WHOLE),
        name="lift",
    )(blocks, *gots)


def spread_kernel(got_ref, out_ref):
    total = got_ref[0].astype(F32)
    for i in range(1, got_ref.shape[0]):
        total = total + got_ref[i].astype(F32)
    total = total.astype(out_ref.dtype)
    for i in range(out_ref.shape[0]):
        out_ref[i] = total


def summed_for(got, copies, kind):
    return pl.pallas_call(
        spread_kernel,
        out_shape=jax.ShapeDtypeStruct((copies, *got.shape[1:]), kind),
        cost_estimate=pl.CostEstimate(flops=10**7, bytes_accessed=10**6, transcendentals=0),
        compiler_params=pltpu.CompilerParams(vmem_limit_bytes=ROOM),
    )(got)


def contract_kernel(lifted_ref, cot_o, cot_v, out_ref, total_o, total_v):
    step = pl.program_id(0)
    rank = total_o.shape[0]
    dims = (((0,), (0,)), ((), ()))

    def term(side, cot):
        rows = lifted_ref[:, side * rank : (side + 1) * rank]
        return lax.dot_general(rows, cot[...], dims, preferred_element_type=F32)

    @pl.when(step == 0)
    def _():
        total_o[...] = term(0, cot_o)
        total_v[...] = term(1, cot_v)

    @pl.when(step > 0)
    def _():
        total_o[...] += term(0, cot_o)
        total_v[...] += term(1, cot_v)

    @pl.when(step == pl.num_programs(0) - 1)
    def _():
        cols_o = total_o.shape[1]
        parts, each, _ = out_ref.shape
        for p in range(parts):
            out_ref[p, :, :cols_o] = total_o[p * each : (p + 1) * each].astype(BF)
            out_ref[p, :, cols_o:] = total_v[p * each : (p + 1) * each].astype(BF)


def contract(lifted, cot_o, cot_v, parts, steps):
    tokens, both = lifted.shape
    rank, cols_o, cols_v = both // 2, cot_o.shape[1], cot_v.shape[1]
    rows = tokens // steps
    shape = (parts, rank // parts, cols_o + cols_v)
    return pl.pallas_call(
        contract_kernel,
        grid=(steps,),
        in_specs=[
            pl.BlockSpec((rows, both), lambda i: (i, 0)),
            pl.BlockSpec((rows, cols_o), lambda i: (i, 0)),
            pl.BlockSpec((rows, cols_v), lambda i: (i, 0)),
        ],
        out_specs=pl.BlockSpec(shape, lambda i: (0, 0, 0)),
        out_shape=jax.ShapeDtypeStruct(shape, BF),
        scratch_shapes=[pltpu.VMEM((rank, cols_o), F32), pltpu.VMEM((rank, cols_v), F32)],
        cost_estimate=pl.CostEstimate(flops=3 * 10**8, bytes_accessed=3 * 10**6, transcendentals=0),
        compiler_params=pltpu.CompilerParams(vmem_limit_bytes=ROOM),
        name="contract",
    )(lifted, cot_o, cot_v)


def direction_kernel(
    rows_o, cols_o, got_ref, mean_o, square_o, mean_v, square_v, b0, b1, b2, b3,
    mean_o_out, square_o_out, mean_v_out, square_v_out, total_out,
):
    near = got_ref.shape[0]
    proj = jnp.concatenate([got_ref[i] for i in range(near)], 0).astype(F32)
    mean = jnp.concatenate([mean_o[...], mean_v[...]], 1)
    square = jnp.concatenate([square_o[...], square_v[...]], 1)
    mean = MEAN_DECAY * mean + (1.0 - MEAN_DECAY) * proj
    square = BETA_SQUARE * square + (1.0 - BETA_SQUARE) * proj * proj
    mean_o_out[...] = mean[:, :cols_o]
    mean_v_out[...] = mean[:, cols_o:]
    square_o_out[...] = square[:, :cols_o]
    square_v_out[...] = square[:, cols_o:]
    upper = (mean / jnp.sqrt(square)).astype(BF)
    upper_o, upper_v = upper[:, :cols_o], upper[:, cols_o:]
    total_o = jnp.zeros((8, cols_o), F32)
    total_v = jnp.zeros((8, upper_v.shape[1]), F32)
    for ref in (b0, b1, b2, b3):
        count = ref.shape[0]
        basis_o = jnp.concatenate([ref[i, :rows_o, :] for i in range(count)], 0)
        basis_v = jnp.concatenate([ref[i, rows_o:, :] for i in range(count)], 0)
        update = dot(basis_o, upper_o)
        total_o = total_o + jnp.sum((update * update).reshape(-1, 8, cols_o), 0)
        update = dot(basis_v, upper_v)
        total_v = total_v + jnp.sum((update * update).reshape(-1, 8, update.shape[1]), 0)
    sums = [
        jnp.broadcast_to(jnp.sum(t, keepdims=True), (4, 128)) for t in (total_o, total_v)
    ]
    tile = jnp.concatenate(sums, 0)
    for i in range(total_out.shape[0]):
        total_out[i] = tile


def directions(rows_o, copies, got, mean_o, square_o, mean_v, square_v, segments):
    cols_o = mean_o.shape[1]
    shape = jax.ShapeDtypeStruct
    return pl.pallas_call(
        functools.partial(direction_kernel, rows_o, cols_o),
        out_shape=(
            shape(mean_o.shape, F32),
            shape(mean_o.shape, F32),
            shape(mean_v.shape, F32),
            shape(mean_v.shape, F32),
            shape((copies, 8, 128), F32),
        ),
        cost_estimate=pl.CostEstimate(flops=4 * 10**8, bytes_accessed=4 * 10**6, transcendentals=10**5),
        compiler_params=pltpu.CompilerParams(vmem_limit_bytes=ROOM),
        name="directions",
    )(got, mean_o, square_o, mean_v, square_v, *segments)


def ready_kernel(
    rows_o, rows_v, mean_o, square_o, mean_v, square_v, local_o, local_v, own_ref, other_ref, b0, b1, b2, b3,
    step_o_out, step_v_out, update_o_out, update_v_out, old_o_out, old_v_out,
):
    uppers = []
    for mean, square, local, step_out in (
        (mean_o, square_o, local_o, step_o_out),
        (mean_v, square_v, local_v, step_v_out),
    ):
        way = mean[...] / jnp.sqrt(square[...])
        upper = way.astype(BF)
        lower = (way - upper.astype(F32)).astype(BF)
        step_out[...] = dot(local[...], upper) + dot(local[...], lower)
        uppers.append(upper)
    upper_o, upper_v = uppers
    y, c = lax.axis_index("y"), lax.axis_index("c")
    z = 4 * lax.axis_index("zh") + lax.axis_index("zl")
    for k, ref in enumerate((b0, b1, b2, b3)):
        origin = lax.rem(y + 4 - k, 4)
        count = ref.shape[0]
        basis_o = jnp.concatenate([ref[i, :rows_o, :] for i in range(count)], 0)
        basis_v = jnp.concatenate([ref[i, rows_o:, :] for i in range(count)], 0)
        update_o = dot(basis_o, upper_o).astype(BF)
        update_v = dot(basis_v, upper_v).astype(BF)
        for i in range(count):
            core, x = divmod(i, count // 2)
            index = 8 * origin + 2 * x + core
            at = pl.multiple_of(index * rows_o, rows_o)
            update_o_out[pl.ds(at, rows_o), :] = update_o[i * rows_o : (i + 1) * rows_o]
            at = pl.multiple_of(index * rows_v, rows_v)
            update_v_out[pl.ds(at, rows_v), :] = update_v[i * rows_v : (i + 1) * rows_v]
    for ref, core in ((own_ref, c), (other_ref, 1 - c)):
        for p in range(ref.shape[0]):
            behind = (0, 8, 4, 12)[p & 3] + STEPS[p >> 2]
            index = 2 * lax.rem(z + 32 - behind, 16) + core
            at = pl.multiple_of(index * rows_o, rows_o)
            old_o_out[pl.ds(at, rows_o), :128] = ref[p, :rows_o]
            old_o_out[pl.ds(at, rows_o), 128:] = ref[p, rows_o : 2 * rows_o]
            at = pl.multiple_of(index * rows_v, rows_v)
            old_v_out[pl.ds(at, rows_v), :] = ref[p, 2 * rows_o :]


def ready(moments, local_o, local_v, own, other, segments):
    rows_o, rows_v = local_o.shape[0], local_v.shape[0]
    cols_o, cols_v = moments[0].shape[1], moments[2].shape[1]
    fs = 2 * own.shape[0]
    shape = jax.ShapeDtypeStruct
    return pl.pallas_call(
        functools.partial(ready_kernel, rows_o, rows_v),
        out_shape=(
            shape((rows_o, cols_o), F32),
            shape((rows_v, cols_v), F32),
            shape((rows_o * fs, cols_o), BF),
            shape((rows_v * fs, cols_v), BF),
            shape((rows_o * fs, cols_o), BF),
            shape((rows_v * fs, cols_v), BF),
        ),
        cost_estimate=pl.CostEstimate(flops=4 * 10**8, bytes_accessed=4 * 10**6, transcendentals=0),
        compiler_params=pltpu.CompilerParams(vmem_limit_bytes=WHOLE),
        name="ready",
    )(*moments, local_o, local_v, own, other, *segments)


def output_kernel(
    counts, pieces, total_ref, weight_o, weight_v, step_o, step_v, update_o, update_v, old_o, old_v,
    step_o_out, new_o_out, copy_o_out, step_v_out, new_v_out, copy_v_out,
    update_o_here, update_v_here, old_o_here, old_v_here, copy_o_here, copy_v_here, sems, out_sems,
):
    copies = []
    for n, (source, here) in enumerate(
        ((update_o, update_o_here), (old_o, old_o_here), (update_v, update_v_here), (old_v, old_v_here))
    ):
        rows = source.shape[0] // pieces
        for p in range(pieces):
            part = pl.ds(p * rows, rows)
            copies.append(pltpu.make_async_copy(source.at[part], here.at[part], sems.at[n, p]))
    for copy in copies:
        copy.start()
    total = total_ref[0]
    for i in range(1, total_ref.shape[0]):
        total = total + total_ref[i]
    scales = []
    for row, count, weight, step, step_out, new_out in (
        (0, counts[0], weight_o, step_o, step_o_out, new_o_out),
        (4, counts[1], weight_v, step_v, step_v_out, new_v_out),
    ):
        scale = LEARN_RATE * lax.rsqrt(total[row : row + 1, 0:1] / count + EPS_RMS)
        mine = step[...] * scale
        step_out[...] = mine
        new_out[...] = weight[...] - mine
        scales.append(scale)
    leaving = []
    for n, (scale, update, old, here, copy_out) in enumerate(
        (
            (scales[0], update_o_here, old_o_here, copy_o_here, copy_o_out),
            (scales[1], update_v_here, old_v_here, copy_v_here, copy_v_out),
        )
    ):
        rows = old.shape[0] // pieces
        for p in range(pieces):
            copies[2 * n * pieces + p].wait()
            copies[(2 * n + 1) * pieces + p].wait()
            part = pl.ds(p * rows, rows)
            here[part, :] = (old[part, :].astype(F32) - update[part, :].astype(F32) * scale).astype(BF)
            leaving.append(pltpu.make_async_copy(here.at[part], copy_out.at[part], out_sems.at[n, p]))
            leaving[-1].start()
    for copy in leaving:
        copy.wait()


def outputs(counts, total, weight_o, weight_v, step_o, step_v, update_o, update_v, old_o, old_v):
    shape = jax.ShapeDtypeStruct
    vmem = pl.BlockSpec(memory_space=pltpu.VMEM)
    hbm = pl.BlockSpec(memory_space=pltpu.HBM)
    pieces = 4
    return pl.pallas_call(
        functools.partial(output_kernel, counts, pieces),
        in_specs=[vmem] * 5 + [hbm] * 4,
        out_specs=(vmem, vmem, hbm, vmem, vmem, hbm),
        out_shape=(
            shape(weight_o.shape, F32),
            shape(weight_o.shape, F32),
            shape(old_o.shape, BF),
            shape(weight_v.shape, F32),
            shape(weight_v.shape, F32),
            shape(old_v.shape, BF),
        ),
        scratch_shapes=[pltpu.VMEM(a.shape, BF) for a in (update_o, update_v, old_o, old_v, old_o, old_v)]
        + [pltpu.SemaphoreType.DMA((4, pieces)), pltpu.SemaphoreType.DMA((2, pieces))],
        cost_estimate=pl.CostEstimate(flops=10**7, bytes_accessed=4 * 10**6, transcendentals=10),
        compiler_params=pltpu.CompilerParams(vmem_limit_bytes=WHOLE),
        name="outputs",
    )(total, weight_o, weight_v, step_o, step_v, update_o, update_v, old_o, old_v)


def per_device(
    attn_out,
    out_cot,
    latent,
    value_cot,
    out_weight,
    value_up_matrix,
    out_basis,
    value_basis,
    out_mean,
    out_square,
    value_mean,
    value_square,
):
    tokens = attn_out.shape[0]
    cols_o = out_cot.shape[1]
    cols_v = value_cot.shape[1]
    rows_o, rank = out_basis.shape
    rows_v = value_basis.shape[0]
    tp = lax.axis_size(TP)
    fs = lax.axis_size(FS)
    xs, ys = lax.axis_size("x"), lax.axis_size("y")


    block = swapped_blocks(jnp.concatenate([out_basis, value_basis], 0))

    gots = list(pack(attn_out, latent.T, xs))
    for k in range(1, xs):
        gots[k] = shifted(gots[k], "x", k)

    own = old_rows(out_weight, value_up_matrix)[None]
    rows = [own]
    for k in (8, 4, 12):
        rows.append(shifted(own, Z, k))
    own = lax.optimization_barrier(jnp.concatenate(rows, 0))
    rows = [own]
    for k in STEPS[1:]:
        rows.append(shifted(own, Z, k))
    own = lax.optimization_barrier(jnp.concatenate(rows, 0))
    other = shifted(own, "c", 1)

    blocks = from_everyone(block, ("c", "x"))
    partial = lift(blocks, gots, rows_o, tokens // xs, ys)
    partial = exchange(partial, "y")
    lifted = summed_for(partial, tp, BF)
    lifted = exchange(lifted, ("x", "y")).reshape(tokens, 2 * rank)

    near = lax.axis_size(NEAR)
    part = contract(lifted, out_cot, value_cot, near, 4)
    part = exchange(part, NEAR)
    part = exchange(summed_for(part, lax.axis_size("zh"), BF), "zh")
    proj = exchange(summed_for(part, near, BF), NEAR)

    segments = [blocks]
    for k in range(1, ys):
        segments.append(shifted(blocks, "y", k))

    mean_o, square_o, mean_v, square_v, total = directions(
        rows_o, tp, proj, out_mean, out_square, value_mean, value_square, segments
    )
    total = exchange(total, TP)
    moments = (mean_o, square_o, mean_v, square_v)
    prepared = ready(moments, out_basis, value_basis, own, other, segments)
    counts = (rows_o * fs * cols_o * tp, rows_v * fs * cols_v * tp)
    step_o, new_o, copy_o, step_v, new_v, copy_v = outputs(
        counts, total, out_weight, value_up_matrix, *prepared
    )
    return (step_o, new_o, copy_o, mean_o, square_o, step_v, new_v, copy_v, mean_v, square_v)


def solution(mesh):
    torus = Mesh(mesh.devices.reshape(4, 4, 2, 4, 4), ALL)
    both = P(FS, TP)
    cols = P(None, TP)
    rows = P(FS, None)

    return jax.shard_map(
        per_device,
        mesh=torus,
        in_specs=(both, both, both, both, both, both, rows, rows, cols, cols, cols, cols),
        out_specs=(both, both, cols, cols, cols, both, both, cols, cols, cols),
        check_vma=False,
    )
```

```python
import functools

import jax
import jax.numpy as jnp
from jax import lax
from jax.experimental import pallas as pl
from jax.experimental.pallas import tpu as pltpu
from jax.sharding import Mesh
from jax.sharding import PartitionSpec as P


TP = ("y", "x")
FS = ("zh", "zl", "c")
NEAR = ("zl", "c")
Z = ("zh", "zl")
ALL = ("zh", "zl", "c", "y", "x")

LEARN_RATE = 0.01
MEAN_DECAY = 0.8
BETA_SQUARE = 0.9
EPS_RMS = 1e-06

BF = jnp.bfloat16
ROOM = 12 * 2**20
WHOLE = 67043328
STEPS = (0, 1, 2, -1)
F32 = jnp.float32


def exchange(value, axes):
    return lax.all_to_all(value, axes, 0, 0, tiled=True)


def from_everyone(value, axes):
    devices = lax.axis_size(axes)
    return exchange(jnp.broadcast_to(value[None], (devices, *value.shape)), axes)


def swapped_blocks(value):
    pairs = []
    for j in range(16):
        for b in range(2):
            for t in range(16):
                pairs.append(((2 * j + b) * 16 + t, (2 * t + b) * 16 + j))
    return lax.ppermute(value, ALL, pairs)


def shifted(value, axis, by):
    devices = lax.axis_size(axis)
    return lax.ppermute(value, axis, [(i, (i + by) % devices) for i in range(devices)])


def dot(a, b):
    return jnp.dot(a, b, preferred_element_type=F32)


def pack_kernel(attn_ref, lat_ref, out_ref, attn_here, lat_here, turned, sems):
    copies = [
        pltpu.make_async_copy(lat_ref, lat_here, sems.at[0]),
        pltpu.make_async_copy(attn_ref, attn_here, sems.at[1]),
    ]
    for copy in copies:
        copy.start()
    groups = out_ref.shape[0]
    each = attn_ref.shape[0] // groups
    half = each // 2
    copies[0].wait()
    turned[...] = lat_here[...].T
    copies[1].wait()
    for g in range(groups):
        at = g * each
        out_ref[g, :each, :] = attn_here[at : at + each, :]
        out_ref[g, each:, :] = jnp.concatenate(
            [turned[at : at + half, :], turned[at + half : at + each, :]], axis=1
        )


def pack(attn_out, lat_turned, groups):
    tokens, heads = attn_out.shape
    each = tokens // groups
    hbm = pl.BlockSpec(memory_space=pltpu.HBM)
    return pl.pallas_call(
        pack_kernel,
        in_specs=[hbm, hbm],
        out_shape=jax.ShapeDtypeStruct((groups, each + each // 2, heads), BF),
        scratch_shapes=[
            pltpu.VMEM(attn_out.shape, BF),
            pltpu.VMEM(lat_turned.shape, BF),
            pltpu.VMEM(lat_turned.shape[::-1], BF),
            pltpu.SemaphoreType.DMA((2,)),
        ],
        cost_estimate=pl.CostEstimate(flops=10**7, bytes_accessed=10**6, transcendentals=0),
        compiler_params=pltpu.CompilerParams(vmem_limit_bytes=WHOLE - 2**18),
        name="pack",
    )(attn_out, lat_turned)


def old_kernel(weight_o, weight_v, out_ref):
    rows_o = weight_o.shape[0]
    out_ref[:rows_o] = weight_o[:, :128].astype(BF)
    out_ref[rows_o : 2 * rows_o] = weight_o[:, 128:].astype(BF)
    out_ref[2 * rows_o :] = weight_v[...].astype(BF)


def old_rows(weight_o, weight_v):
    rows = 2 * weight_o.shape[0] + weight_v.shape[0]
    return pl.pallas_call(
        old_kernel,
        out_shape=jax.ShapeDtypeStruct((rows, 128), BF),
        cost_estimate=pl.CostEstimate(flops=10**6, bytes_accessed=10**5, transcendentals=0),
        compiler_params=pltpu.CompilerParams(vmem_limit_bytes=ROOM),
        name="old",
    )(weight_o, weight_v)


def lift_kernel(rows_o, got_ref, blocks_ref, out_ref):
    groups, packed, _ = got_ref.shape
    each = 2 * packed // 3
    half = each // 2
    rank = blocks_ref.shape[2]
    first = jnp.zeros((each, rank), F32)
    second = jnp.zeros((half, 2 * rank), F32)
    for g in range(groups):
        low, high = blocks_ref[g], blocks_ref[groups + g]
        basis_o = jnp.concatenate([low[:rows_o], high[:rows_o]], 0)
        basis_v = jnp.concatenate([low[rows_o:], high[rows_o:]], 0)
        none = jnp.zeros_like(basis_v)
        pair = jnp.concatenate(
            [jnp.concatenate([basis_v, none], 0), jnp.concatenate([none, basis_v], 0)], 1
        )
        first = first + dot(got_ref[g, :each, :], basis_o)
        second = second + dot(got_ref[g, each:, :], pair)
    first, second = first.astype(BF), second.astype(BF)
    for p in range(out_ref.shape[0]):
        out_ref[p, :, :rank] = first
        out_ref[p, :half, rank:] = second[:, :rank]
        out_ref[p, half:, rank:] = second[:, rank:]


def lift(got, blocks, rows_o):
    groups, packed, _ = got.shape
    return pl.pallas_call(
        functools.partial(lift_kernel, rows_o),
        out_shape=jax.ShapeDtypeStruct((groups, 2 * packed // 3, 2 * blocks.shape[2]), BF),
        cost_estimate=pl.CostEstimate(flops=2 * 10**8, bytes_accessed=3 * 10**6, transcendentals=0),
        compiler_params=pltpu.CompilerParams(vmem_limit_bytes=ROOM),
        name="lift",
    )(got, blocks)


def spread_kernel(got_ref, out_ref):
    total = got_ref[0].astype(F32)
    for i in range(1, got_ref.shape[0]):
        total = total + got_ref[i].astype(F32)
    total = total.astype(out_ref.dtype)
    for i in range(out_ref.shape[0]):
        out_ref[i] = total


def summed_for(got, copies, kind):
    return pl.pallas_call(
        spread_kernel,
        out_shape=jax.ShapeDtypeStruct((copies, *got.shape[1:]), kind),
        cost_estimate=pl.CostEstimate(flops=10**7, bytes_accessed=10**6, transcendentals=0),
        compiler_params=pltpu.CompilerParams(vmem_limit_bytes=ROOM),
    )(got)


def contract_kernel(lifted_ref, cot_o, cot_v, out_ref, total_o, total_v):
    step = pl.program_id(0)
    rank = total_o.shape[0]
    dims = (((0,), (0,)), ((), ()))

    def term(side, cot):
        rows = lifted_ref[:, side * rank : (side + 1) * rank]
        return lax.dot_general(rows, cot[...], dims, preferred_element_type=F32)

    @pl.when(step == 0)
    def _():
        total_o[...] = term(0, cot_o)
        total_v[...] = term(1, cot_v)

    @pl.when(step > 0)
    def _():
        total_o[...] += term(0, cot_o)
        total_v[...] += term(1, cot_v)

    @pl.when(step == pl.num_programs(0) - 1)
    def _():
        cols_o = total_o.shape[1]
        parts, each, _ = out_ref.shape
        for p in range(parts):
            out_ref[p, :, :cols_o] = total_o[p * each : (p + 1) * each].astype(BF)
            out_ref[p, :, cols_o:] = total_v[p * each : (p + 1) * each].astype(BF)


def contract(lifted, cot_o, cot_v, parts, steps):
    tokens, both = lifted.shape
    rank, cols_o, cols_v = both // 2, cot_o.shape[1], cot_v.shape[1]
    rows = tokens // steps
    shape = (parts, rank // parts, cols_o + cols_v)
    return pl.pallas_call(
        contract_kernel,
        grid=(steps,),
        in_specs=[
            pl.BlockSpec((rows, both), lambda i: (i, 0)),
            pl.BlockSpec((rows, cols_o), lambda i: (i, 0)),
            pl.BlockSpec((rows, cols_v), lambda i: (i, 0)),
        ],
        out_specs=pl.BlockSpec(shape, lambda i: (0, 0, 0)),
        out_shape=jax.ShapeDtypeStruct(shape, BF),
        scratch_shapes=[pltpu.VMEM((rank, cols_o), F32), pltpu.VMEM((rank, cols_v), F32)],
        cost_estimate=pl.CostEstimate(flops=3 * 10**8, bytes_accessed=3 * 10**6, transcendentals=0),
        compiler_params=pltpu.CompilerParams(vmem_limit_bytes=ROOM),
        name="contract",
    )(lifted, cot_o, cot_v)


def direction_kernel(
    rows_o, cols_o, got_ref, mean_o, square_o, mean_v, square_v, blocks_ref,
    mean_o_out, square_o_out, mean_v_out, square_v_out, total_out,
):
    near = got_ref.shape[0]
    proj = jnp.concatenate([got_ref[i] for i in range(near)], 0).astype(F32)
    mean = jnp.concatenate([mean_o[...], mean_v[...]], 1)
    square = jnp.concatenate([square_o[...], square_v[...]], 1)
    mean = MEAN_DECAY * mean + (1.0 - MEAN_DECAY) * proj
    square = BETA_SQUARE * square + (1.0 - BETA_SQUARE) * proj * proj
    mean_o_out[...] = mean[:, :cols_o]
    mean_v_out[...] = mean[:, cols_o:]
    square_o_out[...] = square[:, :cols_o]
    square_v_out[...] = square[:, cols_o:]
    upper = (mean / jnp.sqrt(square)).astype(BF)
    upper_o, upper_v = upper[:, :cols_o], upper[:, cols_o:]
    total_o = jnp.zeros((8, cols_o), F32)
    total_v = jnp.zeros((8, upper_v.shape[1]), F32)
    for group in range(4):
        blocks = [blocks_ref[group * 8 + i] for i in range(8)]
        basis_o = jnp.concatenate([b[:rows_o] for b in blocks], 0)
        basis_v = jnp.concatenate([b[rows_o:] for b in blocks], 0)
        update = dot(basis_o, upper_o)
        total_o = total_o + jnp.sum((update * update).reshape(-1, 8, cols_o), 0)
        update = dot(basis_v, upper_v)
        total_v = total_v + jnp.sum((update * update).reshape(-1, 8, update.shape[1]), 0)
    sums = [
        jnp.broadcast_to(jnp.sum(t, keepdims=True), (4, 128)) for t in (total_o, total_v)
    ]
    tile = jnp.concatenate(sums, 0)
    for i in range(total_out.shape[0]):
        total_out[i] = tile


def directions(rows_o, copies, got, mean_o, square_o, mean_v, square_v, blocks):
    cols_o = mean_o.shape[1]
    shape = jax.ShapeDtypeStruct
    return pl.pallas_call(
        functools.partial(direction_kernel, rows_o, cols_o),
        out_shape=(
            shape(mean_o.shape, F32),
            shape(mean_o.shape, F32),
            shape(mean_v.shape, F32),
            shape(mean_v.shape, F32),
            shape((copies, 8, 128), F32),
        ),
        cost_estimate=pl.CostEstimate(flops=4 * 10**8, bytes_accessed=4 * 10**6, transcendentals=10**5),
        compiler_params=pltpu.CompilerParams(vmem_limit_bytes=ROOM),
        name="directions",
    )(got, mean_o, square_o, mean_v, square_v, blocks)


def ready_kernel(
    rows_o, rows_v, mean_o, square_o, mean_v, square_v, local_o, local_v, own_ref, other_ref, blocks_ref,
    step_o_out, step_v_out, update_o_out, update_v_out, old_o_out, old_v_out,
):
    uppers = []
    for mean, square, local, step_out in (
        (mean_o, square_o, local_o, step_o_out),
        (mean_v, square_v, local_v, step_v_out),
    ):
        way = mean[...] / jnp.sqrt(square[...])
        upper = way.astype(BF)
        lower = (way - upper.astype(F32)).astype(BF)
        step_out[...] = dot(local[...], upper) + dot(local[...], lower)
        uppers.append(upper)
    upper_o, upper_v = uppers
    c = lax.axis_index("c")
    z = 4 * lax.axis_index("zh") + lax.axis_index("zl")
    for group in range(4):
        blocks = [blocks_ref[group * 8 + i] for i in range(8)]
        basis_o = jnp.concatenate([b[:rows_o] for b in blocks], 0)
        basis_v = jnp.concatenate([b[rows_o:] for b in blocks], 0)
        update_o = dot(basis_o, upper_o).astype(BF)
        update_v = dot(basis_v, upper_v).astype(BF)
        for i in range(8):
            core, j = divmod(group * 8 + i, 16)
            at = (2 * j + core) * rows_o
            update_o_out[at : at + rows_o, :] = update_o[i * rows_o : (i + 1) * rows_o]
            at = (2 * j + core) * rows_v
            update_v_out[at : at + rows_v, :] = update_v[i * rows_v : (i + 1) * rows_v]
    for ref, core in ((own_ref, c), (other_ref, 1 - c)):
        for p in range(ref.shape[0]):
            behind = (p & 1) * 8 + (p >> 1 & 1) * 4 + STEPS[p >> 2]
            index = 2 * lax.rem(z + 16 - behind, 16) + core
            at = pl.multiple_of(index * rows_o, rows_o)
            old_o_out[pl.ds(at, rows_o), :128] = ref[p, :rows_o]
            old_o_out[pl.ds(at, rows_o), 128:] = ref[p, rows_o : 2 * rows_o]
            at = pl.multiple_of(index * rows_v, rows_v)
            old_v_out[pl.ds(at, rows_v), :] = ref[p, 2 * rows_o :]


def ready(moments, local_o, local_v, own, other, blocks):
    rows_o, rows_v = local_o.shape[0], local_v.shape[0]
    cols_o, cols_v = moments[0].shape[1], moments[2].shape[1]
    fs = 2 * own.shape[0]
    shape = jax.ShapeDtypeStruct
    return pl.pallas_call(
        functools.partial(ready_kernel, rows_o, rows_v),
        out_shape=(
            shape((rows_o, cols_o), F32),
            shape((rows_v, cols_v), F32),
            shape((rows_o * fs, cols_o), BF),
            shape((rows_v * fs, cols_v), BF),
            shape((rows_o * fs, cols_o), BF),
            shape((rows_v * fs, cols_v), BF),
        ),
        cost_estimate=pl.CostEstimate(flops=4 * 10**8, bytes_accessed=4 * 10**6, transcendentals=0),
        compiler_params=pltpu.CompilerParams(vmem_limit_bytes=WHOLE),
        name="ready",
    )(*moments, local_o, local_v, own, other, blocks)


def output_kernel(
    counts, pieces, total_ref, weight_o, weight_v, step_o, step_v, update_o, update_v, old_o, old_v,
    step_o_out, new_o_out, copy_o_out, step_v_out, new_v_out, copy_v_out,
    update_o_here, update_v_here, old_o_here, old_v_here, sems,
):
    copies = []
    for n, (source, here) in enumerate(
        ((update_o, update_o_here), (old_o, old_o_here), (update_v, update_v_here), (old_v, old_v_here))
    ):
        rows = source.shape[0] // pieces
        for p in range(pieces):
            part = pl.ds(p * rows, rows)
            copies.append(pltpu.make_async_copy(source.at[part], here.at[part], sems.at[n, p]))
    for copy in copies:
        copy.start()
    total = total_ref[0]
    for i in range(1, total_ref.shape[0]):
        total = total + total_ref[i]
    scales = []
    for row, count, weight, step, step_out, new_out in (
        (0, counts[0], weight_o, step_o, step_o_out, new_o_out),
        (4, counts[1], weight_v, step_v, step_v_out, new_v_out),
    ):
        scale = LEARN_RATE * lax.rsqrt(total[row : row + 1, 0:1] / count + EPS_RMS)
        mine = step[...] * scale
        step_out[...] = mine
        new_out[...] = weight[...] - mine
        scales.append(scale)
    for n, (scale, update, old, copy_out) in enumerate(
        (
            (scales[0], update_o_here, old_o_here, copy_o_out),
            (scales[1], update_v_here, old_v_here, copy_v_out),
        )
    ):
        rows = old.shape[0] // pieces
        for p in range(pieces):
            copies[2 * n * pieces + p].wait()
            copies[(2 * n + 1) * pieces + p].wait()
            part = pl.ds(p * rows, rows)
            copy_out[part, :] = (old[part, :].astype(F32) - update[part, :].astype(F32) * scale).astype(BF)


def outputs(counts, total, weight_o, weight_v, step_o, step_v, update_o, update_v, old_o, old_v):
    shape = jax.ShapeDtypeStruct
    vmem = pl.BlockSpec(memory_space=pltpu.VMEM)
    hbm = pl.BlockSpec(memory_space=pltpu.HBM)
    pieces = 4
    return pl.pallas_call(
        functools.partial(output_kernel, counts, pieces),
        in_specs=[vmem] * 5 + [hbm] * 4,
        out_shape=(
            shape(weight_o.shape, F32),
            shape(weight_o.shape, F32),
            shape(old_o.shape, BF),
            shape(weight_v.shape, F32),
            shape(weight_v.shape, F32),
            shape(old_v.shape, BF),
        ),
        scratch_shapes=[pltpu.VMEM(a.shape, BF) for a in (update_o, update_v, old_o, old_v)]
        + [pltpu.SemaphoreType.DMA((4, pieces))],
        cost_estimate=pl.CostEstimate(flops=10**7, bytes_accessed=4 * 10**6, transcendentals=10),
        compiler_params=pltpu.CompilerParams(vmem_limit_bytes=WHOLE),
        name="outputs",
    )(total, weight_o, weight_v, step_o, step_v, update_o, update_v, old_o, old_v)


def per_device(
    attn_out,
    out_cot,
    latent,
    value_cot,
    out_weight,
    value_up_matrix,
    out_basis,
    value_basis,
    out_mean,
    out_square,
    value_mean,
    value_square,
):
    tokens = attn_out.shape[0]
    cols_o = out_cot.shape[1]
    cols_v = value_cot.shape[1]
    rows_o, rank = out_basis.shape
    rows_v = value_basis.shape[0]
    tp = lax.axis_size(TP)
    fs = lax.axis_size(FS)


    block = swapped_blocks(jnp.concatenate([out_basis, value_basis], 0))

    sent = pack(attn_out, latent.T, tp)
    got = exchange(sent, TP)

    own = old_rows(out_weight, value_up_matrix)[None]
    for k in (8, 4):
        more = shifted(own, Z, k)
        own = lax.optimization_barrier(jnp.concatenate([own, more], 0))
    rows = [own]
    for k in STEPS[1:]:
        rows.append(shifted(own, Z, k))
    own = lax.optimization_barrier(jnp.concatenate(rows, 0))
    other = shifted(own, "c", 1)

    blocks = from_everyone(block, ("c", "y", "x"))
    lifted = lift(got, blocks, rows_o)
    lifted = exchange(lifted, TP).reshape(tokens, 2 * rank)

    near = lax.axis_size(NEAR)
    part = contract(lifted, out_cot, value_cot, near, 4)
    part = exchange(part, NEAR)
    part = exchange(summed_for(part, lax.axis_size("zh"), BF), "zh")
    proj = exchange(summed_for(part, near, BF), NEAR)

    mean_o, square_o, mean_v, square_v, total = directions(
        rows_o, tp, proj, out_mean, out_square, value_mean, value_square, blocks
    )
    total = exchange(total, TP)
    moments = (mean_o, square_o, mean_v, square_v)
    prepared = ready(moments, out_basis, value_basis, own, other, blocks)
    counts = (rows_o * fs * cols_o * tp, rows_v * fs * cols_v * tp)
    step_o, new_o, copy_o, step_v, new_v, copy_v = outputs(
        counts, total, out_weight, value_up_matrix, *prepared
    )
    return (step_o, new_o, copy_o, mean_o, square_o, step_v, new_v, copy_v, mean_v, square_v)


def solution(mesh):
    torus = Mesh(mesh.devices.reshape(4, 4, 2, 4, 4), ALL)
    both = P(FS, TP)
    cols = P(None, TP)
    rows = P(FS, None)

    return jax.shard_map(
        per_device,
        mesh=torus,
        in_specs=(both, both, both, both, both, both, rows, rows, cols, cols, cols, cols),
        out_specs=(both, both, cols, cols, cols, both, both, cols, cols, cols),
        check_vma=False,
    )
```

```python
import functools

import jax
import jax.numpy as jnp
from jax import lax
from jax.experimental import pallas as pl
from jax.experimental.pallas import tpu as pltpu
from jax.sharding import Mesh
from jax.sharding import PartitionSpec as P


TP = ("y", "x")
FS = ("zh", "zl", "c")
NEAR = ("zl", "c")
Z = ("zh", "zl")
ALL = ("zh", "zl", "c", "y", "x")

LEARN_RATE = 0.01
MEAN_DECAY = 0.8
BETA_SQUARE = 0.9
EPS_RMS = 1e-06

BF = jnp.bfloat16
ROOM = 12 * 2**20
WHOLE = 67043328
STEPS = (0, 1, 2, -1)
F32 = jnp.float32


def exchange(value, axes):
    return lax.all_to_all(value, axes, 0, 0, tiled=True)


def from_everyone(value, axes):
    devices = lax.axis_size(axes)
    return exchange(jnp.broadcast_to(value[None], (devices, *value.shape)), axes)


def swapped_blocks(value):
    pairs = []
    for j in range(16):
        for b in range(2):
            for t in range(16):
                pairs.append(((2 * j + b) * 16 + t, (2 * t + b) * 16 + j))
    return lax.ppermute(value, ALL, pairs)


def shifted(value, axis, by):
    devices = lax.axis_size(axis)
    return lax.ppermute(value, axis, [(i, (i + by) % devices) for i in range(devices)])


def dot(a, b):
    return jnp.dot(a, b, preferred_element_type=F32)


def pack_kernel(groups, first, attn_ref, lat_ref, *refs):
    outs, (attn_here, lat_here, turned, sems) = refs[:-4], refs[-4:]
    each = attn_ref.shape[0] // groups**2
    copies = [
        pltpu.make_async_copy(lat_ref, lat_here, sems.at[0]),
        pltpu.make_async_copy(attn_ref, attn_here, sems.at[1]),
    ]
    for copy in copies:
        copy.start()
    copies[0].wait()
    turned[...] = lat_here[...].T
    copies[1].wait()
    for k, out in enumerate(outs):
        g = lax.rem(lax.axis_index("x") + first + k, groups)
        pieces = []
        for p in range(groups):
            at = pl.multiple_of((p * groups + g) * each, each)
            out[p * each : (p + 1) * each, :] = attn_here[pl.ds(at, each), :]
            pieces.append(turned[pl.ds(at, each), :])
        half = groups // 2
        for p in range(half):
            at = (groups + p) * each
            out[at : at + each, :] = jnp.concatenate([pieces[p], pieces[half + p]], axis=1)


def pack(attn_out, lat_turned, groups, first, count, limit):
    tokens, heads = attn_out.shape
    rows = tokens // groups
    hbm = pl.BlockSpec(memory_space=pltpu.HBM)
    return pl.pallas_call(
        functools.partial(pack_kernel, groups, first),
        in_specs=[hbm, hbm],
        out_shape=tuple(jax.ShapeDtypeStruct((rows + rows // 2, heads), BF) for _ in range(count)),
        scratch_shapes=[
            pltpu.VMEM(attn_out.shape, BF),
            pltpu.VMEM(lat_turned.shape, BF),
            pltpu.VMEM(lat_turned.shape[::-1], BF),
            pltpu.SemaphoreType.DMA((2,)),
        ],
        cost_estimate=pl.CostEstimate(flops=10**7, bytes_accessed=10**6, transcendentals=0),
        compiler_params=pltpu.CompilerParams(vmem_limit_bytes=limit),
    )(attn_out, lat_turned)


def old_kernel(weight_o, weight_v, out_ref):
    rows_o = weight_o.shape[0]
    out_ref[:rows_o] = weight_o[:, :128].astype(BF)
    out_ref[rows_o : 2 * rows_o] = weight_o[:, 128:].astype(BF)
    out_ref[2 * rows_o :] = weight_v[...].astype(BF)


def old_rows(weight_o, weight_v):
    rows = 2 * weight_o.shape[0] + weight_v.shape[0]
    return pl.pallas_call(
        old_kernel,
        out_shape=jax.ShapeDtypeStruct((rows, 128), BF),
        cost_estimate=pl.CostEstimate(flops=10**6, bytes_accessed=10**5, transcendentals=0),
        compiler_params=pltpu.CompilerParams(vmem_limit_bytes=ROOM),
        name="old",
    )(weight_o, weight_v)


def lift_kernel(rows_o, tokens, blocks_ref, *refs):
    gots, out_ref = refs[:-1], refs[-1]
    groups = len(gots)
    rank = blocks_ref.shape[2]
    half = tokens // 2
    first = jnp.zeros((tokens, rank), F32)
    second = jnp.zeros((half, 2 * rank), F32)
    for k, got_ref in enumerate(gots):
        g = lax.rem(lax.axis_index("x") + groups - k, groups)
        low, high = blocks_ref[g], blocks_ref[groups + g]
        basis_o = jnp.concatenate([low[:rows_o], high[:rows_o]], 0)
        basis_v = jnp.concatenate([low[rows_o:], high[rows_o:]], 0)
        none = jnp.zeros_like(basis_v)
        pair = jnp.concatenate(
            [jnp.concatenate([basis_v, none], 0), jnp.concatenate([none, basis_v], 0)], 1
        )
        first = first + dot(got_ref[:tokens, :], basis_o)
        second = second + dot(got_ref[tokens:, :], pair)
    parts, each = out_ref.shape[:2]
    for p in range(parts):
        at = p * each
        out_ref[p, :, :rank] = first[at : at + each].astype(BF)
        row, side = at % half, at // half
        out_ref[p, :, rank:] = second[row : row + each, side * rank : (side + 1) * rank].astype(BF)


def lift(blocks, gots, rows_o, tokens, parts):
    rank = blocks.shape[2]
    return pl.pallas_call(
        functools.partial(lift_kernel, rows_o, tokens),
        out_shape=jax.ShapeDtypeStruct((parts, tokens // parts, 2 * rank), BF),
        cost_estimate=pl.CostEstimate(flops=2 * 10**8, bytes_accessed=10**6, transcendentals=0),
        compiler_params=pltpu.CompilerParams(vmem_limit_bytes=ROOM),
        name="lift",
    )(blocks, *gots)


def spread_kernel(got_ref, out_ref):
    total = got_ref[0].astype(F32)
    for i in range(1, got_ref.shape[0]):
        total = total + got_ref[i].astype(F32)
    total = total.astype(out_ref.dtype)
    for i in range(out_ref.shape[0]):
        out_ref[i] = total


def summed_for(got, copies, kind):
    return pl.pallas_call(
        spread_kernel,
        out_shape=jax.ShapeDtypeStruct((copies, *got.shape[1:]), kind),
        cost_estimate=pl.CostEstimate(flops=10**7, bytes_accessed=10**6, transcendentals=0),
        compiler_params=pltpu.CompilerParams(vmem_limit_bytes=ROOM),
    )(got)


def contract_kernel(lifted_ref, cot_o, cot_v, out_ref, total_o, total_v):
    step = pl.program_id(0)
    rank = total_o.shape[0]
    dims = (((0,), (0,)), ((), ()))

    def term(side, cot):
        rows = lifted_ref[:, side * rank : (side + 1) * rank]
        return lax.dot_general(rows, cot[...], dims, preferred_element_type=F32)

    @pl.when(step == 0)
    def _():
        total_o[...] = term(0, cot_o)
        total_v[...] = term(1, cot_v)

    @pl.when(step > 0)
    def _():
        total_o[...] += term(0, cot_o)
        total_v[...] += term(1, cot_v)

    @pl.when(step == pl.num_programs(0) - 1)
    def _():
        cols_o = total_o.shape[1]
        parts, each, _ = out_ref.shape
        for p in range(parts):
            out_ref[p, :, :cols_o] = total_o[p * each : (p + 1) * each].astype(BF)
            out_ref[p, :, cols_o:] = total_v[p * each : (p + 1) * each].astype(BF)


def contract(lifted, cot_o, cot_v, parts, steps):
    tokens, both = lifted.shape
    rank, cols_o, cols_v = both // 2, cot_o.shape[1], cot_v.shape[1]
    rows = tokens // steps
    shape = (parts, rank // parts, cols_o + cols_v)
    return pl.pallas_call(
        contract_kernel,
        grid=(steps,),
        in_specs=[
            pl.BlockSpec((rows, both), lambda i: (i, 0)),
            pl.BlockSpec((rows, cols_o), lambda i: (i, 0)),
            pl.BlockSpec((rows, cols_v), lambda i: (i, 0)),
        ],
        out_specs=pl.BlockSpec(shape, lambda i: (0, 0, 0)),
        out_shape=jax.ShapeDtypeStruct(shape, BF),
        scratch_shapes=[pltpu.VMEM((rank, cols_o), F32), pltpu.VMEM((rank, cols_v), F32)],
        cost_estimate=pl.CostEstimate(flops=3 * 10**8, bytes_accessed=3 * 10**6, transcendentals=0),
        compiler_params=pltpu.CompilerParams(vmem_limit_bytes=ROOM),
        name="contract",
    )(lifted, cot_o, cot_v)


def direction_kernel(
    rows_o, cols_o, got_ref, mean_o, square_o, mean_v, square_v, b0, b1, b2, b3,
    mean_o_out, square_o_out, mean_v_out, square_v_out, total_out,
):
    near = got_ref.shape[0]
    proj = jnp.concatenate([got_ref[i] for i in range(near)], 0).astype(F32)
    mean = jnp.concatenate([mean_o[...], mean_v[...]], 1)
    square = jnp.concatenate([square_o[...], square_v[...]], 1)
    mean = MEAN_DECAY * mean + (1.0 - MEAN_DECAY) * proj
    square = BETA_SQUARE * square + (1.0 - BETA_SQUARE) * proj * proj
    mean_o_out[...] = mean[:, :cols_o]
    mean_v_out[...] = mean[:, cols_o:]
    square_o_out[...] = square[:, :cols_o]
    square_v_out[...] = square[:, cols_o:]
    upper = (mean / jnp.sqrt(square)).astype(BF)
    upper_o, upper_v = upper[:, :cols_o], upper[:, cols_o:]
    total_o = jnp.zeros((8, cols_o), F32)
    total_v = jnp.zeros((8, upper_v.shape[1]), F32)
    for ref in (b0, b1, b2, b3):
        count = ref.shape[0]
        basis_o = jnp.concatenate([ref[i, :rows_o, :] for i in range(count)], 0)
        basis_v = jnp.concatenate([ref[i, rows_o:, :] for i in range(count)], 0)
        update = dot(basis_o, upper_o)
        total_o = total_o + jnp.sum((update * update).reshape(-1, 8, cols_o), 0)
        update = dot(basis_v, upper_v)
        total_v = total_v + jnp.sum((update * update).reshape(-1, 8, update.shape[1]), 0)
    sums = [
        jnp.broadcast_to(jnp.sum(t, keepdims=True), (4, 128)) for t in (total_o, total_v)
    ]
    tile = jnp.concatenate(sums, 0)
    for i in range(total_out.shape[0]):
        total_out[i] = tile


def directions(rows_o, copies, got, mean_o, square_o, mean_v, square_v, segments):
    cols_o = mean_o.shape[1]
    shape = jax.ShapeDtypeStruct
    return pl.pallas_call(
        functools.partial(direction_kernel, rows_o, cols_o),
        out_shape=(
            shape(mean_o.shape, F32),
            shape(mean_o.shape, F32),
            shape(mean_v.shape, F32),
            shape(mean_v.shape, F32),
            shape((copies, 8, 128), F32),
        ),
        cost_estimate=pl.CostEstimate(flops=4 * 10**8, bytes_accessed=4 * 10**6, transcendentals=10**5),
        compiler_params=pltpu.CompilerParams(vmem_limit_bytes=ROOM),
        name="directions",
    )(got, mean_o, square_o, mean_v, square_v, *segments)


def ready_kernel(
    rows_o, rows_v, mean_o, square_o, mean_v, square_v, local_o, local_v, h0, h1, h2, h3, b0, b1, b2, b3,
    step_o_out, step_v_out, update_o_out, update_v_out, old_o_out, old_v_out,
):
    uppers = []
    for mean, square, local, step_out in (
        (mean_o, square_o, local_o, step_o_out),
        (mean_v, square_v, local_v, step_v_out),
    ):
        way = mean[...] / jnp.sqrt(square[...])
        upper = way.astype(BF)
        lower = (way - upper.astype(F32)).astype(BF)
        step_out[...] = dot(local[...], upper) + dot(local[...], lower)
        uppers.append(upper)
    upper_o, upper_v = uppers
    y, c = lax.axis_index("y"), lax.axis_index("c")
    z = 4 * lax.axis_index("zh") + lax.axis_index("zl")
    for k, ref in enumerate((b0, b1, b2, b3)):
        origin = lax.rem(y + 4 - k, 4)
        count = ref.shape[0]
        basis_o = jnp.concatenate([ref[i, :rows_o, :] for i in range(count)], 0)
        basis_v = jnp.concatenate([ref[i, rows_o:, :] for i in range(count)], 0)
        update_o = dot(basis_o, upper_o).astype(BF)
        update_v = dot(basis_v, upper_v).astype(BF)
        for i in range(count):
            core, x = divmod(i, count // 2)
            index = 8 * origin + 2 * x + core
            at = pl.multiple_of(index * rows_o, rows_o)
            update_o_out[pl.ds(at, rows_o), :] = update_o[i * rows_o : (i + 1) * rows_o]
            at = pl.multiple_of(index * rows_v, rows_v)
            update_v_out[pl.ds(at, rows_v), :] = update_v[i * rows_v : (i + 1) * rows_v]
    for ref, step in zip((h0, h1, h2, h3), STEPS):
        for p in range(8):
            behind = (0, 8, 4, 12)[p & 3] + step
            core = c if p < 4 else 1 - c
            index = 2 * lax.rem(z + 32 - behind, 16) + core
            at = pl.multiple_of(index * rows_o, rows_o)
            old_o_out[pl.ds(at, rows_o), :128] = ref[p, :rows_o]
            old_o_out[pl.ds(at, rows_o), 128:] = ref[p, rows_o : 2 * rows_o]
            at = pl.multiple_of(index * rows_v, rows_v)
            old_v_out[pl.ds(at, rows_v), :] = ref[p, 2 * rows_o :]


def ready(moments, local_o, local_v, held, segments):
    rows_o, rows_v = local_o.shape[0], local_v.shape[0]
    cols_o, cols_v = moments[0].shape[1], moments[2].shape[1]
    fs = 4 * held[0].shape[0]
    shape = jax.ShapeDtypeStruct
    return pl.pallas_call(
        functools.partial(ready_kernel, rows_o, rows_v),
        out_shape=(
            shape((rows_o, cols_o), F32),
            shape((rows_v, cols_v), F32),
            shape((rows_o * fs, cols_o), BF),
            shape((rows_v * fs, cols_v), BF),
            shape((rows_o * fs, cols_o), BF),
            shape((rows_v * fs, cols_v), BF),
        ),
        cost_estimate=pl.CostEstimate(flops=4 * 10**8, bytes_accessed=4 * 10**6, transcendentals=0),
        compiler_params=pltpu.CompilerParams(vmem_limit_bytes=WHOLE),
        name="ready",
    )(*moments, local_o, local_v, *held, *segments)


def output_kernel(
    counts, pieces, total_ref, weight_o, weight_v, step_o, step_v, update_o, update_v, old_o, old_v,
    step_o_out, new_o_out, copy_o_out, step_v_out, new_v_out, copy_v_out,
    update_o_here, update_v_here, old_o_here, old_v_here, sems,
):
    copies = []
    for n, (source, here) in enumerate(
        ((update_o, update_o_here), (old_o, old_o_here), (update_v, update_v_here), (old_v, old_v_here))
    ):
        rows = source.shape[0] // pieces
        for p in range(pieces):
            part = pl.ds(p * rows, rows)
            copies.append(pltpu.make_async_copy(source.at[part], here.at[part], sems.at[n, p]))
    for copy in copies:
        copy.start()
    total = total_ref[0]
    for i in range(1, total_ref.shape[0]):
        total = total + total_ref[i]
    scales = []
    for row, count, weight, step, step_out, new_out in (
        (0, counts[0], weight_o, step_o, step_o_out, new_o_out),
        (4, counts[1], weight_v, step_v, step_v_out, new_v_out),
    ):
        scale = LEARN_RATE * lax.rsqrt(total[row : row + 1, 0:1] / count + EPS_RMS)
        mine = step[...] * scale
        step_out[...] = mine
        new_out[...] = weight[...] - mine
        scales.append(scale)
    for n, (scale, update, old, copy_out) in enumerate(
        (
            (scales[0], update_o_here, old_o_here, copy_o_out),
            (scales[1], update_v_here, old_v_here, copy_v_out),
        )
    ):
        rows = old.shape[0] // pieces
        for p in range(pieces):
            copies[2 * n * pieces + p].wait()
            copies[(2 * n + 1) * pieces + p].wait()
            part = pl.ds(p * rows, rows)
            copy_out[part, :] = (old[part, :].astype(F32) - update[part, :].astype(F32) * scale).astype(BF)


def outputs(counts, total, weight_o, weight_v, step_o, step_v, update_o, update_v, old_o, old_v):
    shape = jax.ShapeDtypeStruct
    vmem = pl.BlockSpec(memory_space=pltpu.VMEM)
    hbm = pl.BlockSpec(memory_space=pltpu.HBM)
    pieces = 4
    return pl.pallas_call(
        functools.partial(output_kernel, counts, pieces),
        in_specs=[vmem] * 5 + [hbm] * 4,
        out_shape=(
            shape(weight_o.shape, F32),
            shape(weight_o.shape, F32),
            shape(old_o.shape, BF),
            shape(weight_v.shape, F32),
            shape(weight_v.shape, F32),
            shape(old_v.shape, BF),
        ),
        scratch_shapes=[pltpu.VMEM(a.shape, BF) for a in (update_o, update_v, old_o, old_v)]
        + [pltpu.SemaphoreType.DMA((4, pieces))],
        cost_estimate=pl.CostEstimate(flops=10**7, bytes_accessed=4 * 10**6, transcendentals=10),
        compiler_params=pltpu.CompilerParams(vmem_limit_bytes=WHOLE),
        name="outputs",
    )(total, weight_o, weight_v, step_o, step_v, update_o, update_v, old_o, old_v)


def per_device(
    attn_out,
    out_cot,
    latent,
    value_cot,
    out_weight,
    value_up_matrix,
    out_basis,
    value_basis,
    out_mean,
    out_square,
    value_mean,
    value_square,
):
    tokens = attn_out.shape[0]
    cols_o = out_cot.shape[1]
    cols_v = value_cot.shape[1]
    rows_o, rank = out_basis.shape
    rows_v = value_basis.shape[0]
    tp = lax.axis_size(TP)
    fs = lax.axis_size(FS)
    xs, ys = lax.axis_size("x"), lax.axis_size("y")


    block = swapped_blocks(jnp.concatenate([out_basis, value_basis], 0))

    gots = [None, *pack(attn_out, latent.T, xs, 1, xs - 1, WHOLE - 380000)]
    gots[:1] = pack(attn_out, latent.T, xs, 0, 1, ROOM)
    for k in range(1, xs):
        gots[k] = shifted(gots[k], "x", k)

    own = old_rows(out_weight, value_up_matrix)[None]
    for k in (8, 4):
        more = shifted(own, Z, k)
        own = lax.optimization_barrier(jnp.concatenate([own, more], 0))
    other = shifted(own, "c", 1)
    own = lax.optimization_barrier(jnp.concatenate([own, other], 0))
    held = [own]
    for k in STEPS[1:]:
        held.append(shifted(own, Z, k))

    blocks = from_everyone(block, ("c", "x"))
    partial = lift(blocks, gots, rows_o, tokens // xs, ys)
    partial = exchange(partial, "y")
    lifted = summed_for(partial, tp, BF)
    lifted = exchange(lifted, TP).reshape(tokens, 2 * rank)

    near = lax.axis_size(NEAR)
    part = contract(lifted, out_cot, value_cot, near, 4)
    part = exchange(part, NEAR)
    part = exchange(summed_for(part, lax.axis_size("zh"), BF), "zh")
    proj = exchange(summed_for(part, near, BF), NEAR)

    segments = [blocks]
    for k in range(1, ys):
        segments.append(shifted(blocks, "y", k))

    mean_o, square_o, mean_v, square_v, total = directions(
        rows_o, tp, proj, out_mean, out_square, value_mean, value_square, segments
    )
    total = exchange(total, TP)
    moments = (mean_o, square_o, mean_v, square_v)
    prepared = ready(moments, out_basis, value_basis, held, segments)
    counts = (rows_o * fs * cols_o * tp, rows_v * fs * cols_v * tp)
    step_o, new_o, copy_o, step_v, new_v, copy_v = outputs(
        counts, total, out_weight, value_up_matrix, *prepared
    )
    return (step_o, new_o, copy_o, mean_o, square_o, step_v, new_v, copy_v, mean_v, square_v)


def solution(mesh):
    torus = Mesh(mesh.devices.reshape(4, 4, 2, 4, 4), ALL)
    both = P(FS, TP)
    cols = P(None, TP)
    rows = P(FS, None)

    return jax.shard_map(
        per_device,
        mesh=torus,
        in_specs=(both, both, both, both, both, both, rows, rows, cols, cols, cols, cols),
        out_specs=(both, both, cols, cols, cols, both, both, cols, cols, cols),
        check_vma=False,
    )
```

```python
import functools

import jax
import jax.numpy as jnp
from jax import lax
from jax.experimental import pallas as pl
from jax.experimental.pallas import tpu as pltpu
from jax.sharding import Mesh
from jax.sharding import PartitionSpec as P


TP = ("y", "x")
FS = ("zh", "zl", "c")
NEAR = ("zl", "c")
Z = ("zh", "zl")
ALL = ("zh", "zl", "c", "y", "x")

LEARN_RATE = 0.01
MEAN_DECAY = 0.8
BETA_SQUARE = 0.9
EPS_RMS = 1e-06

BF = jnp.bfloat16
ROOM = 12 * 2**20
WHOLE = 67043328
STEPS = (0, 1, 2, -1)
F32 = jnp.float32


def exchange(value, axes):
    return lax.all_to_all(value, axes, 0, 0, tiled=True)


def from_everyone(value, axes):
    devices = lax.axis_size(axes)
    return exchange(jnp.broadcast_to(value[None], (devices, *value.shape)), axes)


def swapped_blocks(value):
    pairs = []
    for j in range(16):
        for b in range(2):
            for t in range(16):
                pairs.append(((2 * j + b) * 16 + t, (2 * t + b) * 16 + j))
    return lax.ppermute(value, ALL, pairs)


def shifted(value, axis, by):
    devices = lax.axis_size(axis)
    return lax.ppermute(value, axis, [(i, (i + by) % devices) for i in range(devices)])


def dot(a, b):
    return jnp.dot(a, b, preferred_element_type=F32)


def pack_kernel(groups, first, attn_ref, lat_ref, *refs):
    outs, (attn_here, lat_here, turned, sems) = refs[:-4], refs[-4:]
    each = attn_ref.shape[0] // groups**2
    copies = [
        pltpu.make_async_copy(lat_ref, lat_here, sems.at[0]),
        pltpu.make_async_copy(attn_ref, attn_here, sems.at[1]),
    ]
    for copy in copies:
        copy.start()
    copies[0].wait()
    turned[...] = lat_here[...].T
    copies[1].wait()
    for k, out in enumerate(outs):
        g = lax.rem(lax.axis_index("x") + first + k, groups)
        pieces = []
        for p in range(groups):
            at = pl.multiple_of((p * groups + g) * each, each)
            out[p * each : (p + 1) * each, :] = attn_here[pl.ds(at, each), :]
            pieces.append(turned[pl.ds(at, each), :])
        half = groups // 2
        for p in range(half):
            at = (groups + p) * each
            out[at : at + each, :] = jnp.concatenate([pieces[p], pieces[half + p]], axis=1)


def pack(attn_out, lat_turned, groups, first, count, limit):
    tokens, heads = attn_out.shape
    rows = tokens // groups
    hbm = pl.BlockSpec(memory_space=pltpu.HBM)
    return pl.pallas_call(
        functools.partial(pack_kernel, groups, first),
        in_specs=[hbm, hbm],
        out_shape=tuple(jax.ShapeDtypeStruct((rows + rows // 2, heads), BF) for _ in range(count)),
        scratch_shapes=[
            pltpu.VMEM(attn_out.shape, BF),
            pltpu.VMEM(lat_turned.shape, BF),
            pltpu.VMEM(lat_turned.shape[::-1], BF),
            pltpu.SemaphoreType.DMA((2,)),
        ],
        cost_estimate=pl.CostEstimate(flops=10**7, bytes_accessed=10**6, transcendentals=0),
        compiler_params=pltpu.CompilerParams(vmem_limit_bytes=limit),
    )(attn_out, lat_turned)


def old_kernel(weight_o, weight_v, out_ref):
    rows_o = weight_o.shape[0]
    out_ref[:rows_o] = weight_o[:, :128].astype(BF)
    out_ref[rows_o : 2 * rows_o] = weight_o[:, 128:].astype(BF)
    out_ref[2 * rows_o :] = weight_v[...].astype(BF)


def old_rows(weight_o, weight_v):
    rows = 2 * weight_o.shape[0] + weight_v.shape[0]
    return pl.pallas_call(
        old_kernel,
        out_shape=jax.ShapeDtypeStruct((rows, 128), BF),
        cost_estimate=pl.CostEstimate(flops=10**6, bytes_accessed=10**5, transcendentals=0),
        compiler_params=pltpu.CompilerParams(vmem_limit_bytes=ROOM),
        name="old",
    )(weight_o, weight_v)


def lift_kernel(rows_o, tokens, blocks_ref, *refs):
    gots, out_ref = refs[:-1], refs[-1]
    groups = len(gots)
    rank = blocks_ref.shape[2]
    half = tokens // 2
    first = jnp.zeros((tokens, rank), F32)
    second = jnp.zeros((half, 2 * rank), F32)
    for k, got_ref in enumerate(gots):
        g = lax.rem(lax.axis_index("x") + groups - k, groups)
        low, high = blocks_ref[g], blocks_ref[groups + g]
        basis_o = jnp.concatenate([low[:rows_o], high[:rows_o]], 0)
        basis_v = jnp.concatenate([low[rows_o:], high[rows_o:]], 0)
        none = jnp.zeros_like(basis_v)
        pair = jnp.concatenate(
            [jnp.concatenate([basis_v, none], 0), jnp.concatenate([none, basis_v], 0)], 1
        )
        first = first + dot(got_ref[:tokens, :], basis_o)
        second = second + dot(got_ref[tokens:, :], pair)
    parts, each = out_ref.shape[:2]
    for p in range(parts):
        at = p * each
        out_ref[p, :, :rank] = first[at : at + each].astype(BF)
        row, side = at % half, at // half
        out_ref[p, :, rank:] = second[row : row + each, side * rank : (side + 1) * rank].astype(BF)


def lift(blocks, gots, rows_o, tokens, parts):
    rank = blocks.shape[2]
    return pl.pallas_call(
        functools.partial(lift_kernel, rows_o, tokens),
        out_shape=jax.ShapeDtypeStruct((parts, tokens // parts, 2 * rank), BF),
        cost_estimate=pl.CostEstimate(flops=2 * 10**8, bytes_accessed=10**6, transcendentals=0),
        compiler_params=pltpu.CompilerParams(vmem_limit_bytes=ROOM),
        name="lift",
    )(blocks, *gots)


def spread_kernel(got_ref, out_ref):
    total = got_ref[0].astype(F32)
    for i in range(1, got_ref.shape[0]):
        total = total + got_ref[i].astype(F32)
    total = total.astype(out_ref.dtype)
    for i in range(out_ref.shape[0]):
        out_ref[i] = total


def summed_for(got, copies, kind):
    return pl.pallas_call(
        spread_kernel,
        out_shape=jax.ShapeDtypeStruct((copies, *got.shape[1:]), kind),
        cost_estimate=pl.CostEstimate(flops=10**7, bytes_accessed=10**6, transcendentals=0),
        compiler_params=pltpu.CompilerParams(vmem_limit_bytes=ROOM),
    )(got)


def contract_kernel(lifted_ref, cot_o, cot_v, out_ref, total_o, total_v):
    step = pl.program_id(0)
    rank = total_o.shape[0]
    dims = (((0,), (0,)), ((), ()))

    def term(side, cot):
        rows = lifted_ref[:, side * rank : (side + 1) * rank]
        return lax.dot_general(rows, cot[...], dims, preferred_element_type=F32)

    @pl.when(step == 0)
    def _():
        total_o[...] = term(0, cot_o)
        total_v[...] = term(1, cot_v)

    @pl.when(step > 0)
    def _():
        total_o[...] += term(0, cot_o)
        total_v[...] += term(1, cot_v)

    @pl.when(step == pl.num_programs(0) - 1)
    def _():
        cols_o = total_o.shape[1]
        parts, each, _ = out_ref.shape
        for p in range(parts):
            out_ref[p, :, :cols_o] = total_o[p * each : (p + 1) * each].astype(BF)
            out_ref[p, :, cols_o:] = total_v[p * each : (p + 1) * each].astype(BF)


def contract(lifted, cot_o, cot_v, parts, steps):
    tokens, both = lifted.shape
    rank, cols_o, cols_v = both // 2, cot_o.shape[1], cot_v.shape[1]
    rows = tokens // steps
    shape = (parts, rank // parts, cols_o + cols_v)
    return pl.pallas_call(
        contract_kernel,
        grid=(steps,),
        in_specs=[
            pl.BlockSpec((rows, both), lambda i: (i, 0)),
            pl.BlockSpec((rows, cols_o), lambda i: (i, 0)),
            pl.BlockSpec((rows, cols_v), lambda i: (i, 0)),
        ],
        out_specs=pl.BlockSpec(shape, lambda i: (0, 0, 0)),
        out_shape=jax.ShapeDtypeStruct(shape, BF),
        scratch_shapes=[pltpu.VMEM((rank, cols_o), F32), pltpu.VMEM((rank, cols_v), F32)],
        cost_estimate=pl.CostEstimate(flops=3 * 10**8, bytes_accessed=3 * 10**6, transcendentals=0),
        compiler_params=pltpu.CompilerParams(vmem_limit_bytes=ROOM),
        name="contract",
    )(lifted, cot_o, cot_v)


def direction_kernel(
    rows_o, cols_o, got_ref, mean_o, square_o, mean_v, square_v, b0, b1, b2, b3,
    mean_o_out, square_o_out, mean_v_out, square_v_out, total_out,
):
    near = got_ref.shape[0]
    proj = jnp.concatenate([got_ref[i] for i in range(near)], 0).astype(F32)
    mean = jnp.concatenate([mean_o[...], mean_v[...]], 1)
    square = jnp.concatenate([square_o[...], square_v[...]], 1)
    mean = MEAN_DECAY * mean + (1.0 - MEAN_DECAY) * proj
    square = BETA_SQUARE * square + (1.0 - BETA_SQUARE) * proj * proj
    mean_o_out[...] = mean[:, :cols_o]
    mean_v_out[...] = mean[:, cols_o:]
    square_o_out[...] = square[:, :cols_o]
    square_v_out[...] = square[:, cols_o:]
    upper = (mean / jnp.sqrt(square)).astype(BF)
    upper_o, upper_v = upper[:, :cols_o], upper[:, cols_o:]
    total_o = jnp.zeros((8, cols_o), F32)
    total_v = jnp.zeros((8, upper_v.shape[1]), F32)
    for ref in (b0, b1, b2, b3):
        count = ref.shape[0]
        basis_o = jnp.concatenate([ref[i, :rows_o, :] for i in range(count)], 0)
        basis_v = jnp.concatenate([ref[i, rows_o:, :] for i in range(count)], 0)
        update = dot(basis_o, upper_o)
        total_o = total_o + jnp.sum((update * update).reshape(-1, 8, cols_o), 0)
        update = dot(basis_v, upper_v)
        total_v = total_v + jnp.sum((update * update).reshape(-1, 8, update.shape[1]), 0)
    sums = [
        jnp.broadcast_to(jnp.sum(t, keepdims=True), (4, 128)) for t in (total_o, total_v)
    ]
    tile = jnp.concatenate(sums, 0)
    for i in range(total_out.shape[0]):
        total_out[i] = tile


def directions(rows_o, copies, got, mean_o, square_o, mean_v, square_v, segments):
    cols_o = mean_o.shape[1]
    shape = jax.ShapeDtypeStruct
    return pl.pallas_call(
        functools.partial(direction_kernel, rows_o, cols_o),
        out_shape=(
            shape(mean_o.shape, F32),
            shape(mean_o.shape, F32),
            shape(mean_v.shape, F32),
            shape(mean_v.shape, F32),
            shape((copies, 8, 128), F32),
        ),
        cost_estimate=pl.CostEstimate(flops=4 * 10**8, bytes_accessed=4 * 10**6, transcendentals=10**5),
        compiler_params=pltpu.CompilerParams(vmem_limit_bytes=ROOM),
        name="directions",
    )(got, mean_o, square_o, mean_v, square_v, *segments)


def ready_kernel(
    rows_o, rows_v, mean_o, square_o, mean_v, square_v, local_o, local_v, b0, b1, b2, b3,
    step_o_out, step_v_out, update_o_out, update_v_out,
):
    uppers = []
    for mean, square, local, step_out in (
        (mean_o, square_o, local_o, step_o_out),
        (mean_v, square_v, local_v, step_v_out),
    ):
        way = mean[...] / jnp.sqrt(square[...])
        upper = way.astype(BF)
        lower = (way - upper.astype(F32)).astype(BF)
        step_out[...] = dot(local[...], upper) + dot(local[...], lower)
        uppers.append(upper)
    upper_o, upper_v = uppers
    y = lax.axis_index("y")
    for k, ref in enumerate((b0, b1, b2, b3)):
        origin = lax.rem(y + 4 - k, 4)
        count = ref.shape[0]
        basis_o = jnp.concatenate([ref[i, :rows_o, :] for i in range(count)], 0)
        basis_v = jnp.concatenate([ref[i, rows_o:, :] for i in range(count)], 0)
        update_o = dot(basis_o, upper_o).astype(BF)
        update_v = dot(basis_v, upper_v).astype(BF)
        for i in range(count):
            core, x = divmod(i, count // 2)
            index = 8 * origin + 2 * x + core
            at = pl.multiple_of(index * rows_o, rows_o)
            update_o_out[pl.ds(at, rows_o), :] = update_o[i * rows_o : (i + 1) * rows_o]
            at = pl.multiple_of(index * rows_v, rows_v)
            update_v_out[pl.ds(at, rows_v), :] = update_v[i * rows_v : (i + 1) * rows_v]


def arrange_kernel(rows_o, rows_v, h0, h1, h2, h3, old_o_out, old_v_out):
    c = lax.axis_index("c")
    z = 4 * lax.axis_index("zh") + lax.axis_index("zl")
    for ref, step in zip((h0, h1, h2, h3), STEPS):
        for p in range(8):
            behind = (0, 8, 4, 12)[p & 3] + step
            core = c if p < 4 else 1 - c
            index = 2 * lax.rem(z + 32 - behind, 16) + core
            at = pl.multiple_of(index * rows_o, rows_o)
            old_o_out[pl.ds(at, rows_o), :128] = ref[p, :rows_o]
            old_o_out[pl.ds(at, rows_o), 128:] = ref[p, rows_o : 2 * rows_o]
            at = pl.multiple_of(index * rows_v, rows_v)
            old_v_out[pl.ds(at, rows_v), :] = ref[p, 2 * rows_o :]


def arrange(rows_o, rows_v, held):
    fs = 4 * held[0].shape[0]
    shape = jax.ShapeDtypeStruct
    return pl.pallas_call(
        functools.partial(arrange_kernel, rows_o, rows_v),
        out_shape=(shape((rows_o * fs, held[0].shape[2] * 2), BF), shape((rows_v * fs, held[0].shape[2]), BF)),
        cost_estimate=pl.CostEstimate(flops=10**6, bytes_accessed=3 * 10**6, transcendentals=0),
        compiler_params=pltpu.CompilerParams(vmem_limit_bytes=ROOM),
        name="arrange",
    )(*held)


def ready(moments, local_o, local_v, fs, segments):
    rows_o, rows_v = local_o.shape[0], local_v.shape[0]
    cols_o, cols_v = moments[0].shape[1], moments[2].shape[1]
    shape = jax.ShapeDtypeStruct
    return pl.pallas_call(
        functools.partial(ready_kernel, rows_o, rows_v),
        out_shape=(
            shape((rows_o, cols_o), F32),
            shape((rows_v, cols_v), F32),
            shape((rows_o * fs, cols_o), BF),
            shape((rows_v * fs, cols_v), BF),
        ),
        cost_estimate=pl.CostEstimate(flops=4 * 10**8, bytes_accessed=4 * 10**6, transcendentals=0),
        compiler_params=pltpu.CompilerParams(vmem_limit_bytes=WHOLE),
        name="ready",
    )(*moments, local_o, local_v, *segments)


def output_kernel(
    counts, pieces, total_ref, weight_o, weight_v, step_o, step_v, update_o, update_v, old_o, old_v,
    step_o_out, new_o_out, copy_o_out, step_v_out, new_v_out, copy_v_out,
    update_o_here, update_v_here, old_o_here, old_v_here, sems,
):
    copies = []
    for n, (source, here) in enumerate(
        ((update_o, update_o_here), (old_o, old_o_here), (update_v, update_v_here), (old_v, old_v_here))
    ):
        rows = source.shape[0] // pieces
        for p in range(pieces):
            part = pl.ds(p * rows, rows)
            copies.append(pltpu.make_async_copy(source.at[part], here.at[part], sems.at[n, p]))
    for copy in copies:
        copy.start()
    total = total_ref[0]
    for i in range(1, total_ref.shape[0]):
        total = total + total_ref[i]
    scales = []
    for row, count, weight, step, step_out, new_out in (
        (0, counts[0], weight_o, step_o, step_o_out, new_o_out),
        (4, counts[1], weight_v, step_v, step_v_out, new_v_out),
    ):
        scale = LEARN_RATE * lax.rsqrt(total[row : row + 1, 0:1] / count + EPS_RMS)
        mine = step[...] * scale
        step_out[...] = mine
        new_out[...] = weight[...] - mine
        scales.append(scale)
    for n, (scale, update, old, copy_out) in enumerate(
        (
            (scales[0], update_o_here, old_o_here, copy_o_out),
            (scales[1], update_v_here, old_v_here, copy_v_out),
        )
    ):
        rows = old.shape[0] // pieces
        for p in range(pieces):
            copies[2 * n * pieces + p].wait()
            copies[(2 * n + 1) * pieces + p].wait()
            part = pl.ds(p * rows, rows)
            copy_out[part, :] = (old[part, :].astype(F32) - update[part, :].astype(F32) * scale).astype(BF)


def outputs(counts, total, weight_o, weight_v, step_o, step_v, update_o, update_v, old_o, old_v):
    shape = jax.ShapeDtypeStruct
    vmem = pl.BlockSpec(memory_space=pltpu.VMEM)
    hbm = pl.BlockSpec(memory_space=pltpu.HBM)
    pieces = 4
    return pl.pallas_call(
        functools.partial(output_kernel, counts, pieces),
        in_specs=[vmem] * 5 + [hbm] * 4,
        out_shape=(
            shape(weight_o.shape, F32),
            shape(weight_o.shape, F32),
            shape(old_o.shape, BF),
            shape(weight_v.shape, F32),
            shape(weight_v.shape, F32),
            shape(old_v.shape, BF),
        ),
        scratch_shapes=[pltpu.VMEM(a.shape, BF) for a in (update_o, update_v, old_o, old_v)]
        + [pltpu.SemaphoreType.DMA((4, pieces))],
        cost_estimate=pl.CostEstimate(flops=10**7, bytes_accessed=4 * 10**6, transcendentals=10),
        compiler_params=pltpu.CompilerParams(vmem_limit_bytes=WHOLE),
        name="outputs",
    )(total, weight_o, weight_v, step_o, step_v, update_o, update_v, old_o, old_v)


def per_device(
    attn_out,
    out_cot,
    latent,
    value_cot,
    out_weight,
    value_up_matrix,
    out_basis,
    value_basis,
    out_mean,
    out_square,
    value_mean,
    value_square,
):
    tokens = attn_out.shape[0]
    cols_o = out_cot.shape[1]
    cols_v = value_cot.shape[1]
    rows_o, rank = out_basis.shape
    rows_v = value_basis.shape[0]
    tp = lax.axis_size(TP)
    fs = lax.axis_size(FS)
    xs, ys = lax.axis_size("x"), lax.axis_size("y")


    block = swapped_blocks(jnp.concatenate([out_basis, value_basis], 0))

    gots = [None, *pack(attn_out, latent.T, xs, 1, xs - 1, WHOLE - 380000)]
    gots[:1] = pack(attn_out, latent.T, xs, 0, 1, ROOM)
    for k in range(1, xs):
        gots[k] = shifted(gots[k], "x", k)

    own = old_rows(out_weight, value_up_matrix)[None]
    for k in (8, 4):
        more = shifted(own, Z, k)
        own = lax.optimization_barrier(jnp.concatenate([own, more], 0))
    other = shifted(own, "c", 1)
    own = lax.optimization_barrier(jnp.concatenate([own, other], 0))
    held = [own]
    for k in STEPS[1:]:
        held.append(shifted(own, Z, k))

    blocks = from_everyone(block, ("c", "x"))
    partial = lift(blocks, gots, rows_o, tokens // xs, ys)
    partial = exchange(partial, "y")
    lifted = summed_for(partial, tp, BF)
    lifted = exchange(lifted, TP).reshape(tokens, 2 * rank)

    near = lax.axis_size(NEAR)
    part = contract(lifted, out_cot, value_cot, near, 4)
    part = exchange(part, NEAR)
    part = exchange(summed_for(part, lax.axis_size("zh"), BF), "zh")
    proj = exchange(summed_for(part, near, BF), NEAR)

    segments = [blocks]
    for k in range(1, ys):
        segments.append(shifted(blocks, "y", k))

    old = arrange(rows_o, rows_v, held)
    mean_o, square_o, mean_v, square_v, total = directions(
        rows_o, tp, proj, out_mean, out_square, value_mean, value_square, segments
    )
    total = exchange(total, TP)
    moments = (mean_o, square_o, mean_v, square_v)
    prepared = ready(moments, out_basis, value_basis, fs, segments)
    counts = (rows_o * fs * cols_o * tp, rows_v * fs * cols_v * tp)
    step_o, new_o, copy_o, step_v, new_v, copy_v = outputs(
        counts, total, out_weight, value_up_matrix, *prepared, *old
    )
    return (step_o, new_o, copy_o, mean_o, square_o, step_v, new_v, copy_v, mean_v, square_v)


def solution(mesh):
    torus = Mesh(mesh.devices.reshape(4, 4, 2, 4, 4), ALL)
    both = P(FS, TP)
    cols = P(None, TP)
    rows = P(FS, None)

    return jax.shard_map(
        per_device,
        mesh=torus,
        in_specs=(both, both, both, both, both, both, rows, rows, cols, cols, cols, cols),
        out_specs=(both, both, cols, cols, cols, both, both, cols, cols, cols),
        check_vma=False,
    )
```

```python
import functools

import jax
import jax.numpy as jnp
from jax import lax
from jax.experimental import pallas as pl
from jax.experimental.pallas import tpu as pltpu
from jax.sharding import Mesh
from jax.sharding import PartitionSpec as P


TP = ("y", "x")
FS = ("zh", "zl", "c")
NEAR = ("zl", "c")
Z = ("zh", "zl")
ALL = ("zh", "zl", "c", "y", "x")

LEARN_RATE = 0.01
MEAN_DECAY = 0.8
BETA_SQUARE = 0.9
EPS_RMS = 1e-06

BF = jnp.bfloat16
ROOM = 12 * 2**20
WHOLE = 67043328
STEPS = (0, 1, 2, -1)
F32 = jnp.float32


def exchange(value, axes):
    return lax.all_to_all(value, axes, 0, 0, tiled=True)


def from_everyone(value, axes):
    devices = lax.axis_size(axes)
    return exchange(jnp.broadcast_to(value[None], (devices, *value.shape)), axes)


def swapped_blocks(value):
    pairs = []
    for j in range(16):
        for b in range(2):
            for t in range(16):
                pairs.append(((2 * j + b) * 16 + t, (2 * t + b) * 16 + j))
    return lax.ppermute(value, ALL, pairs)


def shifted(value, axis, by):
    devices = lax.axis_size(axis)
    return lax.ppermute(value, axis, [(i, (i + by) % devices) for i in range(devices)])


def dot(a, b):
    return jnp.dot(a, b, preferred_element_type=F32)


def pack_kernel(groups, first, attn_ref, lat_ref, *refs):
    outs, (attn_here, lat_here, turned, sems) = refs[:-4], refs[-4:]
    each = attn_ref.shape[0] // groups**2
    copies = [
        pltpu.make_async_copy(lat_ref, lat_here, sems.at[0]),
        pltpu.make_async_copy(attn_ref, attn_here, sems.at[1]),
    ]
    for copy in copies:
        copy.start()
    copies[0].wait()
    turned[...] = lat_here[...].T
    copies[1].wait()
    for k, out in enumerate(outs):
        g = lax.rem(lax.axis_index("x") + first + k, groups)
        pieces = []
        for p in range(groups):
            at = pl.multiple_of((p * groups + g) * each, each)
            out[p * each : (p + 1) * each, :] = attn_here[pl.ds(at, each), :]
            pieces.append(turned[pl.ds(at, each), :])
        half = groups // 2
        for p in range(half):
            at = (groups + p) * each
            out[at : at + each, :] = jnp.concatenate([pieces[p], pieces[half + p]], axis=1)


def pack(attn_out, lat_turned, groups, first, count, limit):
    tokens, heads = attn_out.shape
    rows = tokens // groups
    hbm = pl.BlockSpec(memory_space=pltpu.HBM)
    return pl.pallas_call(
        functools.partial(pack_kernel, groups, first),
        in_specs=[hbm, hbm],
        out_shape=tuple(jax.ShapeDtypeStruct((rows + rows // 2, heads), BF) for _ in range(count)),
        scratch_shapes=[
            pltpu.VMEM(attn_out.shape, BF),
            pltpu.VMEM(lat_turned.shape, BF),
            pltpu.VMEM(lat_turned.shape[::-1], BF),
            pltpu.SemaphoreType.DMA((2,)),
        ],
        cost_estimate=pl.CostEstimate(flops=10**7, bytes_accessed=10**6, transcendentals=0),
        compiler_params=pltpu.CompilerParams(vmem_limit_bytes=limit),
    )(attn_out, lat_turned)


def old_kernel(weight_o, weight_v, out_ref):
    rows_o = weight_o.shape[0]
    out_ref[:rows_o] = weight_o[:, :128].astype(BF)
    out_ref[rows_o : 2 * rows_o] = weight_o[:, 128:].astype(BF)
    out_ref[2 * rows_o :] = weight_v[...].astype(BF)


def old_rows(weight_o, weight_v):
    rows = 2 * weight_o.shape[0] + weight_v.shape[0]
    return pl.pallas_call(
        old_kernel,
        out_shape=jax.ShapeDtypeStruct((rows, 128), BF),
        cost_estimate=pl.CostEstimate(flops=10**6, bytes_accessed=10**5, transcendentals=0),
        compiler_params=pltpu.CompilerParams(vmem_limit_bytes=ROOM),
        name="old",
    )(weight_o, weight_v)


def lift_kernel(rows_o, tokens, blocks_ref, *refs):
    gots, out_ref = refs[:-1], refs[-1]
    groups = len(gots)
    rank = blocks_ref.shape[2]
    half = tokens // 2
    first = jnp.zeros((tokens, rank), F32)
    second = jnp.zeros((half, 2 * rank), F32)
    for k, got_ref in enumerate(gots):
        g = lax.rem(lax.axis_index("x") + groups - k, groups)
        low, high = blocks_ref[g], blocks_ref[groups + g]
        basis_o = jnp.concatenate([low[:rows_o], high[:rows_o]], 0)
        basis_v = jnp.concatenate([low[rows_o:], high[rows_o:]], 0)
        none = jnp.zeros_like(basis_v)
        pair = jnp.concatenate(
            [jnp.concatenate([basis_v, none], 0), jnp.concatenate([none, basis_v], 0)], 1
        )
        first = first + dot(got_ref[:tokens, :], basis_o)
        second = second + dot(got_ref[tokens:, :], pair)
    parts, each = out_ref.shape[:2]
    for p in range(parts):
        at = p * each
        out_ref[p, :, :rank] = first[at : at + each].astype(BF)
        row, side = at % half, at // half
        out_ref[p, :, rank:] = second[row : row + each, side * rank : (side + 1) * rank].astype(BF)


def lift(blocks, gots, rows_o, tokens, parts):
    rank = blocks.shape[2]
    return pl.pallas_call(
        functools.partial(lift_kernel, rows_o, tokens),
        out_shape=jax.ShapeDtypeStruct((parts, tokens // parts, 2 * rank), BF),
        cost_estimate=pl.CostEstimate(flops=2 * 10**8, bytes_accessed=10**6, transcendentals=0),
        compiler_params=pltpu.CompilerParams(vmem_limit_bytes=ROOM),
        name="lift",
    )(blocks, *gots)


def spread_kernel(got_ref, out_ref):
    total = got_ref[0].astype(F32)
    for i in range(1, got_ref.shape[0]):
        total = total + got_ref[i].astype(F32)
    total = total.astype(out_ref.dtype)
    for i in range(out_ref.shape[0]):
        out_ref[i] = total


def summed_for(got, copies, kind):
    return pl.pallas_call(
        spread_kernel,
        out_shape=jax.ShapeDtypeStruct((copies, *got.shape[1:]), kind),
        cost_estimate=pl.CostEstimate(flops=10**7, bytes_accessed=10**6, transcendentals=0),
        compiler_params=pltpu.CompilerParams(vmem_limit_bytes=ROOM),
    )(got)


def contract_kernel(lifted_ref, cot_o, cot_v, out_ref):
    rank = lifted_ref.shape[1] // 2
    cols_o = cot_o.shape[1]
    dims = (((0,), (0,)), ((), ()))
    total_o = lax.dot_general(lifted_ref[:, :rank], cot_o[...], dims, preferred_element_type=F32)
    total_v = lax.dot_general(lifted_ref[:, rank:], cot_v[...], dims, preferred_element_type=F32)
    parts, each, _ = out_ref.shape
    for p in range(parts):
        out_ref[p, :, :cols_o] = total_o[p * each : (p + 1) * each].astype(BF)
        out_ref[p, :, cols_o:] = total_v[p * each : (p + 1) * each].astype(BF)


def contract(lifted, cot_o, cot_v, parts):
    rank = lifted.shape[1] // 2
    return pl.pallas_call(
        contract_kernel,
        out_shape=jax.ShapeDtypeStruct((parts, rank // parts, cot_o.shape[1] + cot_v.shape[1]), BF),
        cost_estimate=pl.CostEstimate(flops=3 * 10**8, bytes_accessed=3 * 10**6, transcendentals=0),
        compiler_params=pltpu.CompilerParams(vmem_limit_bytes=ROOM),
        name="contract",
    )(lifted, cot_o, cot_v)


def direction_kernel(
    rows_o, cols_o, got_ref, mean_o, square_o, mean_v, square_v, b0, b1, b2, b3,
    mean_o_out, square_o_out, mean_v_out, square_v_out, total_out,
):
    near = got_ref.shape[0]
    proj = jnp.concatenate([got_ref[i] for i in range(near)], 0).astype(F32)
    mean = jnp.concatenate([mean_o[...], mean_v[...]], 1)
    square = jnp.concatenate([square_o[...], square_v[...]], 1)
    mean = MEAN_DECAY * mean + (1.0 - MEAN_DECAY) * proj
    square = BETA_SQUARE * square + (1.0 - BETA_SQUARE) * proj * proj
    mean_o_out[...] = mean[:, :cols_o]
    mean_v_out[...] = mean[:, cols_o:]
    square_o_out[...] = square[:, :cols_o]
    square_v_out[...] = square[:, cols_o:]
    upper = (mean / jnp.sqrt(square)).astype(BF)
    upper_o, upper_v = upper[:, :cols_o], upper[:, cols_o:]
    total_o = jnp.zeros((8, cols_o), F32)
    total_v = jnp.zeros((8, upper_v.shape[1]), F32)
    for ref in (b0, b1, b2, b3):
        count = ref.shape[0]
        basis_o = jnp.concatenate([ref[i, :rows_o, :] for i in range(count)], 0)
        basis_v = jnp.concatenate([ref[i, rows_o:, :] for i in range(count)], 0)
        update = dot(basis_o, upper_o)
        total_o = total_o + jnp.sum((update * update).reshape(-1, 8, cols_o), 0)
        update = dot(basis_v, upper_v)
        total_v = total_v + jnp.sum((update * update).reshape(-1, 8, update.shape[1]), 0)
    sums = [
        jnp.broadcast_to(jnp.sum(t, keepdims=True), (4, 128)) for t in (total_o, total_v)
    ]
    tile = jnp.concatenate(sums, 0)
    for i in range(total_out.shape[0]):
        total_out[i] = tile


def directions(rows_o, copies, got, mean_o, square_o, mean_v, square_v, segments):
    cols_o = mean_o.shape[1]
    shape = jax.ShapeDtypeStruct
    return pl.pallas_call(
        functools.partial(direction_kernel, rows_o, cols_o),
        out_shape=(
            shape(mean_o.shape, F32),
            shape(mean_o.shape, F32),
            shape(mean_v.shape, F32),
            shape(mean_v.shape, F32),
            shape((copies, 8, 128), F32),
        ),
        cost_estimate=pl.CostEstimate(flops=4 * 10**8, bytes_accessed=4 * 10**6, transcendentals=10**5),
        compiler_params=pltpu.CompilerParams(vmem_limit_bytes=ROOM),
        name="directions",
    )(got, mean_o, square_o, mean_v, square_v, *segments)


def ready_kernel(
    rows_o, rows_v, mean_o, square_o, mean_v, square_v, local_o, local_v, b0, b1, b2, b3,
    step_o_out, step_v_out, update_o_out, update_v_out,
):
    uppers = []
    for mean, square, local, step_out in (
        (mean_o, square_o, local_o, step_o_out),
        (mean_v, square_v, local_v, step_v_out),
    ):
        way = mean[...] / jnp.sqrt(square[...])
        upper = way.astype(BF)
        lower = (way - upper.astype(F32)).astype(BF)
        step_out[...] = dot(local[...], upper) + dot(local[...], lower)
        uppers.append(upper)
    upper_o, upper_v = uppers
    y = lax.axis_index("y")
    for k, ref in enumerate((b0, b1, b2, b3)):
        origin = lax.rem(y + 4 - k, 4)
        count = ref.shape[0]
        basis_o = jnp.concatenate([ref[i, :rows_o, :] for i in range(count)], 0)
        basis_v = jnp.concatenate([ref[i, rows_o:, :] for i in range(count)], 0)
        update_o = dot(basis_o, upper_o).astype(BF)
        update_v = dot(basis_v, upper_v).astype(BF)
        for i in range(count):
            core, x = divmod(i, count // 2)
            index = 8 * origin + 2 * x + core
            at = pl.multiple_of(index * rows_o, rows_o)
            update_o_out[pl.ds(at, rows_o), :] = update_o[i * rows_o : (i + 1) * rows_o]
            at = pl.multiple_of(index * rows_v, rows_v)
            update_v_out[pl.ds(at, rows_v), :] = update_v[i * rows_v : (i + 1) * rows_v]


def arrange_kernel(rows_o, rows_v, h0, h1, h2, h3, old_o_out, old_v_out):
    c = lax.axis_index("c")
    z = 4 * lax.axis_index("zh") + lax.axis_index("zl")
    for ref, step in zip((h0, h1, h2, h3), STEPS):
        for p in range(8):
            behind = (0, 8, 4, 12)[p & 3] + step
            core = c if p < 4 else 1 - c
            index = 2 * lax.rem(z + 32 - behind, 16) + core
            at = pl.multiple_of(index * rows_o, rows_o)
            old_o_out[pl.ds(at, rows_o), :128] = ref[p, :rows_o]
            old_o_out[pl.ds(at, rows_o), 128:] = ref[p, rows_o : 2 * rows_o]
            at = pl.multiple_of(index * rows_v, rows_v)
            old_v_out[pl.ds(at, rows_v), :] = ref[p, 2 * rows_o :]


def arrange(rows_o, rows_v, held):
    fs = 4 * held[0].shape[0]
    shape = jax.ShapeDtypeStruct
    return pl.pallas_call(
        functools.partial(arrange_kernel, rows_o, rows_v),
        out_shape=(shape((rows_o * fs, held[0].shape[2] * 2), BF), shape((rows_v * fs, held[0].shape[2]), BF)),
        cost_estimate=pl.CostEstimate(flops=10**6, bytes_accessed=3 * 10**6, transcendentals=0),
        compiler_params=pltpu.CompilerParams(vmem_limit_bytes=ROOM),
        name="arrange",
    )(*held)


def ready(moments, local_o, local_v, fs, segments):
    rows_o, rows_v = local_o.shape[0], local_v.shape[0]
    cols_o, cols_v = moments[0].shape[1], moments[2].shape[1]
    shape = jax.ShapeDtypeStruct
    return pl.pallas_call(
        functools.partial(ready_kernel, rows_o, rows_v),
        out_shape=(
            shape((rows_o, cols_o), F32),
            shape((rows_v, cols_v), F32),
            shape((rows_o * fs, cols_o), BF),
            shape((rows_v * fs, cols_v), BF),
        ),
        cost_estimate=pl.CostEstimate(flops=4 * 10**8, bytes_accessed=4 * 10**6, transcendentals=0),
        compiler_params=pltpu.CompilerParams(vmem_limit_bytes=WHOLE),
        name="ready",
    )(*moments, local_o, local_v, *segments)


def output_kernel(
    counts, pieces, total_ref, weight_o, weight_v, step_o, step_v, update_o, update_v, old_o, old_v,
    step_o_out, new_o_out, copy_o_out, step_v_out, new_v_out, copy_v_out,
    update_o_here, update_v_here, old_o_here, old_v_here, sems,
):
    copies = []
    for n, (source, here) in enumerate(
        ((update_o, update_o_here), (old_o, old_o_here), (update_v, update_v_here), (old_v, old_v_here))
    ):
        rows = source.shape[0] // pieces
        for p in range(pieces):
            part = pl.ds(p * rows, rows)
            copies.append(pltpu.make_async_copy(source.at[part], here.at[part], sems.at[n, p]))
    for copy in copies:
        copy.start()
    total = total_ref[0]
    for i in range(1, total_ref.shape[0]):
        total = total + total_ref[i]
    scales = []
    for row, count, weight, step, step_out, new_out in (
        (0, counts[0], weight_o, step_o, step_o_out, new_o_out),
        (4, counts[1], weight_v, step_v, step_v_out, new_v_out),
    ):
        scale = LEARN_RATE * lax.rsqrt(total[row : row + 1, 0:1] / count + EPS_RMS)
        mine = step[...] * scale
        step_out[...] = mine
        new_out[...] = weight[...] - mine
        scales.append(scale)
    for n, (scale, update, old, copy_out) in enumerate(
        (
            (scales[0], update_o_here, old_o_here, copy_o_out),
            (scales[1], update_v_here, old_v_here, copy_v_out),
        )
    ):
        rows = old.shape[0] // pieces
        for p in range(pieces):
            copies[2 * n * pieces + p].wait()
            copies[(2 * n + 1) * pieces + p].wait()
            part = pl.ds(p * rows, rows)
            copy_out[part, :] = (old[part, :].astype(F32) - update[part, :].astype(F32) * scale).astype(BF)


def outputs(counts, total, weight_o, weight_v, step_o, step_v, update_o, update_v, old_o, old_v):
    shape = jax.ShapeDtypeStruct
    vmem = pl.BlockSpec(memory_space=pltpu.VMEM)
    hbm = pl.BlockSpec(memory_space=pltpu.HBM)
    pieces = 4
    return pl.pallas_call(
        functools.partial(output_kernel, counts, pieces),
        in_specs=[vmem] * 5 + [hbm] * 4,
        out_shape=(
            shape(weight_o.shape, F32),
            shape(weight_o.shape, F32),
            shape(old_o.shape, BF),
            shape(weight_v.shape, F32),
            shape(weight_v.shape, F32),
            shape(old_v.shape, BF),
        ),
        scratch_shapes=[pltpu.VMEM(a.shape, BF) for a in (update_o, update_v, old_o, old_v)]
        + [pltpu.SemaphoreType.DMA((4, pieces))],
        cost_estimate=pl.CostEstimate(flops=10**7, bytes_accessed=4 * 10**6, transcendentals=10),
        compiler_params=pltpu.CompilerParams(vmem_limit_bytes=WHOLE),
        name="outputs",
    )(total, weight_o, weight_v, step_o, step_v, update_o, update_v, old_o, old_v)


def per_device(
    attn_out,
    out_cot,
    latent,
    value_cot,
    out_weight,
    value_up_matrix,
    out_basis,
    value_basis,
    out_mean,
    out_square,
    value_mean,
    value_square,
):
    tokens = attn_out.shape[0]
    cols_o = out_cot.shape[1]
    cols_v = value_cot.shape[1]
    rows_o, rank = out_basis.shape
    rows_v = value_basis.shape[0]
    tp = lax.axis_size(TP)
    fs = lax.axis_size(FS)
    xs, ys = lax.axis_size("x"), lax.axis_size("y")


    block = swapped_blocks(jnp.concatenate([out_basis, value_basis], 0))

    gots = [None, *pack(attn_out, latent.T, xs, 1, xs - 1, WHOLE - 380000)]
    gots[:1] = pack(attn_out, latent.T, xs, 0, 1, ROOM)
    for k in range(1, xs):
        gots[k] = shifted(gots[k], "x", k)

    own = old_rows(out_weight, value_up_matrix)[None]
    for k in (8, 4):
        more = shifted(own, Z, k)
        own = lax.optimization_barrier(jnp.concatenate([own, more], 0))
    other = shifted(own, "c", 1)
    own = lax.optimization_barrier(jnp.concatenate([own, other], 0))
    held = [own]
    for k in STEPS[1:]:
        held.append(shifted(own, Z, k))

    blocks = from_everyone(block, ("c", "x"))
    partial = lift(blocks, gots, rows_o, tokens // xs, ys)
    partial = exchange(partial, "y")
    lifted = summed_for(partial, tp, BF)
    lifted = exchange(lifted, TP).reshape(tokens, 2 * rank)

    near = lax.axis_size(NEAR)
    part = contract(lifted, out_cot, value_cot, near)
    part = exchange(part, NEAR)
    part = exchange(summed_for(part, lax.axis_size("zh"), BF), "zh")
    proj = exchange(summed_for(part, near, BF), NEAR)

    segments = [blocks]
    for k in range(1, ys):
        segments.append(shifted(blocks, "y", k))

    old = arrange(rows_o, rows_v, held)
    mean_o, square_o, mean_v, square_v, total = directions(
        rows_o, tp, proj, out_mean, out_square, value_mean, value_square, segments
    )
    total = exchange(total, TP)
    moments = (mean_o, square_o, mean_v, square_v)
    prepared = ready(moments, out_basis, value_basis, fs, segments)
    counts = (rows_o * fs * cols_o * tp, rows_v * fs * cols_v * tp)
    step_o, new_o, copy_o, step_v, new_v, copy_v = outputs(
        counts, total, out_weight, value_up_matrix, *prepared, *old
    )
    return (step_o, new_o, copy_o, mean_o, square_o, step_v, new_v, copy_v, mean_v, square_v)


def solution(mesh):
    torus = Mesh(mesh.devices.reshape(4, 4, 2, 4, 4), ALL)
    both = P(FS, TP)
    cols = P(None, TP)
    rows = P(FS, None)

    return jax.shard_map(
        per_device,
        mesh=torus,
        in_specs=(both, both, both, both, both, both, rows, rows, cols, cols, cols, cols),
        out_specs=(both, both, cols, cols, cols, both, both, cols, cols, cols),
        check_vma=False,
    )
```
